32 devices in a mesh: sp: 8 (over z, y), tp: 4 (over x, core).
Axes of the slice: x: 2, y: 2, z: 4, core: 2. Of those that a mesh axis runs over, the one named last changes fastest.
Arguments:
- tokens: bfloat16 [8192, 4096], P('sp', 'tp'), may hold values from -16 to 16
- norm_gain: float32 [4096], replicated, may hold values from 0.1 to 1.9
- w_pool_in: bfloat16 [4096, 2048], P('sp', 'tp'), may hold values from -0.09375 to 0.09375
- w_query: bfloat16 [4096, 2048], P('sp', 'tp'), may hold values from -0.09375 to 0.09375
- w_key: bfloat16 [4096, 256], P('sp', 'tp'), may hold values from -0.09375 to 0.09375
- w_value: bfloat16 [4096, 256], P('sp', 'tp'), may hold values from -0.09375 to 0.09375
- pool_map: bfloat16 [4, 512, 512], P('tp'), may hold values from -0.25 to 0.25
- pool_scale: float32 [2048], P('tp'), may hold values from 0.3 to 3
- q_gain: float32 [64], replicated, may hold values from 0.1 to 1.9
- k_gain: float32 [64], replicated, may hold values from 0.1 to 1.9
- sinks: float32 [32], P('tp'), may hold values from 0 to 4
- w_out: bfloat16 [4096, 4096], P('tp', 'sp'), may hold values from -0.09375 to 0.09375
Outputs:
- layer_out: bfloat16 [8192, 4096], P(('sp', 'tp'))
The draws below stay inside these ranges and needn't reach their ends.
All inputs are finite; a program needn't handle non-finite values.
Results may differ from the reference program's by a relative error of at most 0.012.
Values may be sent and summed in bfloat16 or wider, within the bound.
A program may use at most 128 MiB of HBM per device.

```python
import math
import jax
import jax.numpy as jnp
from jax import lax

D = 4096
HEAD_DIM = 64
GROUP = 8
GROUPS = 4
WINDOW = 128
GROUP_WIDTH = 512
Q_HEADS = 32
BRANCH_WIDTH = 2048
MIX = 4096
TOKENS = 8192
N_TP = 4


def draw_tokens(key, part):
    first_key, second_key = jax.random.split(jax.random.fold_in(key, 11), 2)
    base_rows = jnp.clip(jax.random.normal(first_key, (TOKENS, D), jnp.float32), -5.0, 5.0)
    row_scale = jnp.exp(jax.random.uniform(second_key, (TOKENS, 1), jnp.float32, math.log(0.3), math.log(3.0)))
    return (base_rows * row_scale).astype(jnp.bfloat16)


def shard_levels(key, extent, pieces, least, high):
    def one(dim, shards_of):
        steps = jax.random.uniform(jax.random.fold_in(jax.random.fold_in(key, 6), dim), (shards_of,), jnp.float32, least / len(pieces), high / len(pieces))
        return jnp.repeat(jnp.exp(steps), extent[dim] // shards_of).reshape((-1,) + (1,) * (len(extent) - dim - 1))

    level = one(*pieces[0])
    for cut in pieces[1:]:
        level = level * one(*cut)
    return level


def gaussian(own_key, dims, scale, bound, cuts=(), held_as=jnp.bfloat16):
    drawn = jax.random.normal(own_key, dims, jnp.float32) * scale
    if len(cuts) > 0:
        drawn = shard_levels(own_key, dims, cuts, -0.22, 0.18) * drawn
    return jnp.clip(drawn, min=-bound, max=bound).astype(held_as)


def setup_inputs(seed: int = 0) -> dict:
    splits = jax.random.split(jax.random.key(seed), 13)
    return {
        "tokens": draw_tokens(jax.random.fold_in(splits[12], 71), 0),
        "norm_gain": jnp.clip(1.0 + 0.18 * jax.random.normal(splits[1], (D,), jnp.float32), 0.1, 1.9),
        "w_pool_in": gaussian(splits[2], (D, BRANCH_WIDTH), D ** -0.5, 0.09375, ((0, 8), (1, 4))),
        "w_query": gaussian(splits[3], (D, BRANCH_WIDTH), D ** -0.5, 0.09375, ((0, 8), (1, 4))),
        "w_key": gaussian(splits[4], (D, GROUPS * HEAD_DIM), D ** -0.5, 0.09375, ((0, 8), (1, 4))),
        "w_value": gaussian(splits[5], (D, GROUPS * HEAD_DIM), D ** -0.5, 0.09375, ((0, 8), (1, 4))),
        "pool_map": gaussian(splits[6], (GROUPS, GROUP_WIDTH, GROUP_WIDTH), GROUP_WIDTH ** -0.5, 0.25, ((0, 4),)),
        "pool_scale": jnp.clip(jnp.exp(math.log(3.0) - 2.3025851 * jax.random.uniform(splits[7], (BRANCH_WIDTH,), jnp.float32) ** shard_levels(splits[7], (BRANCH_WIDTH,), ((0, 4),), -0.2, 0.2)), 0.3, 3.0),
        "q_gain": jnp.clip(1.0 + 0.18 * jax.random.normal(splits[8], (HEAD_DIM,), jnp.float32), 0.1, 1.9),
        "k_gain": jnp.clip(1.0 + 0.18 * jax.random.normal(splits[9], (HEAD_DIM,), jnp.float32), 0.1, 1.9),
        "sinks": jnp.clip(4.0 * jax.random.uniform(splits[10], (Q_HEADS,), jnp.float32) ** shard_levels(splits[10], (Q_HEADS,), ((0, 4),), -0.2, 0.2), 0.0, 4.0),
        "w_out": gaussian(splits[11], (MIX, D), MIX ** -0.5, 0.09375, ((0, 4), (1, 8))),
    }


epsilon = 1e-06

def rms_scale(values):
    return values * lax.rsqrt(lax.optimization_barrier(jnp.mean(values * values, axis=-1, keepdims=True)) + epsilon)

def reference(tokens, norm_gain, w_pool_in, w_query, w_key, w_value, pool_map, pool_scale, q_gain, k_gain, sinks, w_out):
    widened = tokens.astype(jnp.float32)
    normed = (rms_scale(widened) * norm_gain).astype(jnp.bfloat16)
    pool_in = jnp.dot(normed, w_pool_in, preferred_element_type=jnp.float32).astype(jnp.bfloat16)
    query_rows = jnp.dot(normed, w_query, preferred_element_type=jnp.float32).astype(jnp.bfloat16)
    key_rows = jnp.dot(normed, w_key, preferred_element_type=jnp.float32).astype(jnp.bfloat16)
    value_rows = jnp.dot(normed, w_value, preferred_element_type=jnp.float32).astype(jnp.bfloat16)
    query_float = lax.optimization_barrier(query_rows).astype(jnp.float32).reshape(TOKENS, Q_HEADS, HEAD_DIM)
    query_normed = (rms_scale(query_float) * q_gain).astype(jnp.bfloat16)
    key_float = lax.optimization_barrier(key_rows).astype(jnp.float32).reshape(TOKENS, GROUPS, HEAD_DIM)
    key_normed = (rms_scale(key_float) * k_gain).astype(jnp.bfloat16)
    value_heads = value_rows.reshape(TOKENS, GROUPS, HEAD_DIM)
    positions = jnp.arange(TOKENS, dtype=jnp.int32)
    pool_float = pool_in.astype(jnp.float32).reshape(TOKENS, GROUPS, GROUP_WIDTH)
    padded = jnp.pad(pool_float, ((15, 0), (0, 0), (0, 0)))
    blocks = TOKENS // WINDOW
    key_padded = jnp.concatenate([jnp.zeros((WINDOW, GROUPS, HEAD_DIM), jnp.bfloat16), key_normed], axis=0)
    value_padded = jnp.concatenate([jnp.zeros((WINDOW, GROUPS, HEAD_DIM), jnp.bfloat16), value_heads], axis=0)
    query_pos = jnp.arange(WINDOW, dtype=jnp.int32)[:, None] + WINDOW
    key_pos = jnp.arange(2 * WINDOW, dtype=jnp.int32)[None, :]
    distance = query_pos - key_pos
    in_band = (distance >= 0) & (distance < WINDOW)
    key_global = jnp.arange(blocks, dtype=jnp.int32)[:, None] * WINDOW - WINDOW + jnp.arange(2 * WINDOW, dtype=jnp.int32)[None, :]
    allowed = in_band[None] & (key_global >= 0)[:, None, :]
    branches = []
    for group_index in range(GROUPS):
        span_width = 2 ** (group_index + 1)
        running = jnp.zeros((TOKENS, GROUP_WIDTH), jnp.float32)
        for offset in range(span_width):
            running = running + padded[15 - offset:15 - offset + TOKENS, group_index]
        counts = jnp.minimum(positions.astype(jnp.float32) + 1.0, float(span_width))
        pool_diff = (running / counts[:, None] - pool_float[:, group_index]).astype(jnp.bfloat16)
        mapped = jnp.dot(pool_diff, pool_map[group_index], preferred_element_type=jnp.float32)
        mapped = mapped * pool_scale[group_index * GROUP_WIDTH:(group_index + 1) * GROUP_WIDTH]
        pool_branch = rms_scale(mapped)
        head_first = group_index * GROUP
        query_blocks = query_normed[:, head_first:head_first + GROUP].reshape(blocks, WINDOW, GROUP, HEAD_DIM).astype(jnp.float32)
        key_pairs = jnp.concatenate([key_padded[:TOKENS, group_index].reshape(blocks, WINDOW, HEAD_DIM), key_padded[WINDOW:, group_index].reshape(blocks, WINDOW, HEAD_DIM)], axis=1).astype(jnp.float32)
        value_pairs = jnp.concatenate([value_padded[:TOKENS, group_index].reshape(blocks, WINDOW, HEAD_DIM), value_padded[WINDOW:, group_index].reshape(blocks, WINDOW, HEAD_DIM)], axis=1).astype(jnp.float32)
        scores = jnp.einsum('nqgd,nkd->ngqk', query_blocks, key_pairs) * HEAD_DIM ** (-0.5)
        head_ids = head_first + jnp.arange(GROUP, dtype=jnp.int32) + 1
        slopes = jnp.exp2(-8.0 * head_ids.astype(jnp.float32) / Q_HEADS)
        logits = scores - slopes[None, :, None, None] * distance.astype(jnp.float32)[None, None]
        exp_scores = jnp.exp(jnp.where(allowed[:, None], logits, -jnp.inf))
        sink_logits = sinks[head_first:head_first + GROUP]
        denominator = lax.optimization_barrier(jnp.sum(exp_scores, axis=-1)) + jnp.exp(sink_logits)[None, :, None]
        weights_bf = (exp_scores / denominator[..., None]).astype(jnp.bfloat16)
        attended = jnp.einsum('ngqk,nkd->nqgd', weights_bf.astype(jnp.float32), value_pairs)
        attn_branch = rms_scale(attended.reshape(TOKENS, GROUP_WIDTH))
        branches.append(jnp.stack([pool_branch, attn_branch], axis=1))
    mixed_rows = jnp.stack(branches, axis=1).reshape(TOKENS, MIX).astype(jnp.bfloat16)
    block_width = MIX // N_TP
    summed = jnp.zeros((TOKENS, D), jnp.float32)
    for part_index in range(N_TP):
        row_start = part_index * block_width
        partial_term = jnp.dot(mixed_rows[:, row_start:row_start + block_width], w_out[row_start:row_start + block_width], preferred_element_type=jnp.float32).astype(jnp.bfloat16)
        summed = summed + lax.optimization_barrier(partial_term).astype(jnp.float32)
    return summed.astype(jnp.bfloat16)
```

```python
import functools

import jax
import jax.numpy as jnp
from jax import lax
from jax.experimental import pallas as pl
from jax.experimental.pallas import tpu as pltpu
from jax.sharding import PartitionSpec as P

HEAD_DIM = 64
GROUP = 8
WINDOW = 128
Q_HEADS = 32
LANES = 128
TOKEN_CHUNKS = 4
HALO_ROWS = 16
MASKED = -1e30

epsilon = 1e-06
bf16, f32 = jnp.bfloat16, jnp.float32


def ring_place(device, count):
    return jnp.where(device % 2 == 0, device // 2, count - 1 - device // 2)


def ring_device(place, count):
    place = (place + count) % count
    return jnp.where(place < count // 2, 2 * place, 2 * (count - 1 - place) + 1)


def partners():
    me = lax.axis_index("tp")
    return me, me + 1 - 2 * (me % 2), (me + 2) % 4


def greet(targets):
    barrier = pltpu.get_barrier_semaphore()
    for axis, target in targets:
        pl.semaphore_signal(
            barrier, inc=1, device_id={axis: target}, device_id_type=pl.DeviceIdType.MESH
        )
    pl.semaphore_wait(barrier, len(targets))


def remote(source, target, send_sem, recv_sem, axis, device):
    return pltpu.make_async_remote_copy(
        src_ref=source,
        dst_ref=target,
        send_sem=send_sem,
        recv_sem=recv_sem,
        device_id={axis: device},
        device_id_type=pl.DeviceIdType.MESH,
    )


def aligned(index, size):
    return pl.ds(pl.multiple_of(index * size, size), size)


def dot(left, right):
    return jnp.dot(left, right, preferred_element_type=f32)


class Ring:
    def __init__(self, count, block_at, send, recv):
        self.count, self.last = count, count // 2
        self.place = ring_place(lax.axis_index("sp"), count)
        self.targets = (
            ring_device(self.place + 1, count),
            ring_device(self.place - 1, count),
        )
        self.block_at, self.send, self.recv = block_at, send, recv
        self.started = []
        self.events = [(step, part) for step in range(1, self.last) for part in range(2)]
        self.events.append((self.last, None))
        self.done = 0

    def owner(self, distance):
        return ring_device(self.place - distance, self.count)

    def copy(self, step, way, part):
        block = self.block_at(self.owner((1 - 2 * way) * (step - 1)), part)
        return remote(
            block,
            block,
            self.send.at[way, step - 1, part],
            self.recv.at[way, step - 1, part],
            "sp",
            self.targets[way],
        )

    def start(self, step, way, part):
        self.copy(step, way, part).start()
        self.started.append((step, way, part))

    def begin(self, part):
        for way in range(2):
            if self.last > 1 or part == way:
                self.start(1, way, part)

    def advance(self):
        step, part = self.events[self.done]
        self.done += 1
        for way in range(2):
            held = way if part is None else part
            self.copy(step, way, held).wait_recv()
            if step < self.last and (step + 1 < self.last or held == way):
                self.start(step + 1, way, held)

    def ready(self, step):
        target = len(self.events) if step == self.last else 2 * step
        while self.done < target:
            self.advance()
        return [self.owner(step)] if step == self.last else [self.owner(step), self.owner(-step)]

    def sent(self):
        for step, way, part in self.started:
            self.copy(step, way, part).wait_send()


def layer_kernel(
    count,
    tokens,
    w_pool_in,
    w_query,
    w_key_t,
    w_value_t,
    pool_map,
    w_out,
    gain,
    params,
    out,
    normed,
    first_weights,
    last_weights,
    acc,
    queries,
    keys_low,
    keys_high,
    values_low,
    values_high,
    pool_span,
    pairs,
    mixed,
    bias,
    band,
    ones_block,
    halo_pairs,
    halo_pool,
    recv_near,
    send_far,
    recv_far,
    local_sem,
    first_send,
    first_recv,
    last_send,
    last_recv,
    near_sem,
    far_sem,
    pass_sem,
    halo_sem,
    sum_near_sem,
    sum_far_sem,
):
    me, partner, other = partners()
    across = (partner + 2) % 4
    seq = lax.axis_index("sp")
    rows, width = tokens.shape
    depth, branch = w_pool_in.shape
    head_columns = w_query.shape[1]
    mid = branch + head_columns
    piece = rows // TOKEN_CHUNKS
    blocks = rows // WINDOW
    out_rows = out.shape[0]
    out_width = w_out.shape[1]
    mix = w_out.shape[0]
    pairs_of_heads = head_columns // LANES

    def first_block(owner, part):
        return first_weights.at[
            pl.ds(pl.multiple_of(owner * depth + part * (depth // 2), depth // 2), depth // 2)
        ]

    def last_block(owner, part):
        return last_weights.at[owner, pl.ds(part * (mix // 2), mix // 2)]

    first_ring = Ring(count, first_block, first_send, first_recv)
    last_ring = Ring(count, last_block, last_send, last_recv)
    following = (seq + 1) % count
    preceding = (seq + count - 1) % count

    def columns(owner):
        return aligned(owner, width)

    own_rows = aligned(seq, depth)
    local = [
        pltpu.make_async_copy(source, target, local_sem.at[index])
        for index, (source, target) in enumerate(
            [
                (w_pool_in, first_weights.at[own_rows, pl.ds(0, branch)]),
                (w_query, first_weights.at[own_rows, pl.ds(branch, head_columns)]),
                (tokens, normed.at[:, columns(me)]),
                (w_out, last_weights.at[seq]),
            ]
        )
    ]
    for copy in local:
        copy.start()
    key_value = jnp.concatenate([w_key_t[...], w_value_t[...]], axis=0).astype(f32)
    first_weights[own_rows, pl.ds(mid, LANES)] = key_value.T.astype(bf16)
    greet(
        [
            ("sp", first_ring.targets[0]),
            ("sp", first_ring.targets[1]),
            ("sp", following),
            ("sp", preceding),
            ("tp", partner),
            ("tp", other),
        ]
    )
    local[0].wait()
    local[1].wait()
    first_ring.begin(0)
    first_ring.begin(1)

    def far_copy(chunk):
        return remote(
            tokens.at[pl.ds(chunk * piece, piece)],
            normed.at[pl.ds(chunk * piece, piece), columns(me)],
            far_sem.at[0, chunk],
            far_sem.at[1, chunk],
            "tp",
            other,
        )

    def near_copy():
        return remote(
            tokens, normed.at[:, columns(me)], near_sem.at[0], near_sem.at[1], "tp", partner
        )

    def pass_copy(chunk):
        held = normed.at[pl.ds(chunk * piece, piece), columns(other)]
        return remote(held, held, pass_sem.at[0, chunk], pass_sem.at[1, chunk], "tp", partner)

    for chunk in range(TOKEN_CHUNKS):
        far_copy(chunk).start()
    near_copy().start()

    span = 2.0 * jnp.exp2(me.astype(f32))
    row = lax.broadcasted_iota(jnp.int32, (WINDOW, 2 * WINDOW), 0)
    column = lax.broadcasted_iota(jnp.int32, (WINDOW, 2 * WINDOW), 1)
    distance = (row + WINDOW - column).astype(f32)
    band[...] = jnp.where((distance >= 0.0) & (distance < span), 1.0, 0.0).astype(bf16)
    allowed = (distance >= 0.0) & (distance < float(WINDOW))
    for pair in range(pairs_of_heads):
        for half in range(2):
            head = (me * GROUP + 2 * pair + half + 1).astype(f32)
            slope = jnp.exp2(jnp.full((WINDOW, 2 * WINDOW), -8.0 / Q_HEADS, f32) * head)
            bias[pl.ds(pair * WINDOW, WINDOW), pl.ds(half * 2 * WINDOW, 2 * WINDOW)] = jnp.where(
                allowed, -slope * distance, MASKED
            )
    block_row = lax.broadcasted_iota(jnp.int32, (2 * LANES, 2 * LANES), 0) // HEAD_DIM
    block_column = lax.broadcasted_iota(jnp.int32, (2 * LANES, 2 * LANES), 1) // HEAD_DIM
    ones_block[...] = jnp.where(block_row == block_column, 1.0, 0.0).astype(bf16)
    pool_span[pl.ds(0, WINDOW)] = jnp.zeros((WINDOW, branch), bf16)

    strip = 32

    def normalise(chunk):
        @pl.loop(0, piece // strip)
        def _(index):
            held = pl.ds(pl.multiple_of(chunk * piece + index * strip, strip), strip)
            values = normed[held].astype(f32)
            scale = lax.rsqrt(jnp.mean(values * values, axis=-1, keepdims=True) + epsilon)
            normed[held] = (values * scale * gain[...]).astype(bf16)

    local[2].wait()
    for chunk in range(TOKEN_CHUNKS):
        far_copy(chunk).wait_recv()
        pass_copy(chunk).start()
        if chunk == 0:
            near_copy().wait()
        first_ring_events = len(first_ring.events)
        if chunk < first_ring_events - 1:
            first_ring.advance()
        pass_copy(chunk).wait()
        normalise(chunk)
    for chunk in range(TOKEN_CHUNKS):
        far_copy(chunk).wait_send()

    tile = rows // 4

    def term_of(index, owner):
        return dot(normed[aligned(index, tile), aligned(owner, depth)], first_weights[aligned(owner, depth), :])

    def multiply(owners, fresh):
        @pl.loop(0, rows // tile)
        def _(index):
            total = term_of(index, owners[0])
            for owner in owners[1:]:
                total += term_of(index, owner)
            held = aligned(index, tile)
            acc[held] = total if fresh else acc[held] + total

    multiply([first_ring.owner(0)], True)
    for step in range(1, first_ring.last):
        owners = first_ring.ready(step)
        if step == first_ring.last - 1:
            local[3].wait()
            last_ring.begin(0)
        multiply(owners, False)
    if first_ring.last == 1:
        local[3].wait()
        last_ring.begin(0)
    final_owner = first_ring.ready(first_ring.last)[0]

    lane = lax.broadcasted_iota(jnp.int32, (1, LANES), 1)
    low = lane < HEAD_DIM
    query_gain = params[0:1, :]
    sink = jnp.exp(params[1:2, :])
    pool_scale = params[2:3, :]
    pair_gain = params[3:4, :LANES]
    one_low = jnp.where(low, 1.0, 0.0)

    def spread(kv, held, count_scale):
        size = kv.shape[0]
        key_low = jnp.where(low, kv, 0.0)
        value_high = jnp.where(low, 0.0, kv)
        keys_low[held] = key_low.astype(bf16)
        keys_high[held] = pltpu.roll(key_low, HEAD_DIM, 1).astype(bf16)
        ones_low = jnp.broadcast_to(one_low * count_scale, (size, LANES)).astype(bf16)
        ones_high = jnp.broadcast_to((1.0 - one_low) * count_scale, (size, LANES)).astype(bf16)
        values_low[held, pl.ds(0, LANES)] = pltpu.roll(value_high, HEAD_DIM, 1).astype(bf16)
        values_low[held, pl.ds(LANES, LANES)] = ones_low
        values_high[held, pl.ds(0, LANES)] = value_high.astype(bf16)
        values_high[held, pl.ds(LANES, LANES)] = ones_high

    def finalise(index):
        held = aligned(index, tile)
        sums = (acc[held] + term_of(index, final_owner)).astype(bf16)
        shifted = pl.ds(pl.multiple_of(index * tile + WINDOW, WINDOW), tile)
        pool_span[shifted] = sums[:, :branch]
        kv = sums[:, mid:].astype(f32)
        squares = jnp.where(low, kv * kv, 0.0)
        scale = lax.rsqrt(jnp.sum(squares, axis=-1, keepdims=True) * (1.0 / HEAD_DIM) + epsilon)
        kv = jnp.where(low, kv * scale * pair_gain, kv).astype(bf16)
        pairs[held] = kv
        spread(kv.astype(f32), shifted, 1.0)
        wide = 2 * LANES
        for start in range(0, head_columns, wide):
            query = sums[:, branch + start : branch + start + wide].astype(f32)
            square = query * query
            upper = square.astype(bf16)
            lower = (square - upper.astype(f32)).astype(bf16)
            total = dot(upper, ones_block[...]) + dot(lower, ones_block[...])
            scale = lax.rsqrt(total * (1.0 / HEAD_DIM) + epsilon)
            queries[held, pl.ds(start, wide)] = (
                query * scale * query_gain[:, start : start + wide]
            ).astype(bf16)

    def halo_copies():
        return [
            remote(
                pairs.at[pl.ds(rows - WINDOW, WINDOW)],
                halo_pairs,
                halo_sem.at[0, 0],
                halo_sem.at[1, 0],
                "sp",
                following,
            ),
            remote(
                pool_span.at[pl.ds(WINDOW + rows - HALO_ROWS, HALO_ROWS)],
                halo_pool,
                halo_sem.at[0, 1],
                halo_sem.at[1, 1],
                "sp",
                following,
            ),
        ]

    finalise(rows // tile - 1)
    for copy in halo_copies():
        copy.start()
    last_ring.begin(1)

    @pl.loop(0, rows // tile - 1)
    def _(index):
        finalise(index)

    def pool(block):
        held = aligned(block, WINDOW)
        span_rows = pool_span[pl.ds(pl.multiple_of(block * WINDOW, WINDOW), 2 * WINDOW)]
        running = dot(band[...], span_rows)
        offset = lax.broadcasted_iota(jnp.int32, (WINDOW, 1), 0)
        position = (seq * rows + block * WINDOW + offset).astype(f32)
        counted = jnp.minimum(position + 1.0, span)
        difference = (running / counted - span_rows[WINDOW:].astype(f32)).astype(bf16)
        mapped = dot(difference, pool_map[...]) * pool_scale
        scale = lax.rsqrt(jnp.mean(mapped * mapped, axis=-1, keepdims=True) + epsilon)
        mixed[held, pl.ds(0, branch)] = (mapped * scale).astype(bf16)

    def attend(block):
        held = aligned(block, WINDOW)
        both = pl.ds(pl.multiple_of(block * WINDOW, WINDOW), 2 * WINDOW)
        key_pair = jnp.concatenate([keys_low[both], keys_high[both]], axis=0)
        value_pair = jnp.concatenate([values_low[both], values_high[both]], axis=0)
        parts, squares = [], None
        for pair in range(pairs_of_heads):
            lanes = pl.ds(pair * LANES, LANES)
            scores = lax.dot_general(
                queries[held, lanes],
                key_pair,
                (((1,), (1,)), ((), ())),
                preferred_element_type=f32,
            )
            weights = jnp.exp(scores + bias[pl.ds(pair * WINDOW, WINDOW)]).astype(bf16)
            result = dot(weights, value_pair)
            part = result[:, :LANES] / (
                result[:, LANES:] + sink[:, pair * LANES : (pair + 1) * LANES]
            )
            parts.append(part)
            squares = part * part if squares is None else squares + part * part
        mean = jnp.sum(squares, axis=-1, keepdims=True) * (1.0 / head_columns)
        scale = lax.rsqrt(mean + epsilon)
        for pair, part in enumerate(parts):
            mixed[held, pl.ds(branch + pair * LANES, LANES)] = (part * scale).astype(bf16)

    half = (blocks + 1) // 2

    @pl.loop(1, half + 1)
    def _(block):
        pool(block)
        attend(block)

    if len(last_ring.events) > 2:
        last_ring.advance()

    @pl.loop(half + 1, blocks)
    def _(block):
        pool(block)
        attend(block)

    for copy in halo_copies():
        copy.wait()
    begun = jnp.where(seq > 0, 1.0, 0.0)
    top = pl.ds(0, WINDOW)
    spread(halo_pairs[...].astype(f32) * begun, top, begun)
    pool_span[pl.ds(WINDOW - HALO_ROWS, HALO_ROWS)] = (halo_pool[...].astype(f32) * begun).astype(
        bf16
    )
    pool(0)
    attend(0)

    def output_columns(owner):
        return aligned(owner, out_width)

    def term_at(group, chunk):
        return (
            pl.ds(pl.multiple_of(group * out_rows, out_rows), out_rows),
            pl.ds(chunk * out_width, out_width),
        )

    def sum_near(chunk):
        return remote(
            normed.at[pl.ds(0, 2 * out_rows), pl.ds(chunk * out_width, out_width)],
            recv_near.at[chunk],
            sum_near_sem.at[0, chunk],
            sum_near_sem.at[1, chunk],
            "tp",
            partner,
        )

    def sum_far(chunk):
        return remote(
            send_far.at[chunk],
            recv_far.at[chunk],
            sum_far_sem.at[0, chunk],
            sum_far_sem.at[1, chunk],
            "tp",
            other,
        )

    def first(chunk, owner):
        def term(group):
            held = aligned(group, out_rows)
            return dot(mixed[held, :], last_weights[owner]).astype(bf16)

        @pl.loop(0, 2)
        def _(pick):
            normed[term_at(pick, chunk)] = term(jnp.where(pick == 0, across, partner))

        sum_near(chunk).start()

        @pl.loop(0, 2)
        def _(pick):
            normed[term_at(pick + 2, chunk)] = term(jnp.where(pick == 0, other, me))

    def second(chunk):
        sum_near(chunk).wait_recv()
        send_far[chunk] = (
            normed[term_at(2, chunk)].astype(f32) + recv_near[chunk, :out_rows].astype(f32)
        ).astype(bf16)
        sum_far(chunk).start()

    def third(chunk, owner):
        sum_far(chunk).wait_recv()
        out[:, output_columns(owner)] = (
            normed[term_at(3, chunk)].astype(f32)
            + recv_near[chunk, out_rows:].astype(f32)
            + recv_far[chunk].astype(f32)
        ).astype(bf16)

    owners = [last_ring.owner(0)]
    first(0, owners[0])
    second(0)
    finished = 0
    for step in range(1, last_ring.last + 1):
        fresh = last_ring.ready(step)
        start = len(owners)
        for extra, owner in enumerate(fresh):
            first(start + extra, owner)
        for extra in range(len(fresh)):
            second(start + extra)
        while finished < start:
            third(finished, owners[finished])
            finished += 1
        owners += fresh
    while finished < count:
        third(finished, owners[finished])
        finished += 1
    first_ring.sent()
    last_ring.sent()
    for chunk in range(count):
        sum_near(chunk).wait_send()
        sum_far(chunk).wait_send()


def layer(tokens, w_pool_in, w_query, w_key_t, w_value_t, pool_map, w_out, gain, params):
    count = lax.axis_size("sp")
    rows, width = tokens.shape
    depth, branch = w_pool_in.shape
    head_columns = w_query.shape[1]
    features = width * lax.axis_size("tp")
    mix, out_width = w_out.shape
    out_rows = rows // lax.axis_size("tp")
    dma = pltpu.SemaphoreType.DMA
    last = count // 2
    vmem = pl.BlockSpec(memory_space=pltpu.VMEM)
    hbm = pl.BlockSpec(memory_space=pltpu.HBM)
    flops = 2 * rows * features * (branch + head_columns + LANES) + 2 * rows * mix * count * out_width
    return pl.pallas_call(
        functools.partial(layer_kernel, count),
        out_shape=jax.ShapeDtypeStruct((out_rows, count * out_width), bf16),
        in_specs=[hbm, hbm, hbm, vmem, vmem, vmem, hbm, vmem, vmem],
        out_specs=vmem,
        scratch_shapes=[
            pltpu.VMEM((rows, features), bf16),
            pltpu.VMEM((features, branch + head_columns + LANES), bf16),
            pltpu.VMEM((count, mix, out_width), bf16),
            pltpu.VMEM((rows, branch + head_columns + LANES), f32),
            pltpu.VMEM((rows, head_columns), bf16),
            pltpu.VMEM((WINDOW + rows, LANES), bf16),
            pltpu.VMEM((WINDOW + rows, LANES), bf16),
            pltpu.VMEM((WINDOW + rows, 2 * LANES), bf16),
            pltpu.VMEM((WINDOW + rows, 2 * LANES), bf16),
            pltpu.VMEM((WINDOW + rows, branch), bf16),
            pltpu.VMEM((rows, LANES), bf16),
            pltpu.VMEM((rows, mix), bf16),
            pltpu.VMEM((head_columns // LANES * WINDOW, 4 * WINDOW), f32),
            pltpu.VMEM((WINDOW, 2 * WINDOW), bf16),
            pltpu.VMEM((2 * LANES, 2 * LANES), bf16),
            pltpu.VMEM((WINDOW, LANES), bf16),
            pltpu.VMEM((HALO_ROWS, branch), bf16),
            pltpu.VMEM((count, 2 * out_rows, out_width), bf16),
            pltpu.VMEM((count, out_rows, out_width), bf16),
            pltpu.VMEM((count, out_rows, out_width), bf16),
            dma((4,)),
            dma((2, last, 2)),
            dma((2, last, 2)),
            dma((2, last, 2)),
            dma((2, last, 2)),
            dma((2,)),
            dma((2, TOKEN_CHUNKS)),
            dma((2, TOKEN_CHUNKS)),
            dma((2, 2)),
            dma((2, count)),
            dma((2, count)),
        ],
        compiler_params=pltpu.CompilerParams(
            collective_id=0, has_side_effects=True, vmem_limit_bytes=63 * 1024 * 1024
        ),
        cost_estimate=pl.CostEstimate(
            flops=flops, bytes_accessed=4 * rows * width, transcendentals=0
        ),
    )(tokens, w_pool_in, w_query, w_key_t, w_value_t, pool_map, w_out, gain, params)


def local(
    tokens,
    norm_gain,
    w_pool_in,
    w_query,
    w_key,
    w_value,
    pool_map,
    pool_scale,
    q_gain,
    k_gain,
    sinks,
    w_out,
):
    head_columns = w_query.shape[1]
    params = jnp.stack(
        [
            jnp.tile(q_gain * HEAD_DIM**-0.5, head_columns // HEAD_DIM),
            jnp.repeat(sinks, HEAD_DIM),
            pool_scale,
            jnp.tile(k_gain, head_columns // HEAD_DIM),
        ]
    )
    return layer(
        tokens,
        w_pool_in,
        w_query,
        w_key.T,
        w_value.T,
        pool_map[0],
        w_out,
        norm_gain[None],
        params,
    )


def solution(mesh):
    in_specs = (
        P("sp", "tp"),
        P(),
        P("sp", "tp"),
        P("sp", "tp"),
        P("sp", "tp"),
        P("sp", "tp"),
        P("tp", None, None),
        P("tp"),
        P(),
        P(),
        P("tp"),
        P("tp", "sp"),
    )
    out_specs = P(("sp", "tp"), None)
    return jax.shard_map(local, mesh=mesh, in_specs=in_specs, out_specs=out_specs, check_vma=False)
```

```python
import functools

import jax
import jax.numpy as jnp
from jax import lax
from jax.experimental import pallas as pl
from jax.experimental.pallas import tpu as pltpu
from jax.sharding import PartitionSpec as P

HEAD_DIM = 64
GROUP = 8
WINDOW = 128
Q_HEADS = 32
LANES = 128
TOKEN_CHUNKS = 4
HALO_ROWS = 16
MASKED = -1e30

epsilon = 1e-06
bf16, f32 = jnp.bfloat16, jnp.float32


def ring_place(device, count):
    return jnp.where(device % 2 == 0, device // 2, count - 1 - device // 2)


def ring_device(place, count):
    place = (place + count) % count
    return jnp.where(place < count // 2, 2 * place, 2 * (count - 1 - place) + 1)


def partners():
    me = lax.axis_index("tp")
    return me, me + 1 - 2 * (me % 2), (me + 2) % 4


def greet(targets):
    barrier = pltpu.get_barrier_semaphore()
    for axis, target in targets:
        pl.semaphore_signal(
            barrier, inc=1, device_id={axis: target}, device_id_type=pl.DeviceIdType.MESH
        )


def await_greetings(count):
    pl.semaphore_wait(pltpu.get_barrier_semaphore(), count)


def remote(source, target, send_sem, recv_sem, axis, device):
    return pltpu.make_async_remote_copy(
        src_ref=source,
        dst_ref=target,
        send_sem=send_sem,
        recv_sem=recv_sem,
        device_id={axis: device},
        device_id_type=pl.DeviceIdType.MESH,
    )


def aligned(index, size):
    return pl.ds(pl.multiple_of(index * size, size), size)


def dot(left, right):
    return jnp.dot(left, right, preferred_element_type=f32)


class Ring:
    def __init__(self, count, block_at, send, recv, pieces):
        self.count, self.last, self.pieces = count, count // 2, pieces
        self.place = ring_place(lax.axis_index("sp"), count)
        self.targets = (
            ring_device(self.place + 1, count),
            ring_device(self.place - 1, count),
        )
        self.block_at, self.send, self.recv = block_at, send, recv
        self.started = []
        self.events = [(step, part) for step in range(1, self.last) for part in range(2)]
        self.events += [(self.last, piece) for piece in range(pieces)]
        self.done = 0

    def owner(self, distance):
        return ring_device(self.place - distance, self.count)

    def copy(self, step, way, slot):
        owner = self.owner((1 - 2 * way) * (step - 1))
        if step < self.last:
            block = self.block_at(owner, slot, 0, 1)
        else:
            block = self.block_at(owner, way, slot, self.pieces)
        return remote(
            block,
            block,
            self.send.at[way, step - 1, slot],
            self.recv.at[way, step - 1, slot],
            "sp",
            self.targets[way],
        )

    def start(self, step, way, part):
        if step < self.last:
            slots = [part]
        else:
            slots = range(self.pieces) if part == way else []
        for slot in slots:
            self.copy(step, way, slot).start()
            self.started.append((step, way, slot))

    def begin(self, part):
        for way in range(2):
            self.start(1, way, part)

    def advance(self):
        step, slot = self.events[self.done]
        self.done += 1
        for way in range(2):
            self.copy(step, way, slot).wait_recv()
            if step < self.last:
                self.start(step + 1, way, slot)

    def upto(self, event):
        while self.done <= event:
            self.advance()

    def sent(self):
        for step, way, slot in self.started:
            self.copy(step, way, slot).wait_send()


def layer_kernel(
    count,
    tokens,
    w_pool_in,
    w_query,
    w_key_t,
    w_value_t,
    pool_map,
    w_out,
    gain_in,
    pool_scale_in,
    q_gain_in,
    k_gain_in,
    sinks_in,
    out,
    normed,
    first_weights,
    last_weights,
    acc,
    queries,
    keys_low,
    keys_high,
    values_low,
    values_high,
    pool_span,
    pairs,
    mixed,
    bias,
    band,
    ones_block,
    halo_pairs,
    halo_pool,
    recv_near,
    send_far,
    recv_far,
    key_value,
    pool_maps,
    gain,
    pool_scales,
    q_gain,
    k_gain,
    sinks,
    head_rows,
    local_sem,
    first_send,
    first_recv,
    last_send,
    last_recv,
    near_sem,
    far_sem,
    pass_sem,
    halo_sem,
    sum_near_sem,
    sum_far_sem,
):
    me, partner, other = partners()
    across = (partner + 2) % 4
    seq = lax.axis_index("sp")
    rows, width = tokens.shape
    depth, branch = w_pool_in.shape
    head_columns = w_query.shape[1]
    mid = branch + head_columns
    piece = rows // TOKEN_CHUNKS
    blocks = rows // WINDOW
    out_rows = out.shape[0]
    out_width = w_out.shape[1]
    mix = w_out.shape[0]
    pairs_of_heads = head_columns // LANES

    halves = out_width % (2 * LANES) == 0
    pieces = 2 if out_width % (4 * LANES) == 0 else 1

    def first_block(owner, part, piece, pieces):
        size = depth // 2 // pieces
        return first_weights.at[
            pl.ds(pl.multiple_of(owner * depth + part * (depth // 2) + piece * size, size), size)
        ]

    def last_block(owner, part, piece, pieces):
        if halves:
            size = out_width // 2 // pieces
            return last_weights.at[
                owner, :, pl.ds(part * (out_width // 2) + piece * size, size)
            ]
        size = mix // 2 // pieces
        return last_weights.at[owner, pl.ds(part * (mix // 2) + piece * size, size)]

    first_ring = Ring(count, first_block, first_send, first_recv, 1)
    last_ring = Ring(count, last_block, last_send, last_recv, pieces)
    following = (seq + 1) % count

    def columns(owner):
        return aligned(owner, width)

    own_rows = aligned(seq, depth)
    greetings = [
        ("sp", first_ring.targets[0]),
        ("sp", first_ring.targets[1]),
        ("tp", partner),
        ("tp", other),
    ]
    greet(greetings)
    local = [
        pltpu.make_async_copy(source, target, local_sem.at[index])
        for index, (source, target) in enumerate(
            [
                (w_key_t, key_value.at[pl.ds(0, HEAD_DIM)]),
                (w_value_t, key_value.at[pl.ds(HEAD_DIM, HEAD_DIM)]),
                (w_pool_in, first_weights.at[own_rows, pl.ds(0, branch)]),
                (w_query, first_weights.at[own_rows, pl.ds(branch, head_columns)]),
                (tokens, normed.at[:, columns(me)]),
                (w_out, last_weights.at[seq]),
                (pool_map, pool_maps),
                (gain_in, gain),
                (pool_scale_in, pool_scales),
                (q_gain_in, q_gain),
                (k_gain_in, k_gain),
                (sinks_in, sinks),
            ]
        )
    ]
    for copy in local:
        copy.start()
    local[0].wait()
    local[1].wait()
    first_weights[own_rows, pl.ds(mid, LANES)] = key_value[...].astype(f32).T.astype(bf16)
    await_greetings(len(greetings))
    local[2].wait()
    local[3].wait()
    first_ring.begin(0)
    first_ring.begin(1)

    def far_copy(chunk):
        return remote(
            tokens.at[pl.ds(chunk * piece, piece)],
            normed.at[pl.ds(chunk * piece, piece), columns(me)],
            far_sem.at[0, chunk],
            far_sem.at[1, chunk],
            "tp",
            other,
        )

    def near_copy():
        return remote(
            tokens, normed.at[:, columns(me)], near_sem.at[0], near_sem.at[1], "tp", partner
        )

    def pass_copy(chunk):
        held = normed.at[pl.ds(chunk * piece, piece), columns(other)]
        return remote(held, held, pass_sem.at[0, chunk], pass_sem.at[1, chunk], "tp", partner)

    for chunk in range(TOKEN_CHUNKS):
        far_copy(chunk).start()
    near_copy().start()

    span = 2.0 * jnp.exp2(me.astype(f32))
    row = lax.broadcasted_iota(jnp.int32, (WINDOW, 2 * WINDOW), 0)
    column = lax.broadcasted_iota(jnp.int32, (WINDOW, 2 * WINDOW), 1)
    distance = (row + WINDOW - column).astype(f32)
    band[...] = jnp.where((distance >= 0.0) & (distance < span), 1.0, 0.0).astype(bf16)
    allowed = (distance >= 0.0) & (distance < float(WINDOW))
    for pair in range(pairs_of_heads):
        for half in range(2):
            head = (me * GROUP + 2 * pair + half + 1).astype(f32)
            slope = jnp.exp2(jnp.full((WINDOW, 2 * WINDOW), -8.0 / Q_HEADS, f32) * head)
            bias[pl.ds(pair * WINDOW, WINDOW), pl.ds(half * 2 * WINDOW, 2 * WINDOW)] = jnp.where(
                allowed, -slope * distance, MASKED
            )
    block_row = lax.broadcasted_iota(jnp.int32, (2 * LANES, 2 * LANES), 0) // HEAD_DIM
    block_column = lax.broadcasted_iota(jnp.int32, (2 * LANES, 2 * LANES), 1) // HEAD_DIM
    ones_block[...] = jnp.where(block_row == block_column, 1.0, 0.0).astype(bf16)
    pool_span[pl.ds(0, WINDOW)] = jnp.zeros((WINDOW, branch), bf16)

    strip = 32

    def normalise(chunk):
        @pl.loop(0, piece // strip)
        def _(index):
            held = pl.ds(pl.multiple_of(chunk * piece + index * strip, strip), strip)
            values = normed[held].astype(f32)
            scale = lax.rsqrt(jnp.mean(values * values, axis=-1, keepdims=True) + epsilon)
            normed[held] = (values * scale * gain[...]).astype(bf16)

    lane = lax.broadcasted_iota(jnp.int32, (1, LANES), 1)
    low = lane < HEAD_DIM
    for copy in local[4:]:
        copy.wait()
    head_rows[...] = jnp.zeros(head_rows.shape, f32)
    head_rows[pl.ds(0, 1), pl.ds(0, HEAD_DIM)] = q_gain[...] * HEAD_DIM**-0.5
    head_rows[pl.ds(1, 1), pl.ds(0, HEAD_DIM)] = k_gain[...]
    once = head_rows[pl.ds(0, 1), :]
    head_rows[pl.ds(0, 1), :] = once + pltpu.roll(once, HEAD_DIM, 1)
    for pair in range(pairs_of_heads):
        head_rows[pl.ds(2 + pair, 1), :] = jnp.exp(
            jnp.where(low, sinks[2 * pair], sinks[2 * pair + 1])
        )

    for chunk in range(TOKEN_CHUNKS):
        far_copy(chunk).wait_recv()
        pass_copy(chunk).start()
        if chunk == 0:
            near_copy().wait()
        first_ring_events = len(first_ring.events)
        if chunk < first_ring_events - 1:
            first_ring.advance()
        pass_copy(chunk).wait()
        normalise(chunk)
    for chunk in range(TOKEN_CHUNKS):
        far_copy(chunk).wait_send()

    tile = rows // 4

    def term_of(index, owner):
        return dot(normed[aligned(index, tile), aligned(owner, depth)], first_weights[aligned(owner, depth), :])

    def multiply(owners, fresh):
        @pl.loop(0, rows // tile)
        def _(index):
            total = term_of(index, owners[0])
            for owner in owners[1:]:
                total += term_of(index, owner)
            held = aligned(index, tile)
            acc[held] = total if fresh else acc[held] + total

    multiply([first_ring.owner(0)], True)
    for step in range(1, first_ring.last):
        first_ring.upto(2 * step - 1)
        if step == first_ring.last - 1:
            last_ring.begin(0)
        multiply([first_ring.owner(step), first_ring.owner(-step)], False)
    if first_ring.last == 1:
        last_ring.begin(0)
    first_ring.upto(len(first_ring.events) - 1)
    final_owner = first_ring.owner(first_ring.last)

    one_low = jnp.where(low, 1.0, 0.0)

    def spread(kv, held, count_scale):
        size = kv.shape[0]
        key_low = jnp.where(low, kv, 0.0)
        value_high = jnp.where(low, 0.0, kv)
        keys_low[held] = key_low.astype(bf16)
        keys_high[held] = pltpu.roll(key_low, HEAD_DIM, 1).astype(bf16)
        ones_low = jnp.broadcast_to(one_low * count_scale, (size, LANES)).astype(bf16)
        ones_high = jnp.broadcast_to((1.0 - one_low) * count_scale, (size, LANES)).astype(bf16)
        values_low[held, pl.ds(0, LANES)] = pltpu.roll(value_high, HEAD_DIM, 1).astype(bf16)
        values_low[held, pl.ds(LANES, LANES)] = ones_low
        values_high[held, pl.ds(0, LANES)] = value_high.astype(bf16)
        values_high[held, pl.ds(LANES, LANES)] = ones_high

    def finalise(index):
        held = aligned(index, tile)
        sums = (acc[held] + term_of(index, final_owner)).astype(bf16)
        shifted = pl.ds(pl.multiple_of(index * tile + WINDOW, WINDOW), tile)
        pool_span[shifted] = sums[:, :branch]
        kv = sums[:, mid:].astype(f32)
        squares = jnp.where(low, kv * kv, 0.0)
        scale = lax.rsqrt(jnp.sum(squares, axis=-1, keepdims=True) * (1.0 / HEAD_DIM) + epsilon)
        kv = jnp.where(low, kv * scale * head_rows[pl.ds(1, 1), :], kv).astype(bf16)
        pairs[held] = kv
        spread(kv.astype(f32), shifted, 1.0)
        wide = 2 * LANES
        gain_row = head_rows[pl.ds(0, 1), :]
        query_gain = jnp.concatenate([gain_row, gain_row], axis=1)
        for start in range(0, head_columns, wide):
            query = sums[:, branch + start : branch + start + wide].astype(f32)
            square = query * query
            upper = square.astype(bf16)
            lower = (square - upper.astype(f32)).astype(bf16)
            total = dot(upper, ones_block[...]) + dot(lower, ones_block[...])
            scale = lax.rsqrt(total * (1.0 / HEAD_DIM) + epsilon)
            queries[held, pl.ds(start, wide)] = (
                query * scale * query_gain
            ).astype(bf16)

    def halo_copies():
        return [
            remote(
                pairs.at[pl.ds(rows - WINDOW, WINDOW)],
                halo_pairs,
                halo_sem.at[0, 0],
                halo_sem.at[1, 0],
                "sp",
                following,
            ),
            remote(
                pool_span.at[pl.ds(WINDOW + rows - HALO_ROWS, HALO_ROWS)],
                halo_pool,
                halo_sem.at[0, 1],
                halo_sem.at[1, 1],
                "sp",
                following,
            ),
        ]

    finalise(rows // tile - 1)
    for copy in halo_copies():
        copy.start()
    last_ring.begin(1)

    @pl.loop(0, rows // tile - 1)
    def _(index):
        finalise(index)

    def pool(block):
        held = aligned(block, WINDOW)
        span_rows = pool_span[pl.ds(pl.multiple_of(block * WINDOW, WINDOW), 2 * WINDOW)]
        running = dot(band[...], span_rows)
        offset = lax.broadcasted_iota(jnp.int32, (WINDOW, 1), 0)
        position = (seq * rows + block * WINDOW + offset).astype(f32)
        counted = jnp.minimum(position + 1.0, span)
        difference = (running / counted - span_rows[WINDOW:].astype(f32)).astype(bf16)
        mapped = dot(difference, pool_maps[...]) * pool_scales[...]
        scale = lax.rsqrt(jnp.mean(mapped * mapped, axis=-1, keepdims=True) + epsilon)
        mixed[held, pl.ds(0, branch)] = (mapped * scale).astype(bf16)

    def attend(block):
        held = aligned(block, WINDOW)
        both = pl.ds(pl.multiple_of(block * WINDOW, WINDOW), 2 * WINDOW)
        key_pair = jnp.concatenate([keys_low[both], keys_high[both]], axis=0)
        value_pair = jnp.concatenate([values_low[both], values_high[both]], axis=0)
        parts, squares = [], None
        for pair in range(pairs_of_heads):
            lanes = pl.ds(pair * LANES, LANES)
            scores = lax.dot_general(
                queries[held, lanes],
                key_pair,
                (((1,), (1,)), ((), ())),
                preferred_element_type=f32,
            )
            weights = jnp.exp(scores + bias[pl.ds(pair * WINDOW, WINDOW)]).astype(bf16)
            result = dot(weights, value_pair)
            part = result[:, :LANES] / (
                result[:, LANES:] + head_rows[pl.ds(2 + pair, 1), :]
            )
            parts.append(part)
            squares = part * part if squares is None else squares + part * part
        mean = jnp.sum(squares, axis=-1, keepdims=True) * (1.0 / head_columns)
        scale = lax.rsqrt(mean + epsilon)
        for pair, part in enumerate(parts):
            mixed[held, pl.ds(branch + pair * LANES, LANES)] = (part * scale).astype(bf16)

    half = (blocks + 1) // 2

    @pl.loop(1, half + 1)
    def _(block):
        pool(block)
        attend(block)

    if len(last_ring.events) > 2:
        last_ring.upto(0)

    @pl.loop(half + 1, blocks)
    def _(block):
        pool(block)
        attend(block)

    for copy in halo_copies():
        copy.wait()
    begun = jnp.where(seq > 0, 1.0, 0.0)
    top = pl.ds(0, WINDOW)
    spread(halo_pairs[...].astype(f32) * begun, top, begun)
    pool_span[pl.ds(WINDOW - HALO_ROWS, HALO_ROWS)] = (halo_pool[...].astype(f32) * begun).astype(
        bf16
    )
    pool(0)
    attend(0)

    half_width = out_width // 2
    size_of = half_width if halves else out_width
    batches = []
    if halves:
        batches.append((-1, 2, size_of, lambda unit: (last_ring.owner(0), unit * half_width)))
    else:
        batches.append((-1, 1, size_of, lambda unit: (last_ring.owner(0), 0)))
    for event, (step, slot) in enumerate(last_ring.events):
        final = step == last_ring.last
        if not halves:
            if slot < (pieces if final else 2) - 1:
                continue
            if final:
                batches.append((event, 1, size_of, lambda unit: (last_ring.owner(last_ring.last), 0)))
            else:
                batches.append(
                    (
                        event,
                        2,
                        size_of,
                        lambda unit, step=step: (last_ring.owner((1 - 2 * unit) * step), 0),
                    )
                )
        elif final:
            batches.append(
                (
                    event,
                    2,
                    size_of // pieces,
                    lambda unit, slot=slot: (
                        last_ring.owner(last_ring.last),
                        unit * half_width + slot * (half_width // pieces),
                    ),
                )
            )
        else:
            batches.append(
                (
                    event,
                    2,
                    size_of,
                    lambda unit, step=step, slot=slot: (
                        last_ring.owner((1 - 2 * unit) * step),
                        slot * half_width,
                    ),
                )
            )

    class Batch:
        def __init__(self, first_unit, base, event, units, size, place):
            self.first_unit, self.base, self.event = first_unit, base, event
            self.units, self.size, self.place = units, size, place

        def lanes(self, unit):
            step = min(self.size, LANES)
            return pl.ds(pl.multiple_of(self.base + unit * self.size, step), self.size)

        def group(self, slot):
            return pl.ds(slot * out_rows, out_rows)

        def near(self, unit, pick):
            return remote(
                normed.at[self.group(pick), self.lanes(unit)],
                recv_near.at[self.group(pick), self.lanes(unit)],
                sum_near_sem.at[0, pick, self.first_unit + unit],
                sum_near_sem.at[1, pick, self.first_unit + unit],
                "tp",
                partner,
            )

        def far(self, unit):
            return remote(
                send_far.at[:, self.lanes(unit)],
                recv_far.at[:, self.lanes(unit)],
                sum_far_sem.at[0, self.first_unit + unit],
                sum_far_sem.at[1, self.first_unit + unit],
                "tp",
                other,
            )

        def term(self, unit, slot, target):
            owner, start = self.place(unit)
            if not isinstance(start, int):
                start = pl.multiple_of(start, min(self.size, LANES))
            value = dot(
                mixed[aligned(target, out_rows), :],
                last_weights[owner, :, pl.ds(start, self.size)],
            )
            normed[self.group(slot), self.lanes(unit)] = value.astype(bf16)

        def early(self):
            @pl.loop(0, self.units)
            def _(unit):
                self.term(unit, 0, across)
                self.near(unit, 0).start()
                self.term(unit, 2, other)

        def middle(self):
            @pl.loop(0, self.units)
            def _(unit):
                self.near(unit, 0).wait_recv()
                lanes = self.lanes(unit)
                send_far[:, lanes] = (
                    normed[self.group(2), lanes].astype(f32)
                    + recv_near[self.group(0), lanes].astype(f32)
                ).astype(bf16)
                self.far(unit).start()

        def late(self):
            @pl.loop(0, self.units)
            def _(unit):
                self.term(unit, 1, partner)
                self.near(unit, 1).start()
                self.term(unit, 3, me)

        def finish(self):
            @pl.loop(0, self.units)
            def _(unit):
                self.near(unit, 1).wait_recv()
                self.far(unit).wait_recv()
                lanes = self.lanes(unit)
                owner, start = self.place(unit)
                target = pl.ds(
                    pl.multiple_of(owner * out_width + start, min(self.size, LANES)), self.size
                )
                out[:, target] = (
                    normed[self.group(3), lanes].astype(f32)
                    + recv_near[self.group(1), lanes].astype(f32)
                    + recv_far[:, lanes].astype(f32)
                ).astype(bf16)

        def sent(self):
            @pl.loop(0, self.units)
            def _(unit):
                self.near(unit, 0).wait_send()
                self.near(unit, 1).wait_send()
                self.far(unit).wait_send()

    unit, base, built = 0, 0, []
    for event, units, size, place in batches:
        batch = Batch(unit, base, event, units, size, place)
        last_ring.upto(event)
        batch.early()
        batch.middle()
        batch.late()
        if len(built) > 1:
            built[-2].finish()
        built.append(batch)
        unit, base = unit + units, base + units * size
    for batch in built[-2:]:
        batch.finish()
    first_ring.sent()
    last_ring.sent()
    for batch in built:
        batch.sent()


def layer(tokens, w_pool_in, w_query, w_key_t, w_value_t, pool_map, w_out, *rows_in):
    count = lax.axis_size("sp")
    rows, width = tokens.shape
    depth, branch = w_pool_in.shape
    head_columns = w_query.shape[1]
    features = width * lax.axis_size("tp")
    mix, out_width = w_out.shape
    out_rows = rows // lax.axis_size("tp")
    out_columns = count * out_width
    dma = pltpu.SemaphoreType.DMA
    last = count // 2
    units = 4 * count
    hbm = pl.BlockSpec(memory_space=pltpu.HBM)
    flops = 2 * rows * features * (branch + head_columns + LANES) + 2 * rows * mix * out_columns
    return pl.pallas_call(
        functools.partial(layer_kernel, count),
        out_shape=pltpu.VMEM((out_rows, out_columns), bf16),
        in_specs=[hbm] * 12,
        out_specs=pl.BlockSpec(memory_space=pltpu.VMEM),
        scratch_shapes=[
            pltpu.VMEM((rows, features), bf16),
            pltpu.VMEM((features, branch + head_columns + LANES), bf16),
            pltpu.VMEM((count, mix, out_width), bf16),
            pltpu.VMEM((rows, branch + head_columns + LANES), f32),
            pltpu.VMEM((rows, head_columns), bf16),
            pltpu.VMEM((WINDOW + rows, LANES), bf16),
            pltpu.VMEM((WINDOW + rows, LANES), bf16),
            pltpu.VMEM((WINDOW + rows, 2 * LANES), bf16),
            pltpu.VMEM((WINDOW + rows, 2 * LANES), bf16),
            pltpu.VMEM((WINDOW + rows, branch), bf16),
            pltpu.VMEM((rows, LANES), bf16),
            pltpu.VMEM((rows, mix), bf16),
            pltpu.VMEM((head_columns // LANES * WINDOW, 4 * WINDOW), f32),
            pltpu.VMEM((WINDOW, 2 * WINDOW), bf16),
            pltpu.VMEM((2 * LANES, 2 * LANES), bf16),
            pltpu.VMEM((WINDOW, LANES), bf16),
            pltpu.VMEM((HALO_ROWS, branch), bf16),
            pltpu.VMEM((2 * out_rows, out_columns), bf16),
            pltpu.VMEM((out_rows, out_columns), bf16),
            pltpu.VMEM((out_rows, out_columns), bf16),
            pltpu.VMEM((2 * HEAD_DIM, depth), bf16),
            pltpu.VMEM((branch, branch), bf16),
            pltpu.VMEM((1, features), f32),
            pltpu.VMEM((1, branch), f32),
            pltpu.VMEM((1, HEAD_DIM), f32),
            pltpu.VMEM((1, HEAD_DIM), f32),
            pltpu.SMEM((GROUP,), f32),
            pltpu.VMEM((8, LANES), f32),
            dma((12,)),
            dma((2, last, 2)),
            dma((2, last, 2)),
            dma((2, last, 2)),
            dma((2, last, 2)),
            dma((2,)),
            dma((2, TOKEN_CHUNKS)),
            dma((2, TOKEN_CHUNKS)),
            dma((2, 2)),
            dma((2, 2, units)),
            dma((2, units)),
        ],
        compiler_params=pltpu.CompilerParams(
            collective_id=0, has_side_effects=True, vmem_limit_bytes=58 * 1024 * 1024
        ),
        cost_estimate=pl.CostEstimate(
            flops=flops, bytes_accessed=4 * rows * width, transcendentals=0
        ),
    )(tokens, w_pool_in, w_query, w_key_t, w_value_t, pool_map, w_out, *rows_in)


def local(
    tokens,
    norm_gain,
    w_pool_in,
    w_query,
    w_key,
    w_value,
    pool_map,
    pool_scale,
    q_gain,
    k_gain,
    sinks,
    w_out,
):
    return layer(
        tokens,
        w_pool_in,
        w_query,
        w_key.T,
        w_value.T,
        pool_map[0],
        w_out,
        norm_gain[None],
        pool_scale[None],
        q_gain[None],
        k_gain[None],
        sinks,
    )


def solution(mesh):
    in_specs = (
        P("sp", "tp"),
        P(),
        P("sp", "tp"),
        P("sp", "tp"),
        P("sp", "tp"),
        P("sp", "tp"),
        P("tp", None, None),
        P("tp"),
        P(),
        P(),
        P("tp"),
        P("tp", "sp"),
    )
    out_specs = P(("sp", "tp"), None)
    return jax.shard_map(local, mesh=mesh, in_specs=in_specs, out_specs=out_specs, check_vma=False)
```

```python
import functools

import jax
import jax.numpy as jnp
from jax import lax
from jax.experimental import pallas as pl
from jax.experimental.pallas import tpu as pltpu
from jax.sharding import PartitionSpec as P

HEAD_DIM = 64
GROUP = 8
WINDOW = 128
Q_HEADS = 32
LANES = 128
TOKEN_CHUNKS = 4
HALO_ROWS = 16
MASKED = -1e30

epsilon = 1e-06
bf16, f32 = jnp.bfloat16, jnp.float32


def aligned(index, size):
    return pl.ds(pl.multiple_of(index * size, size), size)


def dot(left, right):
    return jnp.dot(left, right, preferred_element_type=f32)


class Place:
    def __init__(self, count):
        self.planes = count // 2
        self.sp, self.tp = lax.axis_index("sp"), lax.axis_index("tp")
        self.z, self.y = self.sp // 2, self.sp % 2
        self.x, self.c = self.tp // 2, self.tp % 2
        self.home = self.y == self.c
        self.rows_of, self.group = 2 * self.z + self.c, 2 * self.x + self.y

    def sibling(self):
        return {"tp": 2 * self.x + 1 - self.c}

    def along_x(self, core):
        return {"tp": 2 * (1 - self.x) + core}

    def along_y(self, core):
        return {"sp": 2 * self.z + 1 - self.y, "tp": 2 * self.x + core}

    def along_z(self, way):
        return {"sp": self.sp + 2 - 4 * way}

    def source(self, way, steps):
        return self.z - steps if way == 0 else self.z + steps

    def has(self, way, steps):
        return self.z >= steps if way == 0 else self.z + steps < self.planes

    def passes(self, way):
        return self.z + 1 < self.planes if way == 0 else self.z > 0


def remote(source, target, send_sem, recv_sem, device):
    return pltpu.make_async_remote_copy(
        src_ref=source,
        dst_ref=target,
        send_sem=send_sem,
        recv_sem=recv_sem,
        device_id=device,
        device_id_type=pl.DeviceIdType.MESH,
    )


class Chain:
    def __init__(self, place, shard, own_first, sems):
        self.place, self.shard, self.own_first = place, shard, own_first
        self.up_send, self.up_recv, self.pair_send, self.pair_recv, self.edge = sems
        self.events = [(step, slot) for step in range(place.planes) for slot in range(2)]
        self.done, self.whole = 0, set()

    def block(self, plane, slot, half):
        side = slot if not self.own_first else (self.place.y + slot) % 2
        return self.shard(2 * plane + side, half)

    def hop(self, way, step, slot):
        held = self.block(self.place.source(way, step), slot, self.place.c)
        return remote(
            held,
            held,
            self.up_send.at[way, step, slot],
            self.up_recv.at[way, step, slot],
            self.place.along_z(way),
        )

    def pair(self, way, step, slot):
        held = self.block(self.place.source(way, step), slot, self.place.c)
        return remote(
            held,
            held,
            self.pair_send.at[way, step, slot],
            self.pair_recv.at[way, step, slot],
            self.place.sibling(),
        )

    def own_pair(self):
        held = self.shard(self.place.sp, None)
        return remote(
            held,
            held,
            self.edge.at[0],
            self.edge.at[1],
            self.place.sibling(),
        )

    def give(self, half, source):
        return remote(
            source,
            self.shard(self.place.sp, half),
            self.edge.at[2 + half],
            self.edge.at[4],
            self.place.along_y(half),
        )

    def taken(self):
        held = self.shard(2 * self.place.z + 1 - self.place.y, self.place.c)
        return remote(held, held, self.edge.at[2], self.edge.at[4], self.place.along_y(0))

    def pass_on(self, step, slot):
        for way in range(2):

            @pl.when(self.place.passes(way))
            def _(way=way):
                self.hop(way, step, slot).start()

    def share_own(self):
        @pl.when(self.place.home)
        def _():
            self.own_pair().start()

        @pl.when(jnp.logical_not(self.place.home))
        def _():
            self.own_pair().wait_recv()

    def share_taken(self):
        self.taken().wait_recv()
        held = self.shard(2 * self.place.z + 1 - self.place.y, self.place.c)
        self.other_pair(held).start()

    def other_pair(self, held):
        return remote(
            held, held, self.edge.at[5], self.edge.at[6], self.place.sibling()
        )

    def taken_pair(self):
        return self.other_pair(
            self.shard(2 * self.place.z + 1 - self.place.y, self.place.c)
        )

    def advance(self):
        step, slot = self.events[self.done]
        self.done += 1
        if step == 0:
            if self.own_first:
                if slot == 0:
                    self.share_own()
                else:
                    self.share_taken()
            if self.place.planes > 1:
                self.pass_on(0, slot)
            return
        for way in range(2):

            @pl.when(self.place.has(way, step))
            def _(way=way):
                self.hop(way, step - 1, slot).wait_recv()
                self.pair(way, step, slot).start()
                if step + 1 < self.place.planes:

                    @pl.when(self.place.passes(way))
                    def _():
                        self.hop(way, step, slot).start()

    def upto(self, event):
        while self.done <= min(event, len(self.events) - 1):
            self.advance()

    def complete(self, step, slot):
        if (step, slot) in self.whole:
            return
        self.whole.add((step, slot))
        if step == 0:
            if slot == 1:
                self.taken_pair().wait_recv()
            return
        for way in range(2):

            @pl.when(self.place.has(way, step))
            def _(way=way):
                self.pair(way, step, slot).wait_recv()

    def sent_edges(self, gave):
        @pl.when(self.place.home)
        def _():
            self.own_pair().wait_send()

        @pl.when(jnp.logical_not(self.place.home))
        def _():
            for half in range(2):
                gave(half).wait_send()

        self.taken_pair().wait_send()

    def sent(self, event):
        step, slot = self.events[event]
        place = self.place
        for way in range(2):
            if step > 0:

                @pl.when(place.has(way, step))
                def _(way=way):
                    self.pair(way, step, slot).wait_send()

            if step + 1 < place.planes:

                @pl.when(place.has(way, step) & place.passes(way))
                def _(way=way):
                    self.hop(way, step, slot).wait_send()


def layer_kernel(
    count,
    tokens,
    w_pool_in,
    w_query,
    w_key_t,
    w_value_t,
    pool_map,
    w_out,
    gain_in,
    pool_scale_in,
    q_gain_in,
    k_gain_in,
    sinks_in,
    out,
    normed,
    first_weights,
    last_weights,
    own_shard,
    acc,
    queries,
    keys_low,
    keys_high,
    values_low,
    values_high,
    pool_span,
    pairs,
    mixed,
    bias,
    band,
    ones_block,
    halo_pairs,
    halo_pool,
    from_x,
    from_pair,
    from_away,
    from_last,
    key_value,
    pool_maps,
    gain,
    pool_scales,
    q_gain,
    k_gain,
    sinks,
    head_rows,
    local_sem,
    first_sems,
    last_sems,
    first_edge,
    last_edge,
    near_sem,
    far_sem,
    send_sem,
    relay_sem,
    table_sem,
    halo_sem,
    sum_send,
    sum_recv,
):
    place = Place(count)
    x, y, z, c = place.x, place.y, place.z, place.c
    home, away = place.home, jnp.logical_not(place.home)
    me, seq = place.group, place.rows_of
    rows, width = tokens.shape
    depth, branch = w_pool_in.shape
    head_columns = w_query.shape[1]
    mid = branch + head_columns
    piece = rows // TOKEN_CHUNKS
    blocks = rows // WINDOW
    out_rows = out.shape[0]
    out_width = w_out.shape[1]
    mix = w_out.shape[0]
    pairs_of_heads = head_columns // LANES

    barrier = pltpu.get_barrier_semaphore()

    def greet(device):
        pl.semaphore_signal(
            barrier, inc=1, device_id=device, device_id_type=pl.DeviceIdType.MESH
        )

    for way in range(2):

        @pl.when(place.passes(way))
        def _(way=way):
            greet(place.along_z(way))

    for core in range(2):
        greet(place.along_x(core))
        greet(place.along_y(core))
    greet(place.sibling())
    greetings = 5 + jnp.where(place.passes(0), 1, 0) + jnp.where(place.passes(1), 1, 0)

    def first_shard(owner, half):
        if half is None:
            return first_weights.at[aligned(owner, depth)]
        size = depth // 2
        return first_weights.at[pl.ds(pl.multiple_of(owner * depth + half * size, size), size)]

    def last_shard(owner, half):
        if half is None:
            return last_weights.at[owner]
        return last_weights.at[owner, aligned(half, mix // 2)]

    first = Chain(
        place, first_shard, True, [first_sems.at[i] for i in range(4)] + [first_edge]
    )
    last = Chain(place, last_shard, False, [last_sems.at[i] for i in range(4)] + [last_edge])

    def local_copy(index, source, target):
        return pltpu.make_async_copy(source, target, local_sem.at[index])

    own_rows = aligned(place.sp, depth)
    small = [
        local_copy(0, w_key_t, key_value.at[pl.ds(0, HEAD_DIM)]),
        local_copy(1, w_value_t, key_value.at[pl.ds(HEAD_DIM, HEAD_DIM)]),
        local_copy(2, gain_in, gain),
        local_copy(3, q_gain_in, q_gain),
        local_copy(4, k_gain_in, k_gain),
    ]

    def shard_copies(target):
        return [
            local_copy(5, w_pool_in, target.at[:, pl.ds(0, branch)]),
            local_copy(6, w_query, target.at[:, pl.ds(branch, head_columns)]),
        ]

    def home_copies():
        return [
            local_copy(7, tokens, normed.at[:, aligned(place.tp, width)]),
            local_copy(8, w_out, last_weights.at[place.sp]),
            local_copy(9, pool_map, pool_maps),
            local_copy(10, pool_scale_in, pool_scales),
            local_copy(11, sinks_in, sinks),
        ]

    for copy in small[:2]:
        copy.start()

    @pl.when(home)
    def _():
        for copy in shard_copies(first_weights.at[own_rows]) + home_copies():
            copy.start()

    @pl.when(away)
    def _():
        for copy in shard_copies(own_shard):
            copy.start()

    for copy in small[2:]:
        copy.start()
    small[0].wait()
    small[1].wait()
    pair_columns = key_value[...].astype(f32).T.astype(bf16)

    def table_copies():
        return [
            remote(
                source,
                target,
                table_sem.at[0, index],
                table_sem.at[1, index],
                place.sibling(),
            )
            for index, (source, target) in enumerate(
                [(pool_map, pool_maps), (pool_scale_in, pool_scales), (sinks_in, sinks)]
            )
        ]

    def first_gave(half):
        return first.give(half, own_shard.at[pl.ds(half * (depth // 2), depth // 2)])

    def last_gave(half):
        return last.give(half, w_out.at[pl.ds(half * (mix // 2), mix // 2)])

    @pl.when(home)
    def _():
        first_weights[own_rows, pl.ds(mid, LANES)] = pair_columns
        for copy in shard_copies(first_weights.at[own_rows]):
            copy.wait()

    @pl.when(away)
    def _():
        own_shard[:, pl.ds(mid, LANES)] = pair_columns
        for copy in shard_copies(own_shard):
            copy.wait()

    pl.semaphore_wait(barrier, greetings)

    @pl.when(away)
    def _():
        for half in range(2):
            first_gave(half).start()

    def token_rows(chunk):
        return pl.ds(chunk * piece, piece)

    def landing(chunk, side, core):
        owner = 2 * (jnp.where(x == 0, side, 1 - side)) + core
        return normed.at[token_rows(chunk), aligned(owner, width)]

    def to_sibling(chunk):
        return remote(
            tokens.at[token_rows(chunk)],
            landing(chunk, 0, c),
            send_sem.at[0, chunk],
            near_sem.at[c, chunk],
            place.sibling(),
        )

    def to_x(chunk):
        return remote(
            tokens.at[token_rows(chunk)],
            landing(chunk, 0, c),
            send_sem.at[1, chunk],
            far_sem.at[c, chunk],
            place.along_x(y),
        )

    def to_y(chunk):
        return remote(
            tokens.at[token_rows(chunk)],
            landing(chunk, 0, c),
            send_sem.at[2, chunk],
            near_sem.at[c, chunk],
            place.along_y(y),
        )

    def by_x(chunk, core):
        return core == 1 or chunk == 1

    def relay(chunk, core):
        if by_x(chunk, core):
            held = landing(chunk, 0, core)
            device = place.along_x(c)
        else:
            held = landing(chunk, 1, core)
            device = place.along_y(c)
        return remote(
            held, held, relay_sem.at[core, chunk], far_sem.at[core, chunk], device
        )

    def near_wait(chunk, core):
        held = landing(chunk, 0, core)
        remote(
            held, held, send_sem.at[0, chunk], near_sem.at[core, chunk], place.sibling()
        ).wait_recv()

    def far_wait(chunk, core):
        held = landing(chunk, 1, core)
        remote(
            held, held, send_sem.at[0, chunk], far_sem.at[core, chunk], place.sibling()
        ).wait_recv()

    ahead = 3

    def send_tokens(chunk):
        to_x(chunk).start()
        to_y(chunk).start()

    @pl.when(home)
    def _():
        for copy in table_copies():
            copy.start()

    first.upto(0)
    for chunk in range(ahead):
        to_x(chunk).start()

    @pl.when(away)
    def _():
        for chunk in range(TOKEN_CHUNKS):
            to_sibling(chunk).start()
        for chunk in range(ahead):
            to_y(chunk).start()

    span = 2.0 * jnp.exp2(me.astype(f32))
    row = lax.broadcasted_iota(jnp.int32, (WINDOW, 2 * WINDOW), 0)
    column = lax.broadcasted_iota(jnp.int32, (WINDOW, 2 * WINDOW), 1)
    distance = (row + WINDOW - column).astype(f32)
    band[...] = jnp.where((distance >= 0.0) & (distance < span), 1.0, 0.0).astype(bf16)
    allowed = (distance >= 0.0) & (distance < float(WINDOW))
    for pair in range(pairs_of_heads):
        for half in range(2):
            head = (me * GROUP + 2 * pair + half + 1).astype(f32)
            slope = jnp.exp2(jnp.full((WINDOW, 2 * WINDOW), -8.0 / Q_HEADS, f32) * head)
            bias[pl.ds(pair * WINDOW, WINDOW), pl.ds(half * 2 * WINDOW, 2 * WINDOW)] = jnp.where(
                allowed, -slope * distance, MASKED
            )
    block_row = lax.broadcasted_iota(jnp.int32, (2 * LANES, 2 * LANES), 0) // HEAD_DIM
    block_column = lax.broadcasted_iota(jnp.int32, (2 * LANES, 2 * LANES), 1) // HEAD_DIM
    ones_block[...] = jnp.where(block_row == block_column, 1.0, 0.0).astype(bf16)
    pool_span[pl.ds(0, WINDOW)] = jnp.zeros((WINDOW, branch), bf16)

    acc[...] = jnp.zeros(acc.shape, f32)
    strip = 32

    def normalise(chunk):
        @pl.loop(0, piece // strip)
        def _(index):
            held = pl.ds(pl.multiple_of(chunk * piece + index * strip, strip), strip)
            values = normed[held].astype(f32)
            scale = lax.rsqrt(jnp.mean(values * values, axis=-1, keepdims=True) + epsilon)
            normed[held] = (values * scale * gain[...]).astype(bf16)

    lane = lax.broadcasted_iota(jnp.int32, (1, LANES), 1)
    low = lane < HEAD_DIM
    for copy in small[2:]:
        copy.wait()

    @pl.when(home)
    def _():
        for copy in home_copies():
            copy.wait()
        last.own_pair().start()

    @pl.when(away)
    def _():
        for copy in table_copies():
            copy.wait_recv()

    head_rows[...] = jnp.zeros(head_rows.shape, f32)
    head_rows[pl.ds(0, 1), pl.ds(0, HEAD_DIM)] = q_gain[...] * HEAD_DIM**-0.5
    head_rows[pl.ds(1, 1), pl.ds(0, HEAD_DIM)] = k_gain[...]
    once = head_rows[pl.ds(0, 1), :]
    head_rows[pl.ds(0, 1), :] = once + pltpu.roll(once, HEAD_DIM, 1)
    for pair in range(pairs_of_heads):
        one, two = sinks[:, 2 * pair : 2 * pair + 1], sinks[:, 2 * pair + 1 : 2 * pair + 2]
        head_rows[pl.ds(2 + pair, 1), :] = jnp.exp(
            jnp.where(low, jnp.broadcast_to(one, (1, LANES)), jnp.broadcast_to(two, (1, LANES)))
        )

    tile = piece

    def multiply(chunks, steps):
        @pl.loop(steps[0], steps[1])
        def _(step):
            for way in range(2):

                @pl.when(place.has(way, step) & (step + way > 0))
                def _(way=way):
                    block = aligned(place.source(way, step), 2 * depth)

                    @pl.loop(chunks[0], chunks[1])
                    def _(index):
                        held = aligned(index, tile)
                        acc[held] += dot(normed[held, block], first_weights[block, :])

    class Progress:
        rows, steps = 0, 0

    def catch_up(chunks, steps):
        if steps > Progress.steps:
            for step in range(Progress.steps, steps):
                for slot in range(2):
                    first.complete(step, slot)
            if Progress.rows > 0:
                multiply((0, Progress.rows), (Progress.steps, steps))
            Progress.steps = steps
        if chunks > Progress.rows:
            if steps > 0:
                multiply((Progress.rows, chunks), (0, steps))
            Progress.rows = chunks

    def settle(chunk):
        for core in range(2):

            @pl.when(away if by_x(chunk, core) else home)
            def _(core=core):
                relay(chunk, core).wait_send()

        normalise(chunk)

    first.upto(1)
    first.complete(0, 1)

    @pl.when(home)
    def _():
        for chunk in range(ahead):
            to_y(chunk).start()

    events = len(first.events)

    def pass_tokens(chunk):
        @pl.when(home)
        def _():
            for core in range(2):
                far_wait(chunk, core)
                if not by_x(chunk, core):
                    relay(chunk, core).start()
            near_wait(chunk, 1 - c)

        @pl.when(away)
        def _():
            for core in range(2):
                near_wait(chunk, core)
                if by_x(chunk, core):
                    relay(chunk, core).start()

        if chunk + ahead < TOKEN_CHUNKS:
            send_tokens(chunk + ahead)

    def use_tokens(chunk):
        @pl.when(away)
        def _():
            for core in range(2):
                far_wait(chunk, core)
            if chunk == TOKEN_CHUNKS - 1:
                for half in range(2):
                    last_gave(half).start()

        settle(chunk)
        catch_up(chunk + 1, first.done // 2)

    for chunk in range(TOKEN_CHUNKS):
        first.upto((chunk + 3) * events // 8 - 1)
        pass_tokens(chunk)
        if chunk > 1:
            use_tokens(chunk - 2)

    @pl.when(away)
    def _():
        last.own_pair().wait_recv()

    first.upto(7 * events // 8 - 1)
    last.pass_on(0, y)
    for chunk in range(max(0, TOKEN_CHUNKS - 2), TOKEN_CHUNKS):
        use_tokens(chunk)
    first.upto(events - 1)
    catch_up(TOKEN_CHUNKS, place.planes)

    one_low = jnp.where(low, 1.0, 0.0)

    def spread(kv, held, count_scale):
        size = kv.shape[0]
        key_low = jnp.where(low, kv, 0.0)
        value_high = jnp.where(low, 0.0, kv)
        keys_low[held] = key_low.astype(bf16)
        keys_high[held] = pltpu.roll(key_low, HEAD_DIM, 1).astype(bf16)
        ones_low = jnp.broadcast_to(one_low * count_scale, (size, LANES)).astype(bf16)
        ones_high = jnp.broadcast_to((1.0 - one_low) * count_scale, (size, LANES)).astype(bf16)
        values_low[held, pl.ds(0, LANES)] = pltpu.roll(value_high, HEAD_DIM, 1).astype(bf16)
        values_low[held, pl.ds(LANES, LANES)] = ones_low
        values_high[held, pl.ds(0, LANES)] = value_high.astype(bf16)
        values_high[held, pl.ds(LANES, LANES)] = ones_high

    def finalise(index):
        held = aligned(index, tile)
        sums = acc[held].astype(bf16)
        shifted = pl.ds(pl.multiple_of(index * tile + WINDOW, WINDOW), tile)
        pool_span[shifted] = sums[:, :branch]
        kv = sums[:, mid:].astype(f32)
        squares = jnp.where(low, kv * kv, 0.0)
        scale = lax.rsqrt(jnp.sum(squares, axis=-1, keepdims=True) * (1.0 / HEAD_DIM) + epsilon)
        kv = jnp.where(low, kv * scale * head_rows[pl.ds(1, 1), :], kv).astype(bf16)
        pairs[held] = kv
        spread(kv.astype(f32), shifted, 1.0)
        wide = 2 * LANES
        gain_row = head_rows[pl.ds(0, 1), :]
        query_gain = jnp.concatenate([gain_row, gain_row], axis=1)
        for start in range(0, head_columns, wide):
            query = sums[:, branch + start : branch + start + wide].astype(f32)
            square = query * query
            upper = square.astype(bf16)
            lower = (square - upper.astype(f32)).astype(bf16)
            total = dot(upper, ones_block[...]) + dot(lower, ones_block[...])
            scale = lax.rsqrt(total * (1.0 / HEAD_DIM) + epsilon)
            queries[held, pl.ds(start, wide)] = (
                query * scale * query_gain
            ).astype(bf16)

    def halo_copies(device):
        return [
            remote(
                source,
                target,
                halo_sem.at[0, index],
                halo_sem.at[1, index],
                device,
            )
            for index, (source, target) in enumerate(
                [
                    (pairs.at[pl.ds(rows - WINDOW, WINDOW)], halo_pairs),
                    (pool_span.at[pl.ds(WINDOW + rows - HALO_ROWS, HALO_ROWS)], halo_pool),
                ]
            )
        ]

    next_plane = {"sp": place.sp + 2, "tp": 2 * x}
    sends_up = (c == 1) & place.passes(0)
    finalise(rows // tile - 1)

    @pl.when(c == 0)
    def _():
        for copy in halo_copies({"tp": 2 * x + 1}):
            copy.start()

    @pl.when(sends_up)
    def _():
        for copy in halo_copies(next_plane):
            copy.start()

    @pl.loop(0, rows // tile - 1)
    def _(index):
        finalise(index)

    def pool(block):
        held = aligned(block, WINDOW)
        span_rows = pool_span[pl.ds(pl.multiple_of(block * WINDOW, WINDOW), 2 * WINDOW)]
        running = dot(band[...], span_rows)
        offset = lax.broadcasted_iota(jnp.int32, (WINDOW, 1), 0)
        position = (seq * rows + block * WINDOW + offset).astype(f32)
        counted = jnp.minimum(position + 1.0, span)
        difference = (running / counted - span_rows[WINDOW:].astype(f32)).astype(bf16)
        mapped = dot(difference, pool_maps[...]) * pool_scales[...]
        scale = lax.rsqrt(jnp.mean(mapped * mapped, axis=-1, keepdims=True) + epsilon)
        mixed[held, pl.ds(0, branch)] = (mapped * scale).astype(bf16)

    def attend(block):
        held = aligned(block, WINDOW)
        both = pl.ds(pl.multiple_of(block * WINDOW, WINDOW), 2 * WINDOW)
        key_pair = jnp.concatenate([keys_low[both], keys_high[both]], axis=0)
        value_pair = jnp.concatenate([values_low[both], values_high[both]], axis=0)
        parts, squares = [], None
        for pair in range(pairs_of_heads):
            lanes = pl.ds(pair * LANES, LANES)
            scores = lax.dot_general(
                queries[held, lanes],
                key_pair,
                (((1,), (1,)), ((), ())),
                preferred_element_type=f32,
            )
            weights = jnp.exp(scores + bias[pl.ds(pair * WINDOW, WINDOW)]).astype(bf16)
            result = dot(weights, value_pair)
            part = result[:, :LANES] / (
                result[:, LANES:] + head_rows[pl.ds(2 + pair, 1), :]
            )
            parts.append(part)
            squares = part * part if squares is None else squares + part * part
        mean = jnp.sum(squares, axis=-1, keepdims=True) * (1.0 / head_columns)
        scale = lax.rsqrt(mean + epsilon)
        for pair, part in enumerate(parts):
            mixed[held, pl.ds(branch + pair * LANES, LANES)] = (part * scale).astype(bf16)

    half = (blocks + 1) // 2

    @pl.loop(1, half + 1)
    def _(block):
        pool(block)
        attend(block)

    last.share_taken()
    last.pass_on(0, 1 - y)
    last.done = 2

    @pl.loop(half + 1, blocks)
    def _(block):
        pool(block)
        attend(block)

    begun = jnp.where(seq > 0, 1.0, 0.0)
    top = pl.ds(0, WINDOW)

    @pl.when(seq > 0)
    def _():
        for copy in halo_copies(next_plane):
            copy.wait_recv()
        spread(halo_pairs[...].astype(f32), top, 1.0)
        pool_span[pl.ds(WINDOW - HALO_ROWS, HALO_ROWS)] = halo_pool[...]

    @pl.when(seq == 0)
    def _():
        for ref in (keys_low, keys_high, values_low, values_high):
            ref[top] = jnp.zeros((WINDOW, ref.shape[1]), bf16)

    pool(0)
    attend(0)

    if out_width % (2 * LANES) == 0:
        units_of = {0: [(1, 0), (2, out_width // 2)], 1: [(1, 0), (2, out_width // 2)]}
        unit_width = out_width // 2
    else:
        units_of = {0: [(1, 0)], 1: [(2, 0)]}
        unit_width = out_width

    step_of = min(unit_width, LANES)

    class Shard:
        def __init__(self, owner, slot):
            self.owner, self.units = owner, units_of[slot]

        def lanes(self, start, size):
            return pl.ds(pl.multiple_of(self.owner * out_width + start, step_of), size)

        def unit(self, start):
            return self.lanes(start, unit_width)

        def packed(self):
            index = self.owner if len(self.units) == 2 else self.owner // 2
            return aligned(index, unit_width)

        def copy(self, source, target, sent, landed, device):
            return remote(
                source,
                target,
                sum_send.at[sent, self.owner],
                sum_recv.at[landed, self.owner],
                device,
            )

        def row_block(self, index, lanes):
            return normed.at[aligned(index, out_rows), lanes]

        def across_x(self, start):
            lanes = self.unit(start)
            return self.copy(
                normed.at[aligned(1 - x, 2 * out_rows), lanes],
                from_x.at[:, self.packed()],
                0,
                0,
                place.along_x(c),
            )

        def across_y(self, start):
            return self.copy(
                normed.at[:, self.unit(start)],
                from_away.at[:, self.packed()],
                1,
                1,
                place.along_y(c),
            )

        def to_pair(self):
            lanes = self.lanes(0, out_width)
            return self.copy(
                self.row_block(2 * x + 1 - c, lanes),
                from_pair.at[:, lanes],
                1,
                1,
                place.sibling(),
            )

        def away_final(self, start, core):
            lanes = self.unit(start)
            return self.copy(
                self.row_block(2 * x + core, lanes),
                from_last.at[:, lanes],
                2 + core,
                2,
                place.along_y(core),
            )

        def home_final(self, start, core):
            lanes = self.unit(start)
            return self.copy(
                self.row_block(2 * (1 - x) + core, lanes),
                from_last.at[:, lanes],
                4 + core,
                3,
                place.along_x(core),
            )

        def first(self):
            lanes = self.lanes(0, out_width)

            @pl.loop(0, 4)
            def _(index):
                held = aligned((2 * (1 - x) + index) % 4, out_rows)
                normed[held, lanes] = dot(mixed[held, :], last_weights[self.owner]).astype(bf16)

            for scheme, start in self.units:
                if scheme == 1:
                    self.across_x(start).start()
                else:

                    @pl.when(away)
                    def _(start=start):
                        self.across_y(start).start()

        def second(self):
            for scheme, start in self.units:
                lanes = self.unit(start)
                if scheme == 1:
                    self.across_x(start).wait_recv()
                    held = aligned(x, 2 * out_rows)
                    normed[held, lanes] = (
                        normed[held, lanes].astype(f32) + from_x[:, self.packed()].astype(f32)
                    ).astype(bf16)

                    @pl.when(away)
                    def _(start=start):
                        for core in range(2):
                            self.away_final(start, core).start()
                else:

                    @pl.when(home)
                    def _(start=start, lanes=lanes):
                        self.across_y(start).wait_recv()

                        @pl.loop(0, 4)
                        def _(index):
                            held = aligned(index, out_rows)
                            normed[held, lanes] = (
                                normed[held, lanes].astype(f32)
                                + from_away[held, self.packed()].astype(f32)
                            ).astype(bf16)

                        for core in range(2):
                            self.home_final(start, core).start()

            @pl.when(home)
            def _():
                self.to_pair().start()

        def third(self):
            lanes = self.lanes(0, out_width)
            for scheme, start in self.units:
                if scheme == 1:
                    self.away_final(start, 0).wait_recv()
                else:
                    self.home_final(start, 0).wait_recv()

            @pl.when(home)
            def _():
                out[:, lanes] = (
                    normed[aligned(2 * x + c, out_rows), lanes].astype(f32)
                    + from_last[:, lanes].astype(f32)
                ).astype(bf16)

            @pl.when(away)
            def _():
                self.to_pair().wait_recv()
                out[:, lanes] = (
                    from_pair[:, lanes].astype(f32) + from_last[:, lanes].astype(f32)
                ).astype(bf16)

        def sent(self):
            for scheme, start in self.units:
                if scheme == 1:
                    self.across_x(start).wait_send()

                    @pl.when(away)
                    def _(start=start):
                        for core in range(2):
                            self.away_final(start, core).wait_send()
                else:

                    @pl.when(away)
                    def _(start=start):
                        self.across_y(start).wait_send()

                    @pl.when(home)
                    def _(start=start):
                        for core in range(2):
                            self.home_final(start, core).wait_send()

            @pl.when(home)
            def _():
                self.to_pair().wait_send()

    def each(event, stage):
        step, slot = last.events[event]

        @pl.loop(0, 1 if step == 0 else 2)
        def _(way):
            plane = z + (2 * way - 1) * step

            @pl.when((plane >= 0) & (plane < place.planes))
            def _():
                getattr(Shard(2 * plane + slot, slot), stage)()

    last.taken_pair().wait_recv()
    total = len(last.events)

    def early_sends():
        for chunk in range(TOKEN_CHUNKS):
            to_x(chunk).wait_send()
            to_y(chunk).wait_send()

        @pl.when(away)
        def _():
            for chunk in range(TOKEN_CHUNKS):
                to_sibling(chunk).wait_send()

        @pl.when(home)
        def _():
            for copy in table_copies():
                copy.wait_send()

        @pl.when((c == 0) | sends_up)
        def _():
            for copy in halo_copies(next_plane):
                copy.wait_send()

        first.sent_edges(first_gave)
        last.sent_edges(last_gave)
        for event in range(total):
            first.sent(event)

    for event, (step, slot) in enumerate(last.events):
        last.upto(event)
        if step > 0:
            last.complete(step, slot)
        each(event, "first")
        if event > 0:
            each(event - 1, "second")
        if event > 2:
            each(event - 3, "third")
        if event == min(3, total - 1):
            early_sends()
        if event > 3:
            last.sent(event - 4)
            each(event - 4, "sent")
    each(total - 1, "second")
    for event in range(max(0, total - 3), total):
        each(event, "third")
    for event in range(max(0, total - 4), total):
        last.sent(event)
        each(event, "sent")


def layer(tokens, w_pool_in, w_query, w_key_t, w_value_t, pool_map, w_out, *rows_in):
    count = lax.axis_size("sp")
    rows, width = tokens.shape
    depth, branch = w_pool_in.shape
    head_columns = w_query.shape[1]
    features = width * lax.axis_size("tp")
    mix, out_width = w_out.shape
    out_rows = rows // lax.axis_size("tp")
    out_columns = count * out_width
    sums = branch + head_columns + LANES
    dma = pltpu.SemaphoreType.DMA
    planes = count // 2
    hbm = pl.BlockSpec(memory_space=pltpu.HBM)
    flops = 2 * rows * features * sums + 2 * rows * mix * out_columns
    return pl.pallas_call(
        functools.partial(layer_kernel, count),
        out_shape=pltpu.VMEM((out_rows, out_columns), bf16),
        in_specs=[hbm] * 12,
        out_specs=pl.BlockSpec(memory_space=pltpu.VMEM),
        scratch_shapes=[
            pltpu.VMEM((rows, features), bf16),
            pltpu.VMEM((features, sums), bf16),
            pltpu.VMEM((count, mix, out_width), bf16),
            pltpu.VMEM((depth, sums), bf16),
            pltpu.VMEM((rows, sums), f32),
            pltpu.VMEM((rows, head_columns), bf16),
            pltpu.VMEM((WINDOW + rows, LANES), bf16),
            pltpu.VMEM((WINDOW + rows, LANES), bf16),
            pltpu.VMEM((WINDOW + rows, 2 * LANES), bf16),
            pltpu.VMEM((WINDOW + rows, 2 * LANES), bf16),
            pltpu.VMEM((WINDOW + rows, branch), bf16),
            pltpu.VMEM((rows, LANES), bf16),
            pltpu.VMEM((rows, mix), bf16),
            pltpu.VMEM((head_columns // LANES * WINDOW, 4 * WINDOW), f32),
            pltpu.VMEM((WINDOW, 2 * WINDOW), bf16),
            pltpu.VMEM((2 * LANES, 2 * LANES), bf16),
            pltpu.VMEM((WINDOW, LANES), bf16),
            pltpu.VMEM((HALO_ROWS, branch), bf16),
            pltpu.VMEM((2 * out_rows, out_columns // 2), bf16),
            pltpu.VMEM((out_rows, out_columns), bf16),
            pltpu.VMEM((rows, out_columns // 2), bf16),
            pltpu.VMEM((out_rows, out_columns), bf16),
            pltpu.VMEM((2 * HEAD_DIM, depth), bf16),
            pltpu.VMEM((branch, branch), bf16),
            pltpu.VMEM((1, features), f32),
            pltpu.VMEM((1, branch), f32),
            pltpu.VMEM((1, HEAD_DIM), f32),
            pltpu.VMEM((1, HEAD_DIM), f32),
            pltpu.VMEM((1, GROUP), f32),
            pltpu.VMEM((8, LANES), f32),
            dma((12,)),
            dma((4, 2, planes, 2)),
            dma((4, 2, planes, 2)),
            dma((7,)),
            dma((7,)),
            dma((2, TOKEN_CHUNKS)),
            dma((2, TOKEN_CHUNKS)),
            dma((3, TOKEN_CHUNKS)),
            dma((2, TOKEN_CHUNKS)),
            dma((2, 3)),
            dma((2, 2)),
            dma((6, count)),
            dma((4, count)),
        ],
        compiler_params=pltpu.CompilerParams(
            collective_id=0, has_side_effects=True, vmem_limit_bytes=60 * 1024 * 1024
        ),
        cost_estimate=pl.CostEstimate(
            flops=flops, bytes_accessed=4 * rows * width, transcendentals=0
        ),
    )(tokens, w_pool_in, w_query, w_key_t, w_value_t, pool_map, w_out, *rows_in)


def local(
    tokens,
    norm_gain,
    w_pool_in,
    w_query,
    w_key,
    w_value,
    pool_map,
    pool_scale,
    q_gain,
    k_gain,
    sinks,
    w_out,
):
    return layer(
        tokens,
        w_pool_in,
        w_query,
        w_key.T,
        w_value.T,
        pool_map[0],
        w_out,
        norm_gain[None],
        pool_scale[None],
        q_gain[None],
        k_gain[None],
        sinks[None],
    )


def solution(mesh):
    in_specs = (
        P("sp", "tp"),
        P(),
        P("sp", "tp"),
        P("sp", "tp"),
        P("sp", "tp"),
        P("sp", "tp"),
        P("tp", None, None),
        P("tp"),
        P(),
        P(),
        P("tp"),
        P("tp", "sp"),
    )
    out_specs = P(("sp", "tp"), None)
    return jax.shard_map(local, mesh=mesh, in_specs=in_specs, out_specs=out_specs, check_vma=False)
```

```python
import functools

import jax
import jax.numpy as jnp
from jax import lax
from jax.experimental import pallas as pl
from jax.experimental.pallas import tpu as pltpu
from jax.sharding import PartitionSpec as P

HEAD_DIM = 64
GROUP = 8
WINDOW = 128
Q_HEADS = 32
LANES = 128
TOKEN_CHUNKS = 4
HALO_ROWS = 16
MASKED = -1e30

epsilon = 1e-06
bf16, f32 = jnp.bfloat16, jnp.float32


def aligned(index, size):
    return pl.ds(pl.multiple_of(index * size, size), size)


def dot(left, right):
    return jnp.dot(left, right, preferred_element_type=f32)


class Place:
    def __init__(self, count):
        self.planes = count // 2
        self.sp, self.tp = lax.axis_index("sp"), lax.axis_index("tp")
        self.z, self.y = self.sp // 2, self.sp % 2
        self.x, self.c = self.tp // 2, self.tp % 2
        self.home = self.y == self.c
        self.rows_of, self.group = 2 * self.z + self.c, 2 * self.x + self.y

    def sibling(self):
        return {"tp": 2 * self.x + 1 - self.c}

    def along_x(self, core):
        return {"tp": 2 * (1 - self.x) + core}

    def along_y(self, core):
        return {"sp": 2 * self.z + 1 - self.y, "tp": 2 * self.x + core}

    def along_z(self, way):
        return {"sp": self.sp + 2 - 4 * way}

    def source(self, way, steps):
        return self.z - steps if way == 0 else self.z + steps

    def has(self, way, steps):
        return self.z >= steps if way == 0 else self.z + steps < self.planes

    def passes(self, way):
        return self.z + 1 < self.planes if way == 0 else self.z > 0


def remote(source, target, send_sem, recv_sem, device):
    return pltpu.make_async_remote_copy(
        src_ref=source,
        dst_ref=target,
        send_sem=send_sem,
        recv_sem=recv_sem,
        device_id=device,
        device_id_type=pl.DeviceIdType.MESH,
    )


class Chain:
    def __init__(self, place, shard, own_first, sems):
        self.place, self.shard, self.own_first = place, shard, own_first
        self.up_send, self.up_recv, self.pair_recv, self.edge = sems
        self.events = [(step, slot) for step in range(place.planes) for slot in range(2)]
        self.done, self.whole = 0, set()

    def block(self, plane, slot, half):
        side = slot if not self.own_first else (self.place.y + slot) % 2
        return self.shard(2 * plane + side, half)

    def hop(self, way, step, slot):
        held = self.block(self.place.source(way, step), slot, self.place.c)
        return remote(
            held,
            held,
            self.up_send.at[way, step, slot],
            self.up_recv.at[way, step, slot],
            self.place.along_z(way),
        )

    def pair(self, way, step, slot):
        held = self.block(self.place.source(way, step), slot, self.place.c)
        return remote(
            held,
            held,
            self.edge.at[7],
            self.pair_recv.at[way, step - 1, slot],
            self.place.sibling(),
        )

    def own_pair(self):
        held = self.shard(self.place.sp, None)
        return remote(
            held,
            held,
            self.edge.at[0],
            self.edge.at[1],
            self.place.sibling(),
        )

    def give(self, half, source):
        return remote(
            source,
            self.shard(self.place.sp, half),
            self.edge.at[2 + half],
            self.edge.at[4],
            self.place.along_y(half),
        )

    def taken(self):
        held = self.shard(2 * self.place.z + 1 - self.place.y, self.place.c)
        return remote(held, held, self.edge.at[2], self.edge.at[4], self.place.along_y(0))

    def pass_on(self, step, slot):
        for way in range(2):

            @pl.when(self.place.passes(way))
            def _(way=way):
                self.hop(way, step, slot).start()

    def share_own(self):
        @pl.when(self.place.home)
        def _():
            self.own_pair().start()

        @pl.when(jnp.logical_not(self.place.home))
        def _():
            self.own_pair().wait_recv()

    def share_taken(self):
        self.taken().wait_recv()
        held = self.shard(2 * self.place.z + 1 - self.place.y, self.place.c)
        self.other_pair(held).start()

    def other_pair(self, held):
        return remote(
            held, held, self.edge.at[5], self.edge.at[6], self.place.sibling()
        )

    def taken_pair(self):
        return self.other_pair(
            self.shard(2 * self.place.z + 1 - self.place.y, self.place.c)
        )

    def advance(self):
        step, slot = self.events[self.done]
        self.done += 1
        if step == 0:
            if self.own_first:
                if slot == 0:
                    self.share_own()
                else:
                    self.share_taken()
            if self.place.planes > 1:
                self.pass_on(0, slot)
            return
        for way in range(2):

            @pl.when(self.place.has(way, step))
            def _(way=way):
                self.hop(way, step - 1, slot).wait_recv()
                self.pair(way, step, slot).start()
                if step + 1 < self.place.planes:

                    @pl.when(self.place.passes(way))
                    def _():
                        self.hop(way, step, slot).start()

    def upto(self, event):
        while self.done <= min(event, len(self.events) - 1):
            self.advance()

    def complete(self, step, slot):
        if (step, slot) in self.whole:
            return
        self.whole.add((step, slot))
        if step == 0:
            if slot == 1:
                self.taken_pair().wait_recv()
            return
        for way in range(2):

            @pl.when(self.place.has(way, step))
            def _(way=way):
                self.pair(way, step, slot).wait_recv()

    def sent_edges(self, gave):
        @pl.when(self.place.home)
        def _():
            self.own_pair().wait_send()

        @pl.when(jnp.logical_not(self.place.home))
        def _():
            for half in range(2):
                gave(half).wait_send()

        self.taken_pair().wait_send()

    def sent(self, event):
        step, slot = self.events[event]
        place = self.place
        if step + 1 < place.planes:
            for way in range(2):

                @pl.when(place.has(way, step) & place.passes(way))
                def _(way=way):
                    self.hop(way, step, slot).wait_send()

    def shared(self, whole):
        remote(
            whole, whole, self.edge.at[7], self.edge.at[0], self.place.sibling()
        ).wait_send()


def layer_kernel(
    count,
    tokens,
    w_pool_in,
    w_query,
    w_key_t,
    w_value_t,
    pool_map,
    w_out,
    gain_in,
    pool_scale_in,
    q_gain_in,
    k_gain_in,
    sinks_in,
    out,
    normed,
    first_weights,
    last_weights,
    own_shard,
    acc,
    queries,
    keys_low,
    keys_high,
    values_low,
    values_high,
    pool_span,
    pairs,
    mixed,
    bias,
    band,
    ones_block,
    halo_pairs,
    halo_pool,
    from_x,
    from_pair,
    from_away,
    from_last,
    key_value,
    pool_maps,
    gain,
    pool_scales,
    q_gain,
    k_gain,
    sinks,
    head_rows,
    local_sem,
    first_sems,
    last_sems,
    first_edge,
    last_edge,
    near_sem,
    far_sem,
    send_sem,
    relay_sem,
    table_sem,
    halo_sem,
    sum_send,
    sum_recv,
    half_recv,
):
    place = Place(count)
    x, y, z, c = place.x, place.y, place.z, place.c
    home, away = place.home, jnp.logical_not(place.home)
    me, seq = place.group, place.rows_of
    rows, width = tokens.shape
    depth, branch = w_pool_in.shape
    head_columns = w_query.shape[1]
    mid = branch + head_columns
    piece = rows // TOKEN_CHUNKS
    blocks = rows // WINDOW
    out_rows = out.shape[0]
    out_width = w_out.shape[1]
    mix = w_out.shape[0]
    pairs_of_heads = head_columns // LANES

    barrier = pltpu.get_barrier_semaphore()

    def greet(device):
        pl.semaphore_signal(
            barrier, inc=1, device_id=device, device_id_type=pl.DeviceIdType.MESH
        )

    for way in range(2):

        @pl.when(place.passes(way))
        def _(way=way):
            greet(place.along_z(way))

    for core in range(2):
        greet(place.along_x(core))
        greet(place.along_y(core))
    greet(place.sibling())
    greetings = 5 + jnp.where(place.passes(0), 1, 0) + jnp.where(place.passes(1), 1, 0)

    def first_shard(owner, half):
        if half is None:
            return first_weights.at[aligned(owner, depth)]
        size = depth // 2
        return first_weights.at[pl.ds(pl.multiple_of(owner * depth + half * size, size), size)]

    def last_shard(owner, half):
        if half is None:
            return last_weights.at[owner]
        return last_weights.at[owner, aligned(half, mix // 2)]

    first = Chain(
        place, first_shard, True, [first_sems.at[i] for i in range(3)] + [first_edge]
    )
    last = Chain(place, last_shard, False, [last_sems.at[i] for i in range(3)] + [last_edge])

    def local_copy(index, source, target):
        return pltpu.make_async_copy(source, target, local_sem.at[index])

    own_rows = aligned(place.sp, depth)
    small = [
        local_copy(0, w_key_t, key_value.at[pl.ds(0, HEAD_DIM)]),
        local_copy(1, w_value_t, key_value.at[pl.ds(HEAD_DIM, HEAD_DIM)]),
        local_copy(2, gain_in, gain),
        local_copy(3, q_gain_in, q_gain),
        local_copy(4, k_gain_in, k_gain),
    ]

    def shard_copies(target):
        return [
            local_copy(5, w_pool_in, target.at[:, pl.ds(0, branch)]),
            local_copy(6, w_query, target.at[:, pl.ds(branch, head_columns)]),
        ]

    def home_copies():
        return [
            local_copy(7, tokens, normed.at[:, aligned(place.tp, width)]),
            local_copy(8, w_out, last_weights.at[place.sp]),
            local_copy(9, pool_map, pool_maps),
            local_copy(10, pool_scale_in, pool_scales),
            local_copy(11, sinks_in, sinks),
        ]

    for copy in small[:2]:
        copy.start()

    @pl.when(home)
    def _():
        for copy in shard_copies(first_weights.at[own_rows]) + home_copies():
            copy.start()

    @pl.when(away)
    def _():
        for copy in shard_copies(own_shard):
            copy.start()

    for copy in small[2:]:
        copy.start()
    small[0].wait()
    small[1].wait()
    pair_columns = key_value[...].astype(f32).T.astype(bf16)

    def table_copies():
        return [
            remote(
                source,
                target,
                table_sem.at[0, index],
                table_sem.at[1, index],
                place.sibling(),
            )
            for index, (source, target) in enumerate(
                [(pool_map, pool_maps), (pool_scale_in, pool_scales), (sinks_in, sinks)]
            )
        ]

    def first_gave(half):
        return first.give(half, own_shard.at[pl.ds(half * (depth // 2), depth // 2)])

    def last_gave(half):
        return last.give(half, w_out.at[pl.ds(half * (mix // 2), mix // 2)])

    @pl.when(home)
    def _():
        first_weights[own_rows, pl.ds(mid, LANES)] = pair_columns
        for copy in shard_copies(first_weights.at[own_rows]):
            copy.wait()

    @pl.when(away)
    def _():
        own_shard[:, pl.ds(mid, LANES)] = pair_columns
        for copy in shard_copies(own_shard):
            copy.wait()

    pl.semaphore_wait(barrier, greetings)

    @pl.when(away)
    def _():
        for half in range(2):
            first_gave(half).start()

    def token_rows(chunk):
        return pl.ds(chunk * piece, piece)

    def landing(chunk, side, core):
        owner = 2 * (jnp.where(x == 0, side, 1 - side)) + core
        return normed.at[token_rows(chunk), aligned(owner, width)]

    def to_sibling(chunk):
        return remote(
            tokens.at[token_rows(chunk)],
            landing(chunk, 0, c),
            send_sem.at[0],
            near_sem.at[c, chunk],
            place.sibling(),
        )

    def to_x(chunk):
        return remote(
            tokens.at[token_rows(chunk)],
            landing(chunk, 0, c),
            send_sem.at[1],
            far_sem.at[c, chunk],
            place.along_x(y),
        )

    def to_y(chunk):
        return remote(
            tokens.at[token_rows(chunk)],
            landing(chunk, 0, c),
            send_sem.at[2],
            near_sem.at[c, chunk],
            place.along_y(y),
        )

    def by_x(chunk, core):
        return core == 1 or chunk == 1

    def relay(chunk, core):
        if by_x(chunk, core):
            held = landing(chunk, 0, core)
            device = place.along_x(c)
        else:
            held = landing(chunk, 1, core)
            device = place.along_y(c)
        return remote(
            held, held, relay_sem.at[core, chunk], far_sem.at[core, chunk], device
        )

    def near_wait(chunk, core):
        held = landing(chunk, 0, core)
        remote(
            held, held, send_sem.at[0], near_sem.at[core, chunk], place.sibling()
        ).wait_recv()

    def far_wait(chunk, core):
        held = landing(chunk, 1, core)
        remote(
            held, held, send_sem.at[0], far_sem.at[core, chunk], place.sibling()
        ).wait_recv()

    ahead = 3

    def send_tokens(chunk):
        to_x(chunk).start()
        to_y(chunk).start()

    @pl.when(home)
    def _():
        for copy in table_copies():
            copy.start()

    first.upto(0)
    for chunk in range(ahead):
        to_x(chunk).start()

    @pl.when(away)
    def _():
        for chunk in range(TOKEN_CHUNKS):
            to_sibling(chunk).start()
        for chunk in range(ahead):
            to_y(chunk).start()

    span = 2.0 * jnp.exp2(me.astype(f32))
    row = lax.broadcasted_iota(jnp.int32, (WINDOW, 2 * WINDOW), 0)
    column = lax.broadcasted_iota(jnp.int32, (WINDOW, 2 * WINDOW), 1)
    distance = (row + WINDOW - column).astype(f32)
    band[...] = jnp.where((distance >= 0.0) & (distance < span), 1.0, 0.0).astype(bf16)
    allowed = (distance >= 0.0) & (distance < float(WINDOW))
    for pair in range(pairs_of_heads):
        for half in range(2):
            head = (me * GROUP + 2 * pair + half + 1).astype(f32)
            slope = jnp.exp2(jnp.full((WINDOW, 2 * WINDOW), -8.0 / Q_HEADS, f32) * head)
            bias[pl.ds(pair * WINDOW, WINDOW), pl.ds(half * 2 * WINDOW, 2 * WINDOW)] = jnp.where(
                allowed, -slope * distance, MASKED
            )
    block_row = lax.broadcasted_iota(jnp.int32, (2 * LANES, 2 * LANES), 0) // HEAD_DIM
    block_column = lax.broadcasted_iota(jnp.int32, (2 * LANES, 2 * LANES), 1) // HEAD_DIM
    ones_block[...] = jnp.where(block_row == block_column, 1.0, 0.0).astype(bf16)
    pool_span[pl.ds(0, WINDOW)] = jnp.zeros((WINDOW, branch), bf16)

    acc[...] = jnp.zeros(acc.shape, f32)
    strip = 32

    def normalise(chunk):
        @pl.loop(0, piece // strip)
        def _(index):
            held = pl.ds(pl.multiple_of(chunk * piece + index * strip, strip), strip)
            values = normed[held].astype(f32)
            scale = lax.rsqrt(jnp.mean(values * values, axis=-1, keepdims=True) + epsilon)
            normed[held] = (values * scale * gain[...]).astype(bf16)

    lane = lax.broadcasted_iota(jnp.int32, (1, LANES), 1)
    low = lane < HEAD_DIM
    for copy in small[2:]:
        copy.wait()

    @pl.when(home)
    def _():
        for copy in home_copies():
            copy.wait()
        last.own_pair().start()

    @pl.when(away)
    def _():
        for copy in table_copies():
            copy.wait_recv()

    head_rows[...] = jnp.zeros(head_rows.shape, f32)
    head_rows[pl.ds(0, 1), pl.ds(0, HEAD_DIM)] = q_gain[...] * HEAD_DIM**-0.5
    head_rows[pl.ds(1, 1), pl.ds(0, HEAD_DIM)] = k_gain[...]
    once = head_rows[pl.ds(0, 1), :]
    head_rows[pl.ds(0, 1), :] = once + pltpu.roll(once, HEAD_DIM, 1)
    for pair in range(pairs_of_heads):
        one, two = sinks[:, 2 * pair : 2 * pair + 1], sinks[:, 2 * pair + 1 : 2 * pair + 2]
        head_rows[pl.ds(2 + pair, 1), :] = jnp.exp(
            jnp.where(low, jnp.broadcast_to(one, (1, LANES)), jnp.broadcast_to(two, (1, LANES)))
        )

    tile = piece

    def multiply(chunks, steps):
        @pl.loop(steps[0], steps[1])
        def _(step):
            for way in range(2):

                @pl.when(place.has(way, step) & (step + way > 0))
                def _(way=way):
                    block = aligned(place.source(way, step), 2 * depth)

                    @pl.loop(chunks[0], chunks[1])
                    def _(index):
                        held = aligned(index, tile)
                        acc[held] += dot(normed[held, block], first_weights[block, :])

    class Progress:
        rows, steps = 0, 0

    def catch_up(chunks, steps):
        if steps > Progress.steps:
            for step in range(Progress.steps, steps):
                for slot in range(2):
                    first.complete(step, slot)
            if Progress.rows > 0:
                multiply((0, Progress.rows), (Progress.steps, steps))
            Progress.steps = steps
        if chunks > Progress.rows:
            if steps > 0:
                multiply((Progress.rows, chunks), (0, steps))
            Progress.rows = chunks

    def settle(chunk):
        for core in range(2):

            @pl.when(away if by_x(chunk, core) else home)
            def _(core=core):
                relay(chunk, core).wait_send()

        normalise(chunk)

    first.upto(1)
    first.complete(0, 1)

    @pl.when(home)
    def _():
        for chunk in range(ahead):
            to_y(chunk).start()

    events = len(first.events)

    def pass_tokens(chunk):
        @pl.when(home)
        def _():
            for core in range(2):
                far_wait(chunk, core)
                if not by_x(chunk, core):
                    relay(chunk, core).start()
            near_wait(chunk, 1 - c)

        @pl.when(away)
        def _():
            for core in range(2):
                near_wait(chunk, core)
                if by_x(chunk, core):
                    relay(chunk, core).start()

        if chunk + ahead < TOKEN_CHUNKS:
            send_tokens(chunk + ahead)

    def use_tokens(chunk):
        @pl.when(away)
        def _():
            for core in range(2):
                far_wait(chunk, core)
            if chunk == TOKEN_CHUNKS - 1:
                for half in range(2):
                    last_gave(half).start()

        settle(chunk)
        known = first.done // 2
        if chunk == TOKEN_CHUNKS - 1:
            first.upto(events - 1)
        catch_up(chunk + 1, known)

    for chunk in range(TOKEN_CHUNKS):
        first.upto((chunk + 3) * events // 8 - 1)
        pass_tokens(chunk)
        if chunk > 1:
            use_tokens(chunk - 2)

    @pl.when(away)
    def _():
        last.own_pair().wait_recv()

    first.upto(7 * events // 8 - 1)
    last.pass_on(0, y)
    for chunk in range(max(0, TOKEN_CHUNKS - 2), TOKEN_CHUNKS):
        use_tokens(chunk)
    catch_up(TOKEN_CHUNKS, place.planes)

    one_low = jnp.where(low, 1.0, 0.0)

    def spread(kv, held, count_scale):
        size = kv.shape[0]
        key_low = jnp.where(low, kv, 0.0)
        value_high = jnp.where(low, 0.0, kv)
        keys_low[held] = key_low.astype(bf16)
        keys_high[held] = pltpu.roll(key_low, HEAD_DIM, 1).astype(bf16)
        ones_low = jnp.broadcast_to(one_low * count_scale, (size, LANES)).astype(bf16)
        ones_high = jnp.broadcast_to((1.0 - one_low) * count_scale, (size, LANES)).astype(bf16)
        values_low[held, pl.ds(0, LANES)] = pltpu.roll(value_high, HEAD_DIM, 1).astype(bf16)
        values_low[held, pl.ds(LANES, LANES)] = ones_low
        values_high[held, pl.ds(0, LANES)] = value_high.astype(bf16)
        values_high[held, pl.ds(LANES, LANES)] = ones_high

    def finalise(index):
        held = aligned(index, tile)
        sums = acc[held].astype(bf16)
        shifted = pl.ds(pl.multiple_of(index * tile + WINDOW, WINDOW), tile)
        pool_span[shifted] = sums[:, :branch]
        kv = sums[:, mid:].astype(f32)
        squares = jnp.where(low, kv * kv, 0.0)
        scale = lax.rsqrt(jnp.sum(squares, axis=-1, keepdims=True) * (1.0 / HEAD_DIM) + epsilon)
        kv = jnp.where(low, kv * scale * head_rows[pl.ds(1, 1), :], kv).astype(bf16)
        pairs[held] = kv
        spread(kv.astype(f32), shifted, 1.0)
        wide = 2 * LANES
        gain_row = head_rows[pl.ds(0, 1), :]
        query_gain = jnp.concatenate([gain_row, gain_row], axis=1)
        for start in range(0, head_columns, wide):
            query = sums[:, branch + start : branch + start + wide].astype(f32)
            square = query * query
            upper = square.astype(bf16)
            lower = (square - upper.astype(f32)).astype(bf16)
            total = dot(upper, ones_block[...]) + dot(lower, ones_block[...])
            scale = lax.rsqrt(total * (1.0 / HEAD_DIM) + epsilon)
            queries[held, pl.ds(start, wide)] = (
                query * scale * query_gain
            ).astype(bf16)

    def halo_copies(device):
        return [
            remote(
                source,
                target,
                halo_sem.at[0, index],
                halo_sem.at[1, index],
                device,
            )
            for index, (source, target) in enumerate(
                [
                    (pairs.at[pl.ds(rows - WINDOW, WINDOW)], halo_pairs),
                    (pool_span.at[pl.ds(WINDOW + rows - HALO_ROWS, HALO_ROWS)], halo_pool),
                ]
            )
        ]

    next_plane = {"sp": place.sp + 2, "tp": 2 * x}
    sends_up = (c == 1) & place.passes(0)
    finalise(rows // tile - 1)

    @pl.when(c == 0)
    def _():
        for copy in halo_copies({"tp": 2 * x + 1}):
            copy.start()

    @pl.when(sends_up)
    def _():
        for copy in halo_copies(next_plane):
            copy.start()

    @pl.loop(0, rows // tile - 1)
    def _(index):
        finalise(index)

    def pool(block):
        held = aligned(block, WINDOW)
        span_rows = pool_span[pl.ds(pl.multiple_of(block * WINDOW, WINDOW), 2 * WINDOW)]
        running = dot(band[...], span_rows)
        offset = lax.broadcasted_iota(jnp.int32, (WINDOW, 1), 0)
        position = (seq * rows + block * WINDOW + offset).astype(f32)
        counted = jnp.minimum(position + 1.0, span)
        difference = (running / counted - span_rows[WINDOW:].astype(f32)).astype(bf16)
        mapped = dot(difference, pool_maps[...]) * pool_scales[...]
        scale = lax.rsqrt(jnp.mean(mapped * mapped, axis=-1, keepdims=True) + epsilon)
        mixed[held, pl.ds(0, branch)] = (mapped * scale).astype(bf16)

    def attend(block):
        held = aligned(block, WINDOW)
        both = pl.ds(pl.multiple_of(block * WINDOW, WINDOW), 2 * WINDOW)
        key_pair = jnp.concatenate([keys_low[both], keys_high[both]], axis=0)
        value_pair = jnp.concatenate([values_low[both], values_high[both]], axis=0)
        parts, squares = [], None
        for pair in range(pairs_of_heads):
            lanes = pl.ds(pair * LANES, LANES)
            scores = lax.dot_general(
                queries[held, lanes],
                key_pair,
                (((1,), (1,)), ((), ())),
                preferred_element_type=f32,
            )
            weights = jnp.exp(scores + bias[pl.ds(pair * WINDOW, WINDOW)]).astype(bf16)
            result = dot(weights, value_pair)
            part = result[:, :LANES] / (
                result[:, LANES:] + head_rows[pl.ds(2 + pair, 1), :]
            )
            parts.append(part)
            squares = part * part if squares is None else squares + part * part
        mean = jnp.sum(squares, axis=-1, keepdims=True) * (1.0 / head_columns)
        scale = lax.rsqrt(mean + epsilon)
        for pair, part in enumerate(parts):
            mixed[held, pl.ds(branch + pair * LANES, LANES)] = (part * scale).astype(bf16)

    if out_width % (2 * LANES) == 0:
        units_of = {0: [(1, 0), (2, out_width // 2)], 1: [(1, 0), (2, out_width // 2)]}
        unit_width = out_width // 2
    else:
        units_of = {0: [(1, 0)], 1: [(2, 0)]}
        unit_width = out_width

    step_of = min(unit_width, LANES)

    class Shard:
        def __init__(self, owner, event):
            slot = last.events[event][1]
            self.owner, self.event = owner, event
            self.units = units_of[slot]

        def lanes(self, start, size):
            return pl.ds(pl.multiple_of(self.owner * out_width + start, step_of), size)

        def unit(self, start):
            return self.lanes(start, unit_width)

        def packed(self):
            return aligned(self.owner if len(self.units) == 2 else self.owner // 2, unit_width)

        def copy(self, source, target, sent, landed, device):
            return remote(
                source, target, sum_send.at[sent], sum_recv.at[landed, self.owner], device
            )

        def row_block(self, index, lanes):
            return normed.at[aligned(index, out_rows), lanes]

        def across_x(self, start):
            return self.copy(
                normed.at[aligned(1 - x, 2 * out_rows), self.unit(start)],
                from_x.at[:, self.packed()],
                0,
                0,
                place.along_x(c),
            )

        def across_y(self, start, part=None):
            if part is None:
                held = pl.ds(0, rows)
            else:
                held = aligned(1 - x if part == 0 else x, 2 * out_rows)
            landed = half_recv.at[self.event] if part == 0 else sum_recv.at[1, self.owner]
            return remote(
                normed.at[held, self.unit(start)],
                from_away.at[held, self.packed()],
                sum_send.at[1],
                landed,
                place.along_y(c),
            )

        def to_pair(self):
            lanes = self.lanes(0, out_width)
            return self.copy(
                self.row_block(2 * x + 1 - c, lanes),
                from_pair.at[:, lanes],
                1,
                1,
                place.sibling(),
            )

        def away_final(self, start, core):
            lanes = self.unit(start)
            return self.copy(
                self.row_block(2 * x + core, lanes),
                from_last.at[:, lanes],
                2 + core,
                2,
                place.along_y(core),
            )

        def home_final(self, start, core):
            lanes = self.unit(start)
            return self.copy(
                self.row_block(2 * (1 - x) + core, lanes),
                from_last.at[:, lanes],
                2 + core,
                3,
                place.along_x(core),
            )

        def terms(self, least, end):
            lanes = self.lanes(0, out_width)

            @pl.loop(least, end)
            def _(index):
                held = aligned((2 * (1 - x) + index) % 4, out_rows)
                normed[held, lanes] = dot(mixed[held, :], last_weights[self.owner]).astype(bf16)

        def go_across(self, part):
            for scheme, start in self.units:
                if scheme == 1:
                    if part != 1:
                        self.across_x(start).start()
                else:

                    @pl.when(away)
                    def _():
                        self.across_y(start, part).start()

        def first(self):
            self.terms(0, 4)
            self.go_across(None)

        def first_rows(self):
            self.terms(0, 2)
            self.go_across(0)

        def other_rows(self):
            self.terms(2, 4)
            self.go_across(1)

        def second(self):
            for scheme, start in self.units:
                lanes = self.unit(start)
                if scheme == 1:
                    self.across_x(start).wait_recv()
                    held = aligned(x, 2 * out_rows)
                    normed[held, lanes] = (
                        normed[held, lanes].astype(f32) + from_x[:, self.packed()].astype(f32)
                    ).astype(bf16)

                    @pl.when(away)
                    def _():
                        for core in range(2):
                            self.away_final(start, core).start()
                else:

                    @pl.when(home)
                    def _():
                        if self.event < 2:
                            self.across_y(start, 0).wait_recv()
                            self.across_y(start, 1).wait_recv()
                        else:
                            self.across_y(start).wait_recv()

                        @pl.loop(0, 4)
                        def _(index):
                            held = aligned(index, out_rows)
                            normed[held, lanes] = (
                                normed[held, lanes].astype(f32)
                                + from_away[held, self.packed()].astype(f32)
                            ).astype(bf16)

                        for core in range(2):
                            self.home_final(start, core).start()

            @pl.when(home)
            def _():
                self.to_pair().start()

        def third(self):
            lanes = self.lanes(0, out_width)
            for scheme, start in self.units:
                if scheme == 1:
                    self.away_final(start, 0).wait_recv()
                else:
                    self.home_final(start, 0).wait_recv()

            @pl.when(home)
            def _():
                out[:, lanes] = (
                    normed[aligned(2 * x + c, out_rows), lanes].astype(f32)
                    + from_last[:, lanes].astype(f32)
                ).astype(bf16)

            @pl.when(away)
            def _():
                self.to_pair().wait_recv()
                out[:, lanes] = (
                    from_pair[:, lanes].astype(f32) + from_last[:, lanes].astype(f32)
                ).astype(bf16)

    def each(event, stage):
        step, slot = last.events[event]

        @pl.loop(0, 1 if step == 0 else 2)
        def _(way):
            plane = z + (2 * way - 1) * step

            @pl.when((plane >= 0) & (plane < place.planes))
            def _():
                getattr(Shard(2 * plane + slot, event), stage)()

    def take_halo():
        top = pl.ds(0, WINDOW)

        @pl.when(seq > 0)
        def _():
            for copy in halo_copies(next_plane):
                copy.wait_recv()
            spread(halo_pairs[...].astype(f32), top, 1.0)
            pool_span[pl.ds(WINDOW - HALO_ROWS, HALO_ROWS)] = halo_pool[...]

        @pl.when(seq == 0)
        def _():
            for ref in (keys_low, keys_high, values_low, values_high):
                ref[top] = jnp.zeros((WINDOW, ref.shape[1]), bf16)

    half = blocks // 2

    def mix_half(side):
        @pl.loop(0, half)
        def _(index):
            block = side * half + (index + 1) % half

            @pl.when(block == 0)
            def _():
                take_halo()

            pool(block)
            attend(block)

    mix_half(1 - x)
    last.share_taken()
    last.pass_on(0, 1 - y)
    last.done = 2
    last.taken_pair().wait_recv()
    for event in range(2):
        each(event, "first_rows")
    mix_half(x)
    for event in range(2):
        each(event, "other_rows")

    total = len(last.events)

    def all_sent(index, whole):
        remote(
            whole, whole, sum_send.at[index], sum_recv.at[0, 0], place.sibling()
        ).wait_send()

    def early_sends():
        def tokens_sent(index):
            remote(
                tokens, tokens, send_sem.at[index], near_sem.at[0, 0], place.sibling()
            ).wait_send()

        tokens_sent(1)
        tokens_sent(2)

        @pl.when(away)
        def _():
            tokens_sent(0)

        @pl.when(home)
        def _():
            for copy in table_copies():
                copy.wait_send()

        @pl.when((c == 0) | sends_up)
        def _():
            for copy in halo_copies(next_plane):
                copy.wait_send()

        first.sent_edges(first_gave)
        last.sent_edges(last_gave)
        for event in range(total):
            first.sent(event)
        if place.planes > 1:
            first.shared(first_weights.at[pl.ds(0, (place.planes - 1) * depth)])

    for event, (step, slot) in enumerate(last.events):
        last.upto(event)
        if step > 0:
            last.complete(step, slot)
            each(event, "first")
        if event > 0:
            each(event - 1, "second")
        if event > 2:
            each(event - 3, "third")
        if event == min(3, total - 1):
            early_sends()
        if event > 3:
            last.sent(event - 4)
    each(total - 1, "second")
    for event in range(max(0, total - 3), total):
        each(event, "third")
    for event in range(max(0, total - 4), total):
        last.sent(event)
    if place.planes > 1:
        last.shared(last_weights.at[pl.ds(0, place.planes - 1)])
    all_sent(0, from_x)

    @pl.when(home)
    def _():
        all_sent(1, from_pair)

    @pl.when(away)
    def _():
        all_sent(1, from_away)

    for core in range(2):
        all_sent(2 + core, from_last.at[:, pl.ds(0, from_x.shape[1])])


def layer(tokens, w_pool_in, w_query, w_key_t, w_value_t, pool_map, w_out, *rows_in):
    count = lax.axis_size("sp")
    rows, width = tokens.shape
    depth, branch = w_pool_in.shape
    head_columns = w_query.shape[1]
    features = width * lax.axis_size("tp")
    mix, out_width = w_out.shape
    out_rows = rows // lax.axis_size("tp")
    out_columns = count * out_width
    sums = branch + head_columns + LANES
    dma = pltpu.SemaphoreType.DMA
    planes = count // 2
    hbm = pl.BlockSpec(memory_space=pltpu.HBM)
    flops = 2 * rows * features * sums + 2 * rows * mix * out_columns
    return pl.pallas_call(
        functools.partial(layer_kernel, count),
        out_shape=pltpu.VMEM((out_rows, out_columns), bf16),
        in_specs=[hbm] * 12,
        out_specs=pl.BlockSpec(memory_space=pltpu.VMEM),
        scratch_shapes=[
            pltpu.VMEM((rows, features), bf16),
            pltpu.VMEM((features, sums), bf16),
            pltpu.VMEM((count, mix, out_width), bf16),
            pltpu.VMEM((depth, sums), bf16),
            pltpu.VMEM((rows, sums), f32),
            pltpu.VMEM((rows, head_columns), bf16),
            pltpu.VMEM((WINDOW + rows, LANES), bf16),
            pltpu.VMEM((WINDOW + rows, LANES), bf16),
            pltpu.VMEM((WINDOW + rows, 2 * LANES), bf16),
            pltpu.VMEM((WINDOW + rows, 2 * LANES), bf16),
            pltpu.VMEM((WINDOW + rows, branch), bf16),
            pltpu.VMEM((rows, LANES), bf16),
            pltpu.VMEM((rows, mix), bf16),
            pltpu.VMEM((head_columns // LANES * WINDOW, 4 * WINDOW), f32),
            pltpu.VMEM((WINDOW, 2 * WINDOW), bf16),
            pltpu.VMEM((2 * LANES, 2 * LANES), bf16),
            pltpu.VMEM((WINDOW, LANES), bf16),
            pltpu.VMEM((HALO_ROWS, branch), bf16),
            pltpu.VMEM((2 * out_rows, out_columns // 2), bf16),
            pltpu.VMEM((out_rows, out_columns), bf16),
            pltpu.VMEM((rows, out_columns // 2), bf16),
            pltpu.VMEM((out_rows, out_columns), bf16),
            pltpu.VMEM((2 * HEAD_DIM, depth), bf16),
            pltpu.VMEM((branch, branch), bf16),
            pltpu.VMEM((1, features), f32),
            pltpu.VMEM((1, branch), f32),
            pltpu.VMEM((1, HEAD_DIM), f32),
            pltpu.VMEM((1, HEAD_DIM), f32),
            pltpu.VMEM((1, GROUP), f32),
            pltpu.VMEM((8, LANES), f32),
            dma((12,)),
            dma((3, 2, max(1, planes - 1), 2)),
            dma((3, 2, max(1, planes - 1), 2)),
            dma((8,)),
            dma((8,)),
            dma((2, TOKEN_CHUNKS)),
            dma((2, TOKEN_CHUNKS)),
            dma((3,)),
            dma((2, TOKEN_CHUNKS)),
            dma((2, 3)),
            dma((2, 2)),
            dma((4,)),
            dma((4, count)),
            dma((2,)),
        ],
        compiler_params=pltpu.CompilerParams(
            collective_id=0, has_side_effects=True, vmem_limit_bytes=60 * 1024 * 1024
        ),
        cost_estimate=pl.CostEstimate(
            flops=flops, bytes_accessed=4 * rows * width, transcendentals=0
        ),
    )(tokens, w_pool_in, w_query, w_key_t, w_value_t, pool_map, w_out, *rows_in)


def local(
    tokens,
    norm_gain,
    w_pool_in,
    w_query,
    w_key,
    w_value,
    pool_map,
    pool_scale,
    q_gain,
    k_gain,
    sinks,
    w_out,
):
    return layer(
        tokens,
        w_pool_in,
        w_query,
        w_key.T,
        w_value.T,
        pool_map[0],
        w_out,
        norm_gain[None],
        pool_scale[None],
        q_gain[None],
        k_gain[None],
        sinks[None],
    )


def solution(mesh):
    in_specs = (
        P("sp", "tp"),
        P(),
        P("sp", "tp"),
        P("sp", "tp"),
        P("sp", "tp"),
        P("sp", "tp"),
        P("tp", None, None),
        P("tp"),
        P(),
        P(),
        P("tp"),
        P("tp", "sp"),
    )
    out_specs = P(("sp", "tp"), None)
    return jax.shard_map(local, mesh=mesh, in_specs=in_specs, out_specs=out_specs, check_vma=False)
```

```python
import functools

import jax
import jax.numpy as jnp
from jax import lax
from jax.experimental import pallas as pl
from jax.experimental.pallas import tpu as pltpu
from jax.sharding import PartitionSpec as P

HEAD_DIM = 64
GROUP = 8
WINDOW = 128
Q_HEADS = 32
LANES = 128
TOKEN_CHUNKS = 4
HALO_ROWS = 16
MASKED = -1e30

epsilon = 1e-06
bf16, f32 = jnp.bfloat16, jnp.float32


def aligned(index, size):
    return pl.ds(pl.multiple_of(index * size, size), size)


def dot(left, right):
    return jnp.dot(left, right, preferred_element_type=f32)


class Place:
    def __init__(self, count):
        self.planes = count // 2
        self.sp, self.tp = lax.axis_index("sp"), lax.axis_index("tp")
        self.z, self.y = self.sp // 2, self.sp % 2
        self.x, self.c = self.tp // 2, self.tp % 2
        self.home = self.y == self.c
        self.rows_of, self.group = 2 * self.z + self.c, 2 * self.x + self.y

    def sibling(self):
        return {"tp": 2 * self.x + 1 - self.c}

    def along_x(self, core):
        return {"tp": 2 * (1 - self.x) + core}

    def along_y(self, core):
        return {"sp": 2 * self.z + 1 - self.y, "tp": 2 * self.x + core}

    def along_z(self, way):
        return {"sp": self.sp + 2 - 4 * way}

    def source(self, way, steps):
        return self.z - steps if way == 0 else self.z + steps

    def has(self, way, steps):
        return self.z >= steps if way == 0 else self.z + steps < self.planes

    def passes(self, way):
        return self.z + 1 < self.planes if way == 0 else self.z > 0


def remote(source, target, send_sem, recv_sem, device):
    return pltpu.make_async_remote_copy(
        src_ref=source,
        dst_ref=target,
        send_sem=send_sem,
        recv_sem=recv_sem,
        device_id=device,
        device_id_type=pl.DeviceIdType.MESH,
    )


class Chain:
    def __init__(self, place, shard, own_first, sems, cuts=1):
        self.place, self.shard, self.own_first = place, shard, own_first
        self.up_send, self.up_recv, self.pair_recv, self.edge = sems
        self.cuts = cuts if place.planes > 2 else 1
        self.events = [(step, slot, None) for step in range(place.planes) for slot in range(2)]
        if self.cuts > 1:
            step, slot, _ = self.events.pop()
            self.events += [(step, slot, cut) for cut in range(cuts)]
        self.done, self.whole = 0, set()

    def cuts_of(self, step, slot):
        if self.cuts > 1 and step == self.place.planes - 1 and slot == 1:
            return range(self.cuts)
        return [None]

    def block(self, plane, slot, half, cut=None):
        side = slot if not self.own_first else (self.place.y + slot) % 2
        if cut is None:
            return self.shard(2 * plane + side, half)
        return self.shard(2 * plane + side, half, cut)

    def hop(self, way, step, slot, cut=None):
        held = self.block(self.place.source(way, step), slot, self.place.c, cut)
        return remote(
            held,
            held,
            self.edge.at[8 + way] if cut == 1 else self.up_send.at[way, step, slot],
            self.edge.at[10 + way] if cut == 1 else self.up_recv.at[way, step, slot],
            self.place.along_z(way),
        )

    def hops(self, way, step, slot):
        return [
            self.hop(way, step, slot, cut)
            for cut in (self.cuts_of(step + 1, slot) if step > 0 else [None])
        ]

    def pair(self, way, step, slot, cut=None):
        held = self.block(self.place.source(way, step), slot, self.place.c, cut)
        return remote(
            held,
            held,
            self.edge.at[7],
            self.edge.at[12 + way] if cut == 1 else self.pair_recv.at[way, step - 1, slot],
            self.place.sibling(),
        )

    def own_pair(self):
        held = self.shard(self.place.sp, None)
        return remote(
            held,
            held,
            self.edge.at[0],
            self.edge.at[1],
            self.place.sibling(),
        )

    def give(self, half, source):
        return remote(
            source,
            self.shard(self.place.sp, half),
            self.edge.at[2 + half],
            self.edge.at[4],
            self.place.along_y(half),
        )

    def taken(self):
        held = self.shard(2 * self.place.z + 1 - self.place.y, self.place.c)
        return remote(held, held, self.edge.at[2], self.edge.at[4], self.place.along_y(0))

    def pass_on(self, step, slot):
        for way in range(2):

            @pl.when(self.place.passes(way))
            def _(way=way):
                for copy in self.hops(way, step, slot):
                    copy.start()

    def share_own(self):
        @pl.when(self.place.home)
        def _():
            self.own_pair().start()

        @pl.when(jnp.logical_not(self.place.home))
        def _():
            self.own_pair().wait_recv()

    def share_taken(self):
        self.taken().wait_recv()
        held = self.shard(2 * self.place.z + 1 - self.place.y, self.place.c)
        self.other_pair(held).start()

    def other_pair(self, held):
        return remote(
            held, held, self.edge.at[5], self.edge.at[6], self.place.sibling()
        )

    def taken_pair(self):
        return self.other_pair(
            self.shard(2 * self.place.z + 1 - self.place.y, self.place.c)
        )

    def advance(self):
        step, slot, cut = self.events[self.done]
        self.done += 1
        if step == 0:
            if self.own_first:
                if slot == 0:
                    self.share_own()
                else:
                    self.share_taken()
            if self.place.planes > 1:
                self.pass_on(0, slot)
            return
        for way in range(2):

            @pl.when(self.place.has(way, step))
            def _(way=way):
                self.hop(way, step - 1, slot, cut).wait_recv()
                self.pair(way, step, slot, cut).start()
                if step + 1 < self.place.planes:

                    @pl.when(self.place.passes(way))
                    def _():
                        for copy in self.hops(way, step, slot):
                            copy.start()

    def upto(self, event):
        while self.done <= min(event, len(self.events) - 1):
            self.advance()

    def complete(self, step, slot, cut=None):
        if (step, slot, cut) in self.whole:
            return
        self.whole.add((step, slot, cut))
        if step == 0:
            if slot == 1:
                self.taken_pair().wait_recv()
            return
        for way in range(2):

            @pl.when(self.place.has(way, step))
            def _(way=way):
                self.pair(way, step, slot, cut).wait_recv()

    def sent_edges(self, gave):
        @pl.when(self.place.home)
        def _():
            self.own_pair().wait_send()

        @pl.when(jnp.logical_not(self.place.home))
        def _():
            for half in range(2):
                gave(half).wait_send()

        self.taken_pair().wait_send()

    def sent(self, event):
        step, slot, _ = self.events[event]
        place = self.place
        if step + 1 < place.planes:
            for way in range(2):

                @pl.when(place.has(way, step) & place.passes(way))
                def _(way=way):
                    for copy in self.hops(way, step, slot):
                        copy.wait_send()

    def shared(self, whole):
        remote(
            whole, whole, self.edge.at[7], self.edge.at[0], self.place.sibling()
        ).wait_send()


def layer_kernel(
    count,
    tokens,
    w_pool_in,
    w_query,
    w_key_t,
    w_value_t,
    pool_map,
    w_out,
    gain_in,
    pool_scale_in,
    q_gain_in,
    k_gain_in,
    sinks_in,
    out,
    normed,
    first_weights,
    last_weights,
    own_shard,
    acc,
    queries,
    keys_low,
    keys_high,
    values_low,
    values_high,
    pool_span,
    pairs,
    mixed,
    bias,
    band,
    ones_block,
    halo_pairs,
    halo_pool,
    from_x,
    from_pair,
    from_away,
    from_last,
    key_value,
    pool_maps,
    gain,
    pool_scales,
    q_gain,
    k_gain,
    sinks,
    head_rows,
    local_sem,
    first_sems,
    last_sems,
    first_edge,
    last_edge,
    near_sem,
    far_sem,
    send_sem,
    relay_sem,
    table_sem,
    halo_sem,
    sum_send,
    sum_recv,
    half_recv,
):
    place = Place(count)
    x, y, z, c = place.x, place.y, place.z, place.c
    home, away = place.home, jnp.logical_not(place.home)
    me, seq = place.group, place.rows_of
    rows, width = tokens.shape
    depth, branch = w_pool_in.shape
    head_columns = w_query.shape[1]
    mid = branch + head_columns
    piece = rows // TOKEN_CHUNKS
    blocks = rows // WINDOW
    out_rows = out.shape[0]
    out_width = w_out.shape[1]
    mix = w_out.shape[0]
    pairs_of_heads = head_columns // LANES

    barrier = pltpu.get_barrier_semaphore()

    def greet(device):
        pl.semaphore_signal(
            barrier, inc=1, device_id=device, device_id_type=pl.DeviceIdType.MESH
        )

    for way in range(2):

        @pl.when(place.passes(way))
        def _(way=way):
            greet(place.along_z(way))

    for core in range(2):
        greet(place.along_x(core))
        greet(place.along_y(core))
    greet(place.sibling())
    greetings = 5 + jnp.where(place.passes(0), 1, 0) + jnp.where(place.passes(1), 1, 0)

    def first_shard(owner, half):
        if half is None:
            return first_weights.at[aligned(owner, depth)]
        size = depth // 2
        return first_weights.at[pl.ds(pl.multiple_of(owner * depth + half * size, size), size)]

    def last_shard(owner, half, cut=None):
        if half is None:
            return last_weights.at[owner]
        if cut is not None:
            size = out_width // 2
            return last_weights.at[owner, aligned(half, mix // 2), pl.ds((1 - cut) * size, size)]
        return last_weights.at[owner, aligned(half, mix // 2)]

    first = Chain(
        place, first_shard, True, [first_sems.at[i] for i in range(3)] + [first_edge]
    )
    halves = out_width % (2 * LANES) == 0
    last = Chain(
        place,
        last_shard,
        False,
        [last_sems.at[i] for i in range(3)] + [last_edge],
        2 if halves else 1,
    )

    def local_copy(index, source, target):
        return pltpu.make_async_copy(source, target, local_sem.at[index])

    own_rows = aligned(place.sp, depth)
    small = [
        local_copy(0, w_key_t, key_value.at[pl.ds(0, HEAD_DIM)]),
        local_copy(1, w_value_t, key_value.at[pl.ds(HEAD_DIM, HEAD_DIM)]),
        local_copy(2, gain_in, gain),
        local_copy(3, q_gain_in, q_gain),
        local_copy(4, k_gain_in, k_gain),
    ]

    def shard_copies(target):
        return [
            local_copy(5, w_pool_in, target.at[:, pl.ds(0, branch)]),
            local_copy(6, w_query, target.at[:, pl.ds(branch, head_columns)]),
        ]

    def home_copies():
        return [
            local_copy(7, tokens, normed.at[:, aligned(place.tp, width)]),
            local_copy(8, w_out, last_weights.at[place.sp]),
            local_copy(9, pool_map, pool_maps),
            local_copy(10, pool_scale_in, pool_scales),
            local_copy(11, sinks_in, sinks),
        ]

    for copy in small[:2]:
        copy.start()

    @pl.when(home)
    def _():
        for copy in shard_copies(first_weights.at[own_rows]) + home_copies():
            copy.start()

    @pl.when(away)
    def _():
        for copy in shard_copies(own_shard):
            copy.start()

    for copy in small[2:]:
        copy.start()
    small[0].wait()
    small[1].wait()
    pair_columns = key_value[...].astype(f32).T.astype(bf16)

    def table_copies():
        return [
            remote(
                source,
                target,
                table_sem.at[0, index],
                table_sem.at[1, index],
                place.sibling(),
            )
            for index, (source, target) in enumerate(
                [(pool_map, pool_maps), (pool_scale_in, pool_scales), (sinks_in, sinks)]
            )
        ]

    def first_gave(half):
        return first.give(half, own_shard.at[pl.ds(half * (depth // 2), depth // 2)])

    def last_gave(half):
        return last.give(half, w_out.at[pl.ds(half * (mix // 2), mix // 2)])

    @pl.when(home)
    def _():
        first_weights[own_rows, pl.ds(mid, LANES)] = pair_columns
        for copy in shard_copies(first_weights.at[own_rows]):
            copy.wait()

    @pl.when(away)
    def _():
        own_shard[:, pl.ds(mid, LANES)] = pair_columns
        for copy in shard_copies(own_shard):
            copy.wait()

    pl.semaphore_wait(barrier, greetings)

    @pl.when(away)
    def _():
        for half in range(2):
            first_gave(half).start()

    def token_rows(chunk):
        return pl.ds(chunk * piece, piece)

    def landing(chunk, side, core):
        owner = 2 * (jnp.where(x == 0, side, 1 - side)) + core
        return normed.at[token_rows(chunk), aligned(owner, width)]

    def to_sibling(chunk):
        return remote(
            tokens.at[token_rows(chunk)],
            landing(chunk, 0, c),
            send_sem.at[0],
            near_sem.at[c, chunk],
            place.sibling(),
        )

    def to_x(chunk):
        return remote(
            tokens.at[token_rows(chunk)],
            landing(chunk, 0, c),
            send_sem.at[1],
            far_sem.at[c, chunk],
            place.along_x(y),
        )

    def to_y(chunk):
        return remote(
            tokens.at[token_rows(chunk)],
            landing(chunk, 0, c),
            send_sem.at[2],
            near_sem.at[c, chunk],
            place.along_y(y),
        )

    def by_x(chunk, core):
        return core == 1 or chunk == 1

    def relay(chunk, core):
        if by_x(chunk, core):
            held = landing(chunk, 0, core)
            device = place.along_x(c)
        else:
            held = landing(chunk, 1, core)
            device = place.along_y(c)
        return remote(
            held, held, relay_sem.at[core, chunk], far_sem.at[core, chunk], device
        )

    def near_wait(chunk, core):
        held = landing(chunk, 0, core)
        remote(
            held, held, send_sem.at[0], near_sem.at[core, chunk], place.sibling()
        ).wait_recv()

    def far_wait(chunk, core):
        held = landing(chunk, 1, core)
        remote(
            held, held, send_sem.at[0], far_sem.at[core, chunk], place.sibling()
        ).wait_recv()

    ahead = 3

    def send_tokens(chunk):
        to_x(chunk).start()
        to_y(chunk).start()

    @pl.when(home)
    def _():
        for copy in table_copies():
            copy.start()

    first.upto(0)
    for chunk in range(ahead):
        to_x(chunk).start()

    @pl.when(away)
    def _():
        for chunk in range(TOKEN_CHUNKS):
            to_sibling(chunk).start()
        for chunk in range(ahead):
            to_y(chunk).start()

    span = 2.0 * jnp.exp2(me.astype(f32))
    row = lax.broadcasted_iota(jnp.int32, (WINDOW, 2 * WINDOW), 0)
    column = lax.broadcasted_iota(jnp.int32, (WINDOW, 2 * WINDOW), 1)
    distance = (row + WINDOW - column).astype(f32)
    band[...] = jnp.where((distance >= 0.0) & (distance < span), 1.0, 0.0).astype(bf16)
    allowed = (distance >= 0.0) & (distance < float(WINDOW))
    for pair in range(pairs_of_heads):
        for half in range(2):
            head = (me * GROUP + 2 * pair + half + 1).astype(f32)
            slope = jnp.exp2(jnp.full((WINDOW, 2 * WINDOW), -8.0 / Q_HEADS, f32) * head)
            bias[pl.ds(pair * WINDOW, WINDOW), pl.ds(half * 2 * WINDOW, 2 * WINDOW)] = jnp.where(
                allowed, -slope * distance, MASKED
            )
    block_row = lax.broadcasted_iota(jnp.int32, (2 * LANES, 2 * LANES), 0) // HEAD_DIM
    block_column = lax.broadcasted_iota(jnp.int32, (2 * LANES, 2 * LANES), 1) // HEAD_DIM
    ones_block[...] = jnp.where(block_row == block_column, 1.0, 0.0).astype(bf16)
    pool_span[pl.ds(0, WINDOW)] = jnp.zeros((WINDOW, branch), bf16)

    acc[...] = jnp.zeros(acc.shape, f32)
    strip = 32

    def normalise(chunk):
        @pl.loop(0, piece // strip)
        def _(index):
            held = pl.ds(pl.multiple_of(chunk * piece + index * strip, strip), strip)
            values = normed[held].astype(f32)
            scale = lax.rsqrt(jnp.mean(values * values, axis=-1, keepdims=True) + epsilon)
            normed[held] = (values * scale * gain[...]).astype(bf16)

    lane = lax.broadcasted_iota(jnp.int32, (1, LANES), 1)
    low = lane < HEAD_DIM
    for copy in small[2:]:
        copy.wait()

    @pl.when(home)
    def _():
        for copy in home_copies():
            copy.wait()
        last.own_pair().start()

    @pl.when(away)
    def _():
        for copy in table_copies():
            copy.wait_recv()

    head_rows[...] = jnp.zeros(head_rows.shape, f32)
    head_rows[pl.ds(0, 1), pl.ds(0, HEAD_DIM)] = q_gain[...] * HEAD_DIM**-0.5
    head_rows[pl.ds(1, 1), pl.ds(0, HEAD_DIM)] = k_gain[...]
    once = head_rows[pl.ds(0, 1), :]
    head_rows[pl.ds(0, 1), :] = once + pltpu.roll(once, HEAD_DIM, 1)
    for pair in range(pairs_of_heads):
        one, two = sinks[:, 2 * pair : 2 * pair + 1], sinks[:, 2 * pair + 1 : 2 * pair + 2]
        head_rows[pl.ds(2 + pair, 1), :] = jnp.exp(
            jnp.where(low, jnp.broadcast_to(one, (1, LANES)), jnp.broadcast_to(two, (1, LANES)))
        )

    tile = piece

    def multiply(chunks, steps):
        @pl.loop(steps[0], steps[1])
        def _(step):
            for way in range(2):

                @pl.when(place.has(way, step) & (step + way > 0))
                def _(way=way):
                    block = aligned(place.source(way, step), 2 * depth)

                    size = tile * (2 if (chunks[0] | chunks[1]) % 2 == 0 else 1)

                    @pl.loop(chunks[0] * tile // size, chunks[1] * tile // size)
                    def _(index):
                        held = aligned(index, size)
                        acc[held] += dot(normed[held, block], first_weights[block, :])

    class Progress:
        rows, steps = 0, 0

    def catch_up(chunks, steps):
        if steps > Progress.steps:
            for step in range(Progress.steps, steps):
                for slot in range(2):
                    first.complete(step, slot)
            if Progress.rows > 0:
                multiply((0, Progress.rows), (Progress.steps, steps))
            Progress.steps = steps
        if chunks > Progress.rows:
            if steps > 0:
                multiply((Progress.rows, chunks), (0, steps))
            Progress.rows = chunks

    def settle(chunk):
        for core in range(2):

            @pl.when(away if by_x(chunk, core) else home)
            def _(core=core):
                relay(chunk, core).wait_send()

        normalise(chunk)

    first.upto(1)
    first.complete(0, 1)

    @pl.when(home)
    def _():
        for chunk in range(ahead):
            to_y(chunk).start()

    events = len(first.events)

    def pass_tokens(chunk):
        @pl.when(home)
        def _():
            for core in range(2):
                far_wait(chunk, core)
                if not by_x(chunk, core):
                    relay(chunk, core).start()
            near_wait(chunk, 1 - c)

        @pl.when(away)
        def _():
            for core in range(2):
                near_wait(chunk, core)
                if by_x(chunk, core):
                    relay(chunk, core).start()

        if chunk + ahead < TOKEN_CHUNKS:
            send_tokens(chunk + ahead)

    def use_tokens(chunk):
        @pl.when(away)
        def _():
            for core in range(2):
                far_wait(chunk, core)
            if chunk == TOKEN_CHUNKS - 1:
                for half in range(2):
                    last_gave(half).start()

        settle(chunk)
        known = first.done // 2
        if chunk == TOKEN_CHUNKS - 1:
            first.upto(events - 1)
        catch_up(chunk + 1, known)

    for chunk in range(TOKEN_CHUNKS):
        first.upto((chunk + 3) * events // 8 - 1)
        pass_tokens(chunk)
        if chunk > 1:
            use_tokens(chunk - 2)

    @pl.when(away)
    def _():
        last.own_pair().wait_recv()

    first.upto(7 * events // 8 - 1)
    last.pass_on(0, y)
    for chunk in range(max(0, TOKEN_CHUNKS - 2), TOKEN_CHUNKS):
        use_tokens(chunk)
    catch_up(TOKEN_CHUNKS, place.planes)

    one_low = jnp.where(low, 1.0, 0.0)

    def spread(kv, held, count_scale):
        size = kv.shape[0]
        key_low = jnp.where(low, kv, 0.0)
        value_high = jnp.where(low, 0.0, kv)
        keys_low[held] = key_low.astype(bf16)
        keys_high[held] = pltpu.roll(key_low, HEAD_DIM, 1).astype(bf16)
        ones_low = jnp.broadcast_to(one_low * count_scale, (size, LANES)).astype(bf16)
        ones_high = jnp.broadcast_to((1.0 - one_low) * count_scale, (size, LANES)).astype(bf16)
        values_low[held, pl.ds(0, LANES)] = pltpu.roll(value_high, HEAD_DIM, 1).astype(bf16)
        values_low[held, pl.ds(LANES, LANES)] = ones_low
        values_high[held, pl.ds(0, LANES)] = value_high.astype(bf16)
        values_high[held, pl.ds(LANES, LANES)] = ones_high

    def finalise(index):
        held = aligned(index, tile)
        sums = acc[held].astype(bf16)
        shifted = pl.ds(pl.multiple_of(index * tile + WINDOW, WINDOW), tile)
        pool_span[shifted] = sums[:, :branch]
        kv = sums[:, mid:].astype(f32)
        squares = jnp.where(low, kv * kv, 0.0)
        scale = lax.rsqrt(jnp.sum(squares, axis=-1, keepdims=True) * (1.0 / HEAD_DIM) + epsilon)
        kv = jnp.where(low, kv * scale * head_rows[pl.ds(1, 1), :], kv).astype(bf16)
        pairs[held] = kv
        spread(kv.astype(f32), shifted, 1.0)
        wide = 2 * LANES
        gain_row = head_rows[pl.ds(0, 1), :]
        query_gain = jnp.concatenate([gain_row, gain_row], axis=1)
        for start in range(0, head_columns, wide):
            query = sums[:, branch + start : branch + start + wide].astype(f32)
            square = query * query
            upper = square.astype(bf16)
            lower = (square - upper.astype(f32)).astype(bf16)
            total = dot(upper, ones_block[...]) + dot(lower, ones_block[...])
            scale = lax.rsqrt(total * (1.0 / HEAD_DIM) + epsilon)
            queries[held, pl.ds(start, wide)] = (
                query * scale * query_gain
            ).astype(bf16)

    def halo_copies(device):
        return [
            remote(
                source,
                target,
                halo_sem.at[0, index],
                halo_sem.at[1, index],
                device,
            )
            for index, (source, target) in enumerate(
                [
                    (pairs.at[pl.ds(rows - WINDOW, WINDOW)], halo_pairs),
                    (pool_span.at[pl.ds(WINDOW + rows - HALO_ROWS, HALO_ROWS)], halo_pool),
                ]
            )
        ]

    next_plane = {"sp": place.sp + 2, "tp": 2 * x}
    sends_up = (c == 1) & place.passes(0)
    finalise(rows // tile - 1)

    @pl.when(c == 0)
    def _():
        for copy in halo_copies({"tp": 2 * x + 1}):
            copy.start()

    @pl.when(sends_up)
    def _():
        for copy in halo_copies(next_plane):
            copy.start()

    @pl.loop(0, rows // tile - 1)
    def _(index):
        finalise(index)

    def pool(block):
        held = aligned(block, WINDOW)
        span_rows = pool_span[pl.ds(pl.multiple_of(block * WINDOW, WINDOW), 2 * WINDOW)]
        running = dot(band[...], span_rows)
        offset = lax.broadcasted_iota(jnp.int32, (WINDOW, 1), 0)
        position = (seq * rows + block * WINDOW + offset).astype(f32)
        counted = jnp.minimum(position + 1.0, span)
        difference = (running / counted - span_rows[WINDOW:].astype(f32)).astype(bf16)
        mapped = dot(difference, pool_maps[...]) * pool_scales[...]
        scale = lax.rsqrt(jnp.mean(mapped * mapped, axis=-1, keepdims=True) + epsilon)
        mixed[held, pl.ds(0, branch)] = (mapped * scale).astype(bf16)

    def attend(block):
        held = aligned(block, WINDOW)
        both = pl.ds(pl.multiple_of(block * WINDOW, WINDOW), 2 * WINDOW)
        key_pair = jnp.concatenate([keys_low[both], keys_high[both]], axis=0)
        value_pair = jnp.concatenate([values_low[both], values_high[both]], axis=0)
        parts, squares = [], None
        for pair in range(pairs_of_heads):
            lanes = pl.ds(pair * LANES, LANES)
            scores = lax.dot_general(
                queries[held, lanes],
                key_pair,
                (((1,), (1,)), ((), ())),
                preferred_element_type=f32,
            )
            weights = jnp.exp(scores + bias[pl.ds(pair * WINDOW, WINDOW)]).astype(bf16)
            result = dot(weights, value_pair)
            part = result[:, :LANES] / (
                result[:, LANES:] + head_rows[pl.ds(2 + pair, 1), :]
            )
            parts.append(part)
            squares = part * part if squares is None else squares + part * part
        mean = jnp.sum(squares, axis=-1, keepdims=True) * (1.0 / head_columns)
        scale = lax.rsqrt(mean + epsilon)
        for pair, part in enumerate(parts):
            mixed[held, pl.ds(branch + pair * LANES, LANES)] = (part * scale).astype(bf16)

    if halves:
        units_of = {0: [(1, 0), (2, out_width // 2)], 1: [(1, 0), (2, out_width // 2)]}
        unit_width = out_width // 2
    else:
        units_of = {0: [(1, 0)], 1: [(2, 0)]}
        unit_width = out_width

    step_of = min(unit_width, LANES)

    class Shard:
        def __init__(self, owner, event):
            slot, self.cut = last.events[event][1:]
            self.owner, self.event = owner, event
            self.units = units_of[slot] if self.cut is None else [units_of[slot][1 - self.cut]]
            self.columns = (0, out_width) if self.cut is None else (self.units[0][1], unit_width)

        def lanes(self, start, size):
            return pl.ds(pl.multiple_of(self.owner * out_width + start, step_of), size)

        def unit(self, start):
            return self.lanes(start, unit_width)

        def packed(self):
            return aligned(self.owner if halves else self.owner // 2, unit_width)

        def copy(self, source, target, sent, landed, device):
            return remote(
                source, target, sum_send.at[sent], sum_recv.at[landed, self.owner], device
            )

        def row_block(self, index, lanes):
            return normed.at[aligned(index, out_rows), lanes]

        def across_x(self, start):
            return self.copy(
                normed.at[aligned(1 - x, 2 * out_rows), self.unit(start)],
                from_x.at[:, self.packed()],
                0,
                0,
                place.along_x(c),
            )

        def across_y(self, start, part=None):
            if part is None:
                held = pl.ds(0, rows)
            else:
                held = aligned(1 - x if part == 0 else x, 2 * out_rows)
            landed = half_recv.at[self.event] if part == 0 else sum_recv.at[1, self.owner]
            return remote(
                normed.at[held, self.unit(start)],
                from_away.at[held, self.packed()],
                sum_send.at[1],
                landed,
                place.along_y(c),
            )

        def to_pair(self):
            lanes = self.lanes(*self.columns)
            return remote(
                self.row_block(2 * x + 1 - c, lanes),
                from_pair.at[:, lanes],
                sum_send.at[1],
                half_recv.at[2] if self.cut == 1 else sum_recv.at[1, self.owner],
                place.sibling(),
            )

        def away_final(self, start, core):
            lanes = self.unit(start)
            return self.copy(
                self.row_block(2 * x + core, lanes),
                from_last.at[:, lanes],
                2 + core,
                2,
                place.along_y(core),
            )

        def home_final(self, start, core):
            lanes = self.unit(start)
            return self.copy(
                self.row_block(2 * (1 - x) + core, lanes),
                from_last.at[:, lanes],
                2 + core,
                3,
                place.along_x(core),
            )

        def terms(self, least, end):
            lanes = self.lanes(*self.columns)

            @pl.loop(least, end)
            def _(index):
                held = aligned((2 * (1 - x) + index) % 4, out_rows)
                value = dot(mixed[held, :], last_weights[self.owner, :, pl.ds(*self.columns)])
                normed[held, lanes] = value.astype(bf16)

        def go_across(self, part):
            for scheme, start in self.units:
                if scheme == 1:
                    if part != 1:
                        self.across_x(start).start()
                else:

                    @pl.when(away)
                    def _():
                        self.across_y(start, part).start()

        def first(self):
            self.terms(0, 4)
            self.go_across(None)

        def first_rows(self):
            self.terms(0, 2)
            self.go_across(0)

        def other_rows(self):
            self.terms(2, 4)
            self.go_across(1)

        def second(self):
            for scheme, start in self.units:
                lanes = self.unit(start)
                if scheme == 1:
                    self.across_x(start).wait_recv()
                    held = aligned(x, 2 * out_rows)
                    normed[held, lanes] = (
                        normed[held, lanes].astype(f32) + from_x[:, self.packed()].astype(f32)
                    ).astype(bf16)

                    @pl.when(away)
                    def _():
                        for core in range(2):
                            self.away_final(start, core).start()
                else:

                    @pl.when(home)
                    def _():
                        if self.event < 2:
                            self.across_y(start, 0).wait_recv()
                            self.across_y(start, 1).wait_recv()
                        else:
                            self.across_y(start).wait_recv()

                        @pl.loop(0, 4)
                        def _(index):
                            held = aligned(index, out_rows)
                            normed[held, lanes] = (
                                normed[held, lanes].astype(f32)
                                + from_away[held, self.packed()].astype(f32)
                            ).astype(bf16)

                        for core in range(2):
                            self.home_final(start, core).start()

            @pl.when(home)
            def _():
                self.to_pair().start()

        def third(self):
            lanes = self.lanes(*self.columns)
            for scheme, start in self.units:
                if scheme == 1:
                    self.away_final(start, 0).wait_recv()
                else:
                    self.home_final(start, 0).wait_recv()

            @pl.when(home)
            def _():
                out[:, lanes] = (
                    normed[aligned(2 * x + c, out_rows), lanes].astype(f32)
                    + from_last[:, lanes].astype(f32)
                ).astype(bf16)

            @pl.when(away)
            def _():
                self.to_pair().wait_recv()
                out[:, lanes] = (
                    from_pair[:, lanes].astype(f32) + from_last[:, lanes].astype(f32)
                ).astype(bf16)

    def each(event, stage):
        step, slot, _ = last.events[event]

        @pl.loop(0, 1 if step == 0 else 2)
        def _(way):
            plane = z + (2 * way - 1) * step

            @pl.when((plane >= 0) & (plane < place.planes))
            def _():
                getattr(Shard(2 * plane + slot, event), stage)()

    def take_halo():
        top = pl.ds(0, WINDOW)

        @pl.when(seq > 0)
        def _():
            for copy in halo_copies(next_plane):
                copy.wait_recv()
            spread(halo_pairs[...].astype(f32), top, 1.0)
            pool_span[pl.ds(WINDOW - HALO_ROWS, HALO_ROWS)] = halo_pool[...]

        @pl.when(seq == 0)
        def _():
            for ref in (keys_low, keys_high, values_low, values_high):
                ref[top] = jnp.zeros((WINDOW, ref.shape[1]), bf16)

    half = blocks // 2

    def mix_half(side):
        @pl.loop(0, half)
        def _(index):
            block = side * half + (index + 1) % half

            @pl.when(block == 0)
            def _():
                take_halo()

            pool(block)
            attend(block)

    mix_half(1 - x)
    last.share_taken()
    last.pass_on(0, 1 - y)
    last.done = 2
    last.taken_pair().wait_recv()
    for event in range(2):
        each(event, "first_rows")
    mix_half(x)
    for event in range(2):
        each(event, "other_rows")

    total = len(last.events)

    def all_sent(index, whole):
        remote(
            whole, whole, sum_send.at[index], sum_recv.at[0, 0], place.sibling()
        ).wait_send()

    def early_sends():
        def tokens_sent(index):
            remote(
                tokens, tokens, send_sem.at[index], near_sem.at[0, 0], place.sibling()
            ).wait_send()

        tokens_sent(1)
        tokens_sent(2)

        @pl.when(away)
        def _():
            tokens_sent(0)

        @pl.when(home)
        def _():
            for copy in table_copies():
                copy.wait_send()

        @pl.when((c == 0) | sends_up)
        def _():
            for copy in halo_copies(next_plane):
                copy.wait_send()

        first.sent_edges(first_gave)
        last.sent_edges(last_gave)
        for event in range(events):
            first.sent(event)
        if place.planes > 1:
            first.shared(first_weights.at[pl.ds(0, (place.planes - 1) * depth)])

    for event, (step, slot, cut) in enumerate(last.events):
        last.upto(event)
        if step > 0:
            last.complete(step, slot, cut)
            each(event, "first")
        waits = False
        if event > 0 and not waits:
            each(event - 1, "second")
        if event > 2:
            each(event - 3, "third")
        if event == min(3, total - 1):
            early_sends()
        if event > 3:
            last.sent(event - 4)
    each(total - 1, "second")
    for event in range(max(0, total - 3), total):
        each(event, "third")
    for event in range(max(0, total - 4), total):
        last.sent(event)
    if place.planes > 1:
        last.shared(last_weights.at[pl.ds(0, place.planes - 1)])
    all_sent(0, from_x)

    @pl.when(home)
    def _():
        all_sent(1, from_pair)

    @pl.when(away)
    def _():
        all_sent(1, from_away)

    for core in range(2):
        all_sent(2 + core, from_last.at[:, pl.ds(0, from_x.shape[1])])


def layer(tokens, w_pool_in, w_query, w_key_t, w_value_t, pool_map, w_out, *rows_in):
    count = lax.axis_size("sp")
    rows, width = tokens.shape
    depth, branch = w_pool_in.shape
    head_columns = w_query.shape[1]
    features = width * lax.axis_size("tp")
    mix, out_width = w_out.shape
    out_rows = rows // lax.axis_size("tp")
    out_columns = count * out_width
    sums = branch + head_columns + LANES
    dma = pltpu.SemaphoreType.DMA
    planes = count // 2
    hbm = pl.BlockSpec(memory_space=pltpu.HBM)
    flops = 2 * rows * features * sums + 2 * rows * mix * out_columns
    return pl.pallas_call(
        functools.partial(layer_kernel, count),
        out_shape=pltpu.VMEM((out_rows, out_columns), bf16),
        in_specs=[hbm] * 12,
        out_specs=pl.BlockSpec(memory_space=pltpu.VMEM),
        scratch_shapes=[
            pltpu.VMEM((rows, features), bf16),
            pltpu.VMEM((features, sums), bf16),
            pltpu.VMEM((count, mix, out_width), bf16),
            pltpu.VMEM((depth, sums), bf16),
            pltpu.VMEM((rows, sums), f32),
            pltpu.VMEM((rows, head_columns), bf16),
            pltpu.VMEM((WINDOW + rows, LANES), bf16),
            pltpu.VMEM((WINDOW + rows, LANES), bf16),
            pltpu.VMEM((WINDOW + rows, 2 * LANES), bf16),
            pltpu.VMEM((WINDOW + rows, 2 * LANES), bf16),
            pltpu.VMEM((WINDOW + rows, branch), bf16),
            pltpu.VMEM((rows, LANES), bf16),
            pltpu.VMEM((rows, mix), bf16),
            pltpu.VMEM((head_columns // LANES * WINDOW, 4 * WINDOW), f32),
            pltpu.VMEM((WINDOW, 2 * WINDOW), bf16),
            pltpu.VMEM((2 * LANES, 2 * LANES), bf16),
            pltpu.VMEM((WINDOW, LANES), bf16),
            pltpu.VMEM((HALO_ROWS, branch), bf16),
            pltpu.VMEM((2 * out_rows, out_columns // 2), bf16),
            pltpu.VMEM((out_rows, out_columns), bf16),
            pltpu.VMEM((rows, out_columns // 2), bf16),
            pltpu.VMEM((out_rows, out_columns), bf16),
            pltpu.VMEM((2 * HEAD_DIM, depth), bf16),
            pltpu.VMEM((branch, branch), bf16),
            pltpu.VMEM((1, features), f32),
            pltpu.VMEM((1, branch), f32),
            pltpu.VMEM((1, HEAD_DIM), f32),
            pltpu.VMEM((1, HEAD_DIM), f32),
            pltpu.VMEM((1, GROUP), f32),
            pltpu.VMEM((8, LANES), f32),
            dma((12,)),
            dma((3, 2, max(1, planes - 1), 2)),
            dma((3, 2, max(1, planes - 1), 2)),
            dma((8,)),
            dma((14,)),
            dma((2, TOKEN_CHUNKS)),
            dma((2, TOKEN_CHUNKS)),
            dma((3,)),
            dma((2, TOKEN_CHUNKS)),
            dma((2, 3)),
            dma((2, 2)),
            dma((4,)),
            dma((4, count)),
            dma((3,)),
        ],
        compiler_params=pltpu.CompilerParams(
            collective_id=0, has_side_effects=True, vmem_limit_bytes=60 * 1024 * 1024
        ),
        cost_estimate=pl.CostEstimate(
            flops=flops, bytes_accessed=4 * rows * width, transcendentals=0
        ),
    )(tokens, w_pool_in, w_query, w_key_t, w_value_t, pool_map, w_out, *rows_in)


def local(
    tokens,
    norm_gain,
    w_pool_in,
    w_query,
    w_key,
    w_value,
    pool_map,
    pool_scale,
    q_gain,
    k_gain,
    sinks,
    w_out,
):
    return layer(
        tokens,
        w_pool_in,
        w_query,
        w_key.T,
        w_value.T,
        pool_map[0],
        w_out,
        norm_gain[None],
        pool_scale[None],
        q_gain[None],
        k_gain[None],
        sinks[None],
    )


def solution(mesh):
    in_specs = (
        P("sp", "tp"),
        P(),
        P("sp", "tp"),
        P("sp", "tp"),
        P("sp", "tp"),
        P("sp", "tp"),
        P("tp", None, None),
        P("tp"),
        P(),
        P(),
        P("tp"),
        P("tp", "sp"),
    )
    out_specs = P(("sp", "tp"), None)
    return jax.shard_map(local, mesh=mesh, in_specs=in_specs, out_specs=out_specs, check_vma=False)
```

```python
import functools

import jax
import jax.numpy as jnp
from jax import lax
from jax.experimental import pallas as pl
from jax.experimental.pallas import tpu as pltpu
from jax.sharding import PartitionSpec as P

HEAD_DIM = 64
GROUP = 8
WINDOW = 128
Q_HEADS = 32
LANES = 128
TOKEN_CHUNKS = 4
HALO_ROWS = 16
MASKED = -1e30

epsilon = 1e-06
bf16, f32 = jnp.bfloat16, jnp.float32


def aligned(index, size):
    return pl.ds(pl.multiple_of(index * size, size), size)


def dot(left, right):
    return jnp.dot(left, right, preferred_element_type=f32)


class Place:
    def __init__(self, count):
        self.planes = count // 2
        self.sp, self.tp = lax.axis_index("sp"), lax.axis_index("tp")
        self.z, self.y = self.sp // 2, self.sp % 2
        self.x, self.c = self.tp // 2, self.tp % 2
        self.home = self.y == self.c
        self.rows_of, self.group = 2 * self.z + self.c, 2 * self.x + self.y

    def sibling(self):
        return {"tp": 2 * self.x + 1 - self.c}

    def along_x(self, core):
        return {"tp": 2 * (1 - self.x) + core}

    def along_y(self, core):
        return {"sp": 2 * self.z + 1 - self.y, "tp": 2 * self.x + core}

    def along_z(self, way):
        return {"sp": self.sp + 2 - 4 * way}

    def source(self, way, steps):
        return self.z - steps if way == 0 else self.z + steps

    def has(self, way, steps):
        return self.z >= steps if way == 0 else self.z + steps < self.planes

    def passes(self, way):
        return self.z + 1 < self.planes if way == 0 else self.z > 0


def remote(source, target, send_sem, recv_sem, device):
    return pltpu.make_async_remote_copy(
        src_ref=source,
        dst_ref=target,
        send_sem=send_sem,
        recv_sem=recv_sem,
        device_id=device,
        device_id_type=pl.DeviceIdType.MESH,
    )


class Chain:
    def __init__(self, place, shard, own_first, sems, cuts=1):
        self.place, self.shard, self.own_first = place, shard, own_first
        self.up_send, self.up_recv, self.pair_recv, self.edge = sems
        self.cuts = cuts if place.planes > 2 else 1
        self.events = [(step, slot, None) for step in range(place.planes) for slot in range(2)]
        if self.cuts > 1:
            step, slot, _ = self.events.pop()
            self.events += [(step, slot, cut) for cut in range(cuts)]
        self.done, self.whole = 0, set()

    def cuts_of(self, step, slot):
        if self.cuts > 1 and step == self.place.planes - 1 and slot == 1:
            return range(self.cuts)
        return [None]

    def block(self, plane, slot, half, cut=None):
        side = slot if not self.own_first else (self.place.y + slot) % 2
        if cut is None:
            return self.shard(2 * plane + side, half)
        return self.shard(2 * plane + side, half, cut)

    def hop(self, way, step, slot, cut=None):
        held = self.block(self.place.source(way, step), slot, self.place.c, cut)
        return remote(
            held,
            held,
            self.edge.at[8 + way] if cut == 1 else self.up_send.at[way, step, slot],
            self.edge.at[10 + way] if cut == 1 else self.up_recv.at[way, step, slot],
            self.place.along_z(way),
        )

    def hops(self, way, step, slot):
        return [
            self.hop(way, step, slot, cut)
            for cut in (self.cuts_of(step + 1, slot) if step > 0 else [None])
        ]

    def pair(self, way, step, slot, cut=None):
        held = self.block(self.place.source(way, step), slot, self.place.c, cut)
        return remote(
            held,
            held,
            self.edge.at[7],
            self.edge.at[12 + way] if cut == 1 else self.pair_recv.at[way, step - 1, slot],
            self.place.sibling(),
        )

    def own_pair(self):
        held = self.shard(self.place.sp, None)
        return remote(
            held,
            held,
            self.edge.at[0],
            self.edge.at[1],
            self.place.sibling(),
        )

    def give(self, half, source):
        return remote(
            source,
            self.shard(self.place.sp, half),
            self.edge.at[2 + half],
            self.edge.at[4],
            self.place.along_y(half),
        )

    def taken(self):
        held = self.shard(2 * self.place.z + 1 - self.place.y, self.place.c)
        return remote(held, held, self.edge.at[2], self.edge.at[4], self.place.along_y(0))

    def pass_on(self, step, slot):
        for way in range(2):

            @pl.when(self.place.passes(way))
            def _(way=way):
                for copy in self.hops(way, step, slot):
                    copy.start()

    def share_own(self):
        @pl.when(self.place.home)
        def _():
            self.own_pair().start()

        @pl.when(jnp.logical_not(self.place.home))
        def _():
            self.own_pair().wait_recv()

    def share_taken(self):
        self.taken().wait_recv()
        held = self.shard(2 * self.place.z + 1 - self.place.y, self.place.c)
        self.other_pair(held).start()

    def other_pair(self, held):
        return remote(
            held, held, self.edge.at[5], self.edge.at[6], self.place.sibling()
        )

    def taken_pair(self):
        return self.other_pair(
            self.shard(2 * self.place.z + 1 - self.place.y, self.place.c)
        )

    def advance(self):
        step, slot, cut = self.events[self.done]
        self.done += 1
        if step == 0:
            if self.own_first:
                if slot == 0:
                    self.share_own()
                else:
                    self.share_taken()
            if self.place.planes > 1:
                self.pass_on(0, slot)
            return
        for way in range(2):

            @pl.when(self.place.has(way, step))
            def _(way=way):
                self.hop(way, step - 1, slot, cut).wait_recv()
                self.pair(way, step, slot, cut).start()
                if step + 1 < self.place.planes:

                    @pl.when(self.place.passes(way))
                    def _():
                        for copy in self.hops(way, step, slot):
                            copy.start()

    def upto(self, event):
        while self.done <= min(event, len(self.events) - 1):
            self.advance()

    def complete(self, step, slot, cut=None):
        if (step, slot, cut) in self.whole:
            return
        self.whole.add((step, slot, cut))
        if step == 0:
            if slot == 1:
                self.taken_pair().wait_recv()
            return
        for way in range(2):

            @pl.when(self.place.has(way, step))
            def _(way=way):
                self.pair(way, step, slot, cut).wait_recv()

    def sent_edges(self, gave):
        @pl.when(self.place.home)
        def _():
            self.own_pair().wait_send()

        @pl.when(jnp.logical_not(self.place.home))
        def _():
            for half in range(2):
                gave(half).wait_send()

        self.taken_pair().wait_send()

    def sent(self, event):
        step, slot, _ = self.events[event]
        place = self.place
        if step + 1 < place.planes:
            for way in range(2):

                @pl.when(place.has(way, step) & place.passes(way))
                def _(way=way):
                    for copy in self.hops(way, step, slot):
                        copy.wait_send()

    def shared(self, whole):
        remote(
            whole, whole, self.edge.at[7], self.edge.at[0], self.place.sibling()
        ).wait_send()


def layer_kernel(
    count,
    tokens,
    w_pool_in,
    w_query,
    w_key_t,
    w_value_t,
    pool_map,
    w_out,
    gain_in,
    pool_scale_in,
    q_gain_in,
    k_gain_in,
    sinks_in,
    out,
    normed,
    first_weights,
    last_weights,
    own_shard,
    acc,
    queries,
    keys_low,
    keys_high,
    values_low,
    values_high,
    pool_span,
    pairs,
    mixed,
    bias,
    band,
    ones_block,
    halo_pairs,
    halo_pool,
    from_x,
    from_pair,
    from_away,
    from_last,
    key_value,
    pool_maps,
    gain,
    pool_scales,
    q_gain,
    k_gain,
    sinks,
    head_rows,
    local_sem,
    first_sems,
    last_sems,
    first_edge,
    last_edge,
    near_sem,
    far_sem,
    send_sem,
    relay_sem,
    table_sem,
    halo_sem,
    sum_send,
    sum_recv,
    half_recv,
):
    place = Place(count)
    x, y, z, c = place.x, place.y, place.z, place.c
    home, away = place.home, jnp.logical_not(place.home)
    me, seq = place.group, place.rows_of
    rows, width = tokens.shape
    depth, branch = w_pool_in.shape
    head_columns = w_query.shape[1]
    mid = branch + head_columns
    piece = rows // TOKEN_CHUNKS
    blocks = rows // WINDOW
    out_rows = out.shape[0]
    out_width = w_out.shape[1]
    mix = w_out.shape[0]
    pairs_of_heads = head_columns // LANES

    barrier = pltpu.get_barrier_semaphore()

    def greet(device):
        pl.semaphore_signal(
            barrier, inc=1, device_id=device, device_id_type=pl.DeviceIdType.MESH
        )

    for way in range(2):

        @pl.when(place.passes(way))
        def _(way=way):
            greet(place.along_z(way))

    for core in range(2):
        greet(place.along_x(core))
        greet(place.along_y(core))
    greet(place.sibling())
    greetings = 5 + jnp.where(place.passes(0), 1, 0) + jnp.where(place.passes(1), 1, 0)

    def first_shard(owner, half):
        if half is None:
            return first_weights.at[aligned(owner, depth)]
        size = depth // 2
        return first_weights.at[pl.ds(pl.multiple_of(owner * depth + half * size, size), size)]

    def last_shard(owner, half, cut=None):
        if half is None:
            return last_weights.at[owner]
        if cut is not None:
            size = out_width // 2
            return last_weights.at[owner, aligned(half, mix // 2), pl.ds((1 - cut) * size, size)]
        return last_weights.at[owner, aligned(half, mix // 2)]

    first = Chain(
        place, first_shard, True, [first_sems.at[i] for i in range(3)] + [first_edge]
    )
    halves = out_width % (2 * LANES) == 0
    last = Chain(
        place,
        last_shard,
        False,
        [last_sems.at[i] for i in range(3)] + [last_edge],
        2 if halves else 1,
    )

    def local_copy(index, source, target):
        return pltpu.make_async_copy(source, target, local_sem.at[index])

    own_rows = aligned(place.sp, depth)
    small = [
        local_copy(0, w_key_t, key_value.at[pl.ds(0, HEAD_DIM)]),
        local_copy(1, w_value_t, key_value.at[pl.ds(HEAD_DIM, HEAD_DIM)]),
        local_copy(2, gain_in, gain),
        local_copy(3, q_gain_in, q_gain),
        local_copy(4, k_gain_in, k_gain),
    ]

    def shard_copies(target):
        return [
            local_copy(5, w_pool_in, target.at[:, pl.ds(0, branch)]),
            local_copy(6, w_query, target.at[:, pl.ds(branch, head_columns)]),
        ]

    def home_copies():
        return [
            local_copy(7, tokens, normed.at[:, aligned(place.tp, width)]),
            local_copy(8, w_out, last_weights.at[place.sp]),
            local_copy(9, pool_map, pool_maps),
            local_copy(10, pool_scale_in, pool_scales),
            local_copy(11, sinks_in, sinks),
        ]

    for copy in small[:2]:
        copy.start()

    @pl.when(home)
    def _():
        for copy in shard_copies(first_weights.at[own_rows]) + home_copies():
            copy.start()

    @pl.when(away)
    def _():
        for copy in shard_copies(own_shard):
            copy.start()

    for copy in small[2:]:
        copy.start()
    small[0].wait()
    small[1].wait()
    pair_columns = key_value[...].astype(f32).T.astype(bf16)

    def table_copies():
        return [
            remote(
                source,
                target,
                table_sem.at[0, index],
                table_sem.at[1, index],
                place.sibling(),
            )
            for index, (source, target) in enumerate(
                [(pool_map, pool_maps), (pool_scale_in, pool_scales), (sinks_in, sinks)]
            )
        ]

    def first_gave(half):
        return first.give(half, own_shard.at[pl.ds(half * (depth // 2), depth // 2)])

    def last_gave(half):
        return last.give(half, w_out.at[pl.ds(half * (mix // 2), mix // 2)])

    @pl.when(home)
    def _():
        first_weights[own_rows, pl.ds(mid, LANES)] = pair_columns
        for copy in shard_copies(first_weights.at[own_rows]):
            copy.wait()

    @pl.when(away)
    def _():
        own_shard[:, pl.ds(mid, LANES)] = pair_columns
        for copy in shard_copies(own_shard):
            copy.wait()

    pl.semaphore_wait(barrier, greetings)

    @pl.when(away)
    def _():
        for half in range(2):
            first_gave(half).start()

    def token_rows(chunk):
        return pl.ds(chunk * piece, piece)

    def landing(chunk, side, core):
        owner = 2 * (jnp.where(x == 0, side, 1 - side)) + core
        return normed.at[token_rows(chunk), aligned(owner, width)]

    def to_sibling(chunk):
        return remote(
            tokens.at[token_rows(chunk)],
            landing(chunk, 0, c),
            send_sem.at[0],
            near_sem.at[c, chunk],
            place.sibling(),
        )

    def to_x(chunk):
        return remote(
            tokens.at[token_rows(chunk)],
            landing(chunk, 0, c),
            send_sem.at[1],
            far_sem.at[c, chunk],
            place.along_x(y),
        )

    def to_y(chunk):
        return remote(
            tokens.at[token_rows(chunk)],
            landing(chunk, 0, c),
            send_sem.at[2],
            near_sem.at[c, chunk],
            place.along_y(y),
        )

    def by_x(chunk, core):
        return core == 1 or chunk == 1

    def relay(chunk, core):
        if by_x(chunk, core):
            held = landing(chunk, 0, core)
            device = place.along_x(c)
        else:
            held = landing(chunk, 1, core)
            device = place.along_y(c)
        return remote(
            held, held, relay_sem.at[core, chunk], far_sem.at[core, chunk], device
        )

    def near_wait(chunk, core):
        held = landing(chunk, 0, core)
        remote(
            held, held, send_sem.at[0], near_sem.at[core, chunk], place.sibling()
        ).wait_recv()

    def far_wait(chunk, core):
        held = landing(chunk, 1, core)
        remote(
            held, held, send_sem.at[0], far_sem.at[core, chunk], place.sibling()
        ).wait_recv()

    ahead = 3

    def send_tokens(chunk):
        to_x(chunk).start()
        to_y(chunk).start()

    @pl.when(home)
    def _():
        for copy in table_copies():
            copy.start()

    first.upto(0)
    for chunk in range(ahead):
        to_x(chunk).start()

    @pl.when(away)
    def _():
        for chunk in range(TOKEN_CHUNKS):
            to_sibling(chunk).start()
        for chunk in range(ahead):
            to_y(chunk).start()

    span = 2.0 * jnp.exp2(me.astype(f32))
    row = lax.broadcasted_iota(jnp.int32, (WINDOW, 2 * WINDOW), 0)
    column = lax.broadcasted_iota(jnp.int32, (WINDOW, 2 * WINDOW), 1)
    distance = (row + WINDOW - column).astype(f32)
    band[...] = jnp.where((distance >= 0.0) & (distance < span), 1.0, 0.0).astype(bf16)
    allowed = (distance >= 0.0) & (distance < float(WINDOW))
    for pair in range(pairs_of_heads):
        for half in range(2):
            head = (me * GROUP + 2 * pair + half + 1).astype(f32)
            slope = jnp.exp2(jnp.full((WINDOW, 2 * WINDOW), -8.0 / Q_HEADS, f32) * head)
            bias[pl.ds(pair * WINDOW, WINDOW), pl.ds(half * 2 * WINDOW, 2 * WINDOW)] = jnp.where(
                allowed, -slope * distance, MASKED
            )
    block_row = lax.broadcasted_iota(jnp.int32, (2 * LANES, 2 * LANES), 0) // HEAD_DIM
    block_column = lax.broadcasted_iota(jnp.int32, (2 * LANES, 2 * LANES), 1) // HEAD_DIM
    ones_block[...] = jnp.where(block_row == block_column, 1.0, 0.0).astype(bf16)
    pool_span[pl.ds(0, WINDOW)] = jnp.zeros((WINDOW, branch), bf16)

    acc[...] = jnp.zeros(acc.shape, f32)
    strip = 32

    def normalise(chunk):
        @pl.loop(0, piece // strip)
        def _(index):
            held = pl.ds(pl.multiple_of(chunk * piece + index * strip, strip), strip)
            values = normed[held].astype(f32)
            scale = lax.rsqrt(jnp.mean(values * values, axis=-1, keepdims=True) + epsilon)
            normed[held] = (values * scale * gain[...]).astype(bf16)

    lane = lax.broadcasted_iota(jnp.int32, (1, LANES), 1)
    low = lane < HEAD_DIM
    for copy in small[2:]:
        copy.wait()

    @pl.when(home)
    def _():
        for copy in home_copies():
            copy.wait()
        last.own_pair().start()

    @pl.when(away)
    def _():
        for copy in table_copies():
            copy.wait_recv()

    head_rows[...] = jnp.zeros(head_rows.shape, f32)
    head_rows[pl.ds(0, 1), pl.ds(0, HEAD_DIM)] = q_gain[...] * HEAD_DIM**-0.5
    head_rows[pl.ds(1, 1), pl.ds(0, HEAD_DIM)] = k_gain[...]
    once = head_rows[pl.ds(0, 1), :]
    head_rows[pl.ds(0, 1), :] = once + pltpu.roll(once, HEAD_DIM, 1)
    for pair in range(pairs_of_heads):
        one, two = sinks[:, 2 * pair : 2 * pair + 1], sinks[:, 2 * pair + 1 : 2 * pair + 2]
        head_rows[pl.ds(2 + pair, 1), :] = jnp.exp(
            jnp.where(low, jnp.broadcast_to(one, (1, LANES)), jnp.broadcast_to(two, (1, LANES)))
        )

    tile = piece

    def multiply(chunks, steps):
        @pl.loop(steps[0], steps[1])
        def _(step):
            for way in range(2):

                @pl.when(place.has(way, step) & (step + way > 0))
                def _(way=way):
                    block = aligned(place.source(way, step), 2 * depth)

                    size = tile * (2 if (chunks[0] | chunks[1]) % 2 == 0 else 1)

                    @pl.loop(chunks[0] * tile // size, chunks[1] * tile // size)
                    def _(index):
                        held = aligned(index, size)
                        acc[held] += dot(normed[held, block], first_weights[block, :])

    class Progress:
        rows, steps = 0, 0

    def catch_up(chunks, steps):
        if steps > Progress.steps:
            for step in range(Progress.steps, steps):
                for slot in range(2):
                    first.complete(step, slot)
            if Progress.rows > 0:
                multiply((0, Progress.rows), (Progress.steps, steps))
            Progress.steps = steps
        if chunks > Progress.rows:
            if steps > 0:
                multiply((Progress.rows, chunks), (0, steps))
            Progress.rows = chunks

    def settle(chunk):
        for core in range(2):

            @pl.when(away if by_x(chunk, core) else home)
            def _(core=core):
                relay(chunk, core).wait_send()

        normalise(chunk)

    first.upto(1)
    first.complete(0, 1)

    @pl.when(home)
    def _():
        for chunk in range(ahead):
            to_y(chunk).start()

    events = len(first.events)

    def pass_tokens(chunk):
        @pl.when(home)
        def _():
            for core in range(2):
                far_wait(chunk, core)
                if not by_x(chunk, core):
                    relay(chunk, core).start()
            near_wait(chunk, 1 - c)

        @pl.when(away)
        def _():
            for core in range(2):
                near_wait(chunk, core)
                if by_x(chunk, core):
                    relay(chunk, core).start()

        if chunk + ahead < TOKEN_CHUNKS:
            send_tokens(chunk + ahead)

    def use_tokens(chunk):
        @pl.when(away)
        def _():
            for core in range(2):
                far_wait(chunk, core)
            if chunk == TOKEN_CHUNKS - 1:
                for half in range(2):
                    last_gave(half).start()

        settle(chunk)
        known = first.done // 2
        if chunk == TOKEN_CHUNKS - 1:
            first.upto(events - 1)
        catch_up(chunk + 1, known)

    for chunk in range(TOKEN_CHUNKS):
        first.upto((chunk + 3) * events // 8 - 1)
        pass_tokens(chunk)
        if chunk > 1:
            use_tokens(chunk - 2)

    @pl.when(away)
    def _():
        last.own_pair().wait_recv()

    first.upto(7 * events // 8 - 1)
    last.pass_on(0, y)
    for chunk in range(max(0, TOKEN_CHUNKS - 2), TOKEN_CHUNKS):
        use_tokens(chunk)
    catch_up(TOKEN_CHUNKS, place.planes)

    one_low = jnp.where(low, 1.0, 0.0)

    def spread(kv, held, count_scale):
        size = kv.shape[0]
        key_low = jnp.where(low, kv, 0.0)
        value_high = jnp.where(low, 0.0, kv)
        keys_low[held] = key_low.astype(bf16)
        keys_high[held] = pltpu.roll(key_low, HEAD_DIM, 1).astype(bf16)
        ones_low = jnp.broadcast_to(one_low * count_scale, (size, LANES)).astype(bf16)
        ones_high = jnp.broadcast_to((1.0 - one_low) * count_scale, (size, LANES)).astype(bf16)
        values_low[held, pl.ds(0, LANES)] = pltpu.roll(value_high, HEAD_DIM, 1).astype(bf16)
        values_low[held, pl.ds(LANES, LANES)] = ones_low
        values_high[held, pl.ds(0, LANES)] = value_high.astype(bf16)
        values_high[held, pl.ds(LANES, LANES)] = ones_high

    def finalise(index):
        held = aligned(index, tile)
        sums = acc[held].astype(bf16)
        shifted = pl.ds(pl.multiple_of(index * tile + WINDOW, WINDOW), tile)
        pool_span[shifted] = sums[:, :branch]
        kv = sums[:, mid:].astype(f32)
        squares = jnp.where(low, kv * kv, 0.0)
        scale = lax.rsqrt(jnp.sum(squares, axis=-1, keepdims=True) * (1.0 / HEAD_DIM) + epsilon)
        kv = jnp.where(low, kv * scale * head_rows[pl.ds(1, 1), :], kv).astype(bf16)
        pairs[held] = kv
        spread(kv.astype(f32), shifted, 1.0)
        wide = 2 * LANES
        gain_row = head_rows[pl.ds(0, 1), :]
        query_gain = jnp.concatenate([gain_row, gain_row], axis=1)
        for start in range(0, head_columns, wide):
            query = sums[:, branch + start : branch + start + wide].astype(f32)
            square = query * query
            upper = square.astype(bf16)
            lower = (square - upper.astype(f32)).astype(bf16)
            total = dot(upper, ones_block[...]) + dot(lower, ones_block[...])
            scale = lax.rsqrt(total * (1.0 / HEAD_DIM) + epsilon)
            queries[held, pl.ds(start, wide)] = (
                query * scale * query_gain
            ).astype(bf16)

    def halo_copies(device):
        return [
            remote(
                source,
                target,
                halo_sem.at[0, index],
                halo_sem.at[1, index],
                device,
            )
            for index, (source, target) in enumerate(
                [
                    (pairs.at[pl.ds(rows - WINDOW, WINDOW)], halo_pairs),
                    (pool_span.at[pl.ds(WINDOW + rows - HALO_ROWS, HALO_ROWS)], halo_pool),
                ]
            )
        ]

    next_plane = {"sp": place.sp + 2, "tp": 2 * x}
    sends_up = (c == 1) & place.passes(0)
    finalise(rows // tile - 1)

    @pl.when(c == 0)
    def _():
        for copy in halo_copies({"tp": 2 * x + 1}):
            copy.start()

    @pl.when(sends_up)
    def _():
        for copy in halo_copies(next_plane):
            copy.start()

    @pl.loop(0, rows // tile - 1)
    def _(index):
        finalise(index)

    def pool(block):
        held = aligned(block, WINDOW)
        span_rows = pool_span[pl.ds(pl.multiple_of(block * WINDOW, WINDOW), 2 * WINDOW)]
        running = dot(band[...], span_rows)
        offset = lax.broadcasted_iota(jnp.int32, (WINDOW, 1), 0)
        position = (seq * rows + block * WINDOW + offset).astype(f32)
        counted = jnp.minimum(position + 1.0, span)
        difference = (running / counted - span_rows[WINDOW:].astype(f32)).astype(bf16)
        mapped = dot(difference, pool_maps[...]) * pool_scales[...]
        scale = lax.rsqrt(jnp.mean(mapped * mapped, axis=-1, keepdims=True) + epsilon)
        mixed[held, pl.ds(0, branch)] = (mapped * scale).astype(bf16)

    def attend(block):
        held = aligned(block, WINDOW)
        both = pl.ds(pl.multiple_of(block * WINDOW, WINDOW), 2 * WINDOW)
        key_pair = jnp.concatenate([keys_low[both], keys_high[both]], axis=0)
        value_pair = jnp.concatenate([values_low[both], values_high[both]], axis=0)
        parts, squares = [], None
        for pair in range(pairs_of_heads):
            lanes = pl.ds(pair * LANES, LANES)
            scores = lax.dot_general(
                queries[held, lanes],
                key_pair,
                (((1,), (1,)), ((), ())),
                preferred_element_type=f32,
            )
            weights = jnp.exp(scores + bias[pl.ds(pair * WINDOW, WINDOW)]).astype(bf16)
            result = dot(weights, value_pair)
            part = result[:, :LANES] / (
                result[:, LANES:] + head_rows[pl.ds(2 + pair, 1), :]
            )
            parts.append(part)
            squares = part * part if squares is None else squares + part * part
        mean = jnp.sum(squares, axis=-1, keepdims=True) * (1.0 / head_columns)
        scale = lax.rsqrt(mean + epsilon)
        for pair, part in enumerate(parts):
            mixed[held, pl.ds(branch + pair * LANES, LANES)] = (part * scale).astype(bf16)

    if halves:
        units_of = {0: [(1, 0), (2, out_width // 2)], 1: [(1, 0), (2, out_width // 2)]}
        unit_width = out_width // 2
    else:
        units_of = {0: [(1, 0)], 1: [(2, 0)]}
        unit_width = out_width

    step_of = min(unit_width, LANES)

    class Shard:
        def __init__(self, owner, event):
            slot, self.cut = last.events[event][1:]
            self.owner, self.event = owner, event
            self.units = units_of[slot] if self.cut is None else [units_of[slot][1 - self.cut]]
            self.columns = (0, out_width) if self.cut is None else (self.units[0][1], unit_width)

        def lanes(self, start, size):
            return pl.ds(pl.multiple_of(self.owner * out_width + start, step_of), size)

        def unit(self, start):
            return self.lanes(start, unit_width)

        def packed(self):
            return aligned(self.owner if halves else self.owner // 2, unit_width)

        def copy(self, source, target, sent, landed, device):
            return remote(
                source, target, sum_send.at[sent], sum_recv.at[landed, self.owner], device
            )

        def row_block(self, index, lanes):
            return normed.at[aligned(index, out_rows), lanes]

        def across_x(self, start):
            return self.copy(
                normed.at[aligned(1 - x, 2 * out_rows), self.unit(start)],
                from_x.at[:, self.packed()],
                0,
                0,
                place.along_x(c),
            )

        def across_y(self, start, part=None):
            if part is None:
                held = pl.ds(0, rows)
            else:
                held = aligned(1 - x if part == 0 else x, 2 * out_rows)
            landed = half_recv.at[self.event] if part == 0 else sum_recv.at[1, self.owner]
            return remote(
                normed.at[held, self.unit(start)],
                from_away.at[held, self.packed()],
                sum_send.at[1],
                landed,
                place.along_y(c),
            )

        def to_pair(self):
            lanes = self.lanes(*self.columns)
            return remote(
                self.row_block(2 * x + 1 - c, lanes),
                from_pair.at[:, lanes],
                sum_send.at[1],
                half_recv.at[2] if self.cut == 1 else sum_recv.at[1, self.owner],
                place.sibling(),
            )

        def away_final(self, start, core):
            lanes = self.unit(start)
            return self.copy(
                self.row_block(2 * x + core, lanes),
                from_last.at[:, lanes],
                2 + core,
                2,
                place.along_y(core),
            )

        def home_final(self, start, core):
            lanes = self.unit(start)
            return self.copy(
                self.row_block(2 * (1 - x) + core, lanes),
                from_last.at[:, lanes],
                2 + core,
                3,
                place.along_x(core),
            )

        def terms(self, least, end):
            lanes = self.lanes(*self.columns)

            @pl.loop(least // 2, end // 2)
            def _(index):
                held = aligned((1 - x + index) % 2, 2 * out_rows)
                value = dot(mixed[held, :], last_weights[self.owner, :, pl.ds(*self.columns)])
                normed[held, lanes] = value.astype(bf16)

        def go_across(self, part):
            for scheme, start in self.units:
                if scheme == 1:
                    if part != 1:
                        self.across_x(start).start()
                else:

                    @pl.when(away)
                    def _():
                        self.across_y(start, part).start()

        def first(self):
            self.terms(0, 4)
            self.go_across(None)

        def first_rows(self):
            self.terms(0, 2)
            self.go_across(0)

        def other_rows(self):
            self.terms(2, 4)
            self.go_across(1)

        def second(self):
            for scheme, start in self.units:
                lanes = self.unit(start)
                if scheme == 1:
                    self.across_x(start).wait_recv()
                    held = aligned(x, 2 * out_rows)
                    normed[held, lanes] = (
                        normed[held, lanes].astype(f32) + from_x[:, self.packed()].astype(f32)
                    ).astype(bf16)

                    @pl.when(away)
                    def _():
                        for core in range(2):
                            self.away_final(start, core).start()
                else:

                    @pl.when(home)
                    def _():
                        if self.event < 2:
                            self.across_y(start, 0).wait_recv()
                            self.across_y(start, 1).wait_recv()
                        else:
                            self.across_y(start).wait_recv()

                        @pl.loop(0, 4)
                        def _(index):
                            held = aligned(index, out_rows)
                            normed[held, lanes] = (
                                normed[held, lanes].astype(f32)
                                + from_away[held, self.packed()].astype(f32)
                            ).astype(bf16)

                        for core in range(2):
                            self.home_final(start, core).start()

            @pl.when(home)
            def _():
                self.to_pair().start()

        def third(self):
            lanes = self.lanes(*self.columns)
            for scheme, start in self.units:
                if scheme == 1:
                    self.away_final(start, 0).wait_recv()
                else:
                    self.home_final(start, 0).wait_recv()

            @pl.when(home)
            def _():
                out[:, lanes] = (
                    normed[aligned(2 * x + c, out_rows), lanes].astype(f32)
                    + from_last[:, lanes].astype(f32)
                ).astype(bf16)

            @pl.when(away)
            def _():
                self.to_pair().wait_recv()
                out[:, lanes] = (
                    from_pair[:, lanes].astype(f32) + from_last[:, lanes].astype(f32)
                ).astype(bf16)

    def each(event, stage):
        step, slot, _ = last.events[event]

        @pl.loop(0, 1 if step == 0 else 2)
        def _(way):
            plane = z + (2 * way - 1) * step

            @pl.when((plane >= 0) & (plane < place.planes))
            def _():
                getattr(Shard(2 * plane + slot, event), stage)()

    def take_halo():
        top = pl.ds(0, WINDOW)

        @pl.when(seq > 0)
        def _():
            for copy in halo_copies(next_plane):
                copy.wait_recv()
            spread(halo_pairs[...].astype(f32), top, 1.0)
            pool_span[pl.ds(WINDOW - HALO_ROWS, HALO_ROWS)] = halo_pool[...]

        @pl.when(seq == 0)
        def _():
            for ref in (keys_low, keys_high, values_low, values_high):
                ref[top] = jnp.zeros((WINDOW, ref.shape[1]), bf16)

    half = blocks // 2

    def mix_half(side):
        @pl.loop(0, half)
        def _(index):
            block = side * half + (index + 1) % half

            @pl.when(block == 0)
            def _():
                take_halo()

            pool(block)
            attend(block)

    mix_half(1 - x)
    last.share_taken()
    last.pass_on(0, 1 - y)
    last.done = 2
    last.taken_pair().wait_recv()
    for event in range(2):
        each(event, "first_rows")
    mix_half(x)
    for event in range(2):
        each(event, "other_rows")

    total = len(last.events)

    def all_sent(index, whole):
        remote(
            whole, whole, sum_send.at[index], sum_recv.at[0, 0], place.sibling()
        ).wait_send()

    def early_sends():
        def tokens_sent(index):
            remote(
                tokens, tokens, send_sem.at[index], near_sem.at[0, 0], place.sibling()
            ).wait_send()

        tokens_sent(1)
        tokens_sent(2)

        @pl.when(away)
        def _():
            tokens_sent(0)

        @pl.when(home)
        def _():
            for copy in table_copies():
                copy.wait_send()

        @pl.when((c == 0) | sends_up)
        def _():
            for copy in halo_copies(next_plane):
                copy.wait_send()

        first.sent_edges(first_gave)
        last.sent_edges(last_gave)
        for event in range(events):
            first.sent(event)
        if place.planes > 1:
            first.shared(first_weights.at[pl.ds(0, (place.planes - 1) * depth)])

    for event, (step, slot, cut) in enumerate(last.events):
        last.upto(event)
        if step > 0:
            last.complete(step, slot, cut)
            each(event, "first")
        waits = False
        if event > 0 and not waits:
            each(event - 1, "second")
        if event > 2:
            each(event - 3, "third")
        if event == min(3, total - 1):
            early_sends()
        if event > 3:
            last.sent(event - 4)
    each(total - 1, "second")
    for event in range(max(0, total - 3), total):
        each(event, "third")
    for event in range(max(0, total - 4), total):
        last.sent(event)
    if place.planes > 1:
        last.shared(last_weights.at[pl.ds(0, place.planes - 1)])
    all_sent(0, from_x)

    @pl.when(home)
    def _():
        all_sent(1, from_pair)

    @pl.when(away)
    def _():
        all_sent(1, from_away)

    for core in range(2):
        all_sent(2 + core, from_last.at[:, pl.ds(0, from_x.shape[1])])


def layer(tokens, w_pool_in, w_query, w_key_t, w_value_t, pool_map, w_out, *rows_in):
    count = lax.axis_size("sp")
    rows, width = tokens.shape
    depth, branch = w_pool_in.shape
    head_columns = w_query.shape[1]
    features = width * lax.axis_size("tp")
    mix, out_width = w_out.shape
    out_rows = rows // lax.axis_size("tp")
    out_columns = count * out_width
    sums = branch + head_columns + LANES
    dma = pltpu.SemaphoreType.DMA
    planes = count // 2
    hbm = pl.BlockSpec(memory_space=pltpu.HBM)
    flops = 2 * rows * features * sums + 2 * rows * mix * out_columns
    return pl.pallas_call(
        functools.partial(layer_kernel, count),
        out_shape=pltpu.VMEM((out_rows, out_columns), bf16),
        in_specs=[hbm] * 12,
        out_specs=pl.BlockSpec(memory_space=pltpu.VMEM),
        scratch_shapes=[
            pltpu.VMEM((rows, features), bf16),
            pltpu.VMEM((features, sums), bf16),
            pltpu.VMEM((count, mix, out_width), bf16),
            pltpu.VMEM((depth, sums), bf16),
            pltpu.VMEM((rows, sums), f32),
            pltpu.VMEM((rows, head_columns), bf16),
            pltpu.VMEM((WINDOW + rows, LANES), bf16),
            pltpu.VMEM((WINDOW + rows, LANES), bf16),
            pltpu.VMEM((WINDOW + rows, 2 * LANES), bf16),
            pltpu.VMEM((WINDOW + rows, 2 * LANES), bf16),
            pltpu.VMEM((WINDOW + rows, branch), bf16),
            pltpu.VMEM((rows, LANES), bf16),
            pltpu.VMEM((rows, mix), bf16),
            pltpu.VMEM((head_columns // LANES * WINDOW, 4 * WINDOW), f32),
            pltpu.VMEM((WINDOW, 2 * WINDOW), bf16),
            pltpu.VMEM((2 * LANES, 2 * LANES), bf16),
            pltpu.VMEM((WINDOW, LANES), bf16),
            pltpu.VMEM((HALO_ROWS, branch), bf16),
            pltpu.VMEM((2 * out_rows, out_columns // 2), bf16),
            pltpu.VMEM((out_rows, out_columns), bf16),
            pltpu.VMEM((rows, out_columns // 2), bf16),
            pltpu.VMEM((out_rows, out_columns), bf16),
            pltpu.VMEM((2 * HEAD_DIM, depth), bf16),
            pltpu.VMEM((branch, branch), bf16),
            pltpu.VMEM((1, features), f32),
            pltpu.VMEM((1, branch), f32),
            pltpu.VMEM((1, HEAD_DIM), f32),
            pltpu.VMEM((1, HEAD_DIM), f32),
            pltpu.VMEM((1, GROUP), f32),
            pltpu.VMEM((8, LANES), f32),
            dma((12,)),
            dma((3, 2, max(1, planes - 1), 2)),
            dma((3, 2, max(1, planes - 1), 2)),
            dma((8,)),
            dma((14,)),
            dma((2, TOKEN_CHUNKS)),
            dma((2, TOKEN_CHUNKS)),
            dma((3,)),
            dma((2, TOKEN_CHUNKS)),
            dma((2, 3)),
            dma((2, 2)),
            dma((4,)),
            dma((4, count)),
            dma((3,)),
        ],
        compiler_params=pltpu.CompilerParams(
            collective_id=0, has_side_effects=True, vmem_limit_bytes=60 * 1024 * 1024
        ),
        cost_estimate=pl.CostEstimate(
            flops=flops, bytes_accessed=4 * rows * width, transcendentals=0
        ),
    )(tokens, w_pool_in, w_query, w_key_t, w_value_t, pool_map, w_out, *rows_in)


def local(
    tokens,
    norm_gain,
    w_pool_in,
    w_query,
    w_key,
    w_value,
    pool_map,
    pool_scale,
    q_gain,
    k_gain,
    sinks,
    w_out,
):
    return layer(
        tokens,
        w_pool_in,
        w_query,
        w_key.T,
        w_value.T,
        pool_map[0],
        w_out,
        norm_gain[None],
        pool_scale[None],
        q_gain[None],
        k_gain[None],
        sinks[None],
    )


def solution(mesh):
    in_specs = (
        P("sp", "tp"),
        P(),
        P("sp", "tp"),
        P("sp", "tp"),
        P("sp", "tp"),
        P("sp", "tp"),
        P("tp", None, None),
        P("tp"),
        P(),
        P(),
        P("tp"),
        P("tp", "sp"),
    )
    out_specs = P(("sp", "tp"), None)
    return jax.shard_map(local, mesh=mesh, in_specs=in_specs, out_specs=out_specs, check_vma=False)
```
